512 devices in a mesh: grp: 2 (over y), sp: 64 (over z, core), tp: 4 (over x).
Axes of the slice: x: 4, y: 2, z: 32, core: 2. Of those that a mesh axis runs over, the one named last changes fastest.
The devices are a block of a 4x8x32 slice.
Arguments:
- hidden: bfloat16 [49152, 2048], P(('grp', 'sp'), 'tp'), parts along dimension 0, may hold values from -45 to 45
- norm_gain: bfloat16 [2048], replicated, may hold values from 0.099609375 to 1.8984375
- w_query: bfloat16 [2048, 1024], P(None, 'tp'), may hold values from -0.125 to 0.125
- w_key: bfloat16 [2048, 1024], P(None, 'tp'), may hold values from -0.125 to 0.125
- w_value: bfloat16 [2048, 1024], P(None, 'tp'), may hold values from -0.125 to 0.125
- query_gain: float32 [8, 128], P('tp'), may hold values from 0.3 to 16
- key_gain: float32 [8, 128], P('tp'), may hold values from 0.3 to 16
- w_out: bfloat16 [1024, 2048], P('tp'), may hold values from -1.5 to 1.5
Outputs:
- mixed: bfloat16 [49152, 2048], P(('grp', 'sp'), 'tp'), parts along dimension 0
- log_total: float32 [49152, 8], P(('grp', 'sp'), 'tp'), parts along dimension 0
The draws below stay inside these ranges and needn't reach their ends.
There are 2 independent parts, one for each index of `grp`. The reference program is written for one: setup_inputs(seed, part) draws one part's arguments, and reference() takes and returns one part's arrays. A program takes and returns all parts, laid end to end along the dimension named above; an argument that names none is the same for every part. Nothing has to cross between parts.
All inputs are finite; a program needn't handle non-finite values.
Results may differ from the reference program's by a relative error of at most 0.015.
The reference program's roundings to bfloat16 on the way count: a program that leaves them out, or rounds other values in their place, can miss the bound.
Values may be sent and summed in bfloat16 or wider, within the bound.
A program may use at most 64 MiB of HBM per device.

```python
import jax
import jax.numpy as jnp
from jax import lax

D = 2048
HEADS = 8
HEAD_DIM = 128
KEYS_BEHIND = 128
MIDDLE_DILATION = 4
WIDEST_DILATION = 16
TOKENS = 24576


def draw_hidden(key, part):
    row_key, col_key, base_key = jax.random.split(jax.random.fold_in(key, 17), 3)
    row_factor = jnp.exp(jax.random.uniform(row_key, (TOKENS, 1), jnp.float32, -1.2, 1.1))
    rising = 1.0 + 2.0 * jnp.arange(D, dtype=jnp.float32) / D
    col_factor = jnp.exp(jax.random.uniform(col_key, (1, D), jnp.float32, 0.0, 2.3)) * rising * 0.125
    base = jnp.clip(jax.random.normal(base_key, (TOKENS, D), jnp.float32), -4.0, 4.0)
    return (base * row_factor * col_factor).astype(jnp.bfloat16)


def head_gains(key, salt):
    channel_key = jax.random.fold_in(jax.random.fold_in(key, salt), 1)
    noise = jnp.clip(jax.random.normal(channel_key, (HEADS, HEAD_DIM), jnp.float32), -3.5, 3.5)
    return (1.0 + 0.18 * noise).astype(jnp.float32)


def draw_query_gain(key, part):
    return head_gains(key, 31)


def draw_key_gain(key, part):
    return head_gains(key, 47)


def block_levels(stream_key, shape, pieces, low, high):
    factor_of = 1.0
    for dim, parts in pieces:
        draws = jax.random.uniform(jax.random.fold_in(jax.random.fold_in(stream_key, 6), dim), (parts,), jnp.float32, low / len(pieces), high / len(pieces))
        factor_of = factor_of * jnp.repeat(jnp.exp(draws), shape[dim] // parts).reshape((-1,) + (1,) * (len(shape) - 1 - dim))
    return factor_of


def centred(key, dims, scale, bound, cuts=(), held_as=jnp.bfloat16):
    drawn = jax.random.normal(key, dims, jnp.float32) * scale
    if len(cuts) > 0:
        drawn = block_levels(key, dims, cuts, -0.22, 0.18) * drawn
    return jnp.clip(drawn, min=-bound, max=bound).astype(held_as)


def setup_inputs(seed: int = 0, part: int = 0) -> dict:
    seeds = jax.random.split(jax.random.key(seed), 9)
    part_splits = jax.random.split(jax.random.fold_in(seeds[8], part), 9)
    return {
        "hidden": draw_hidden(jax.random.fold_in(jax.random.fold_in(seeds[8], part), 71), part),
        "norm_gain": jnp.clip(1.0 + 0.18 * jax.random.normal(seeds[1], (D,), jnp.float32), 0.099609375, 1.8984375).astype(jnp.bfloat16),
        "w_query": centred(seeds[2], (D, HEADS * HEAD_DIM), D ** -0.5, 0.125, ((1, 4),)),
        "w_key": centred(seeds[3], (D, HEADS * HEAD_DIM), D ** -0.5, 0.125, ((1, 4),)),
        "w_value": centred(seeds[4], (D, HEADS * HEAD_DIM), D ** -0.5, 0.125, ((1, 4),)),
        "query_gain": draw_query_gain(jax.random.fold_in(seeds[8], 71), part),
        "key_gain": draw_key_gain(jax.random.fold_in(seeds[8], 71), part),
        "w_out": centred(seeds[7], (HEADS * HEAD_DIM, D), 16 ** -0.5, 1.5, ((0, 4),)),
    }


EPSILON = 1e-06
ROTARY_BASE = 500000.0

def rotate(values, positions):
    head_width = values.shape[-1]
    inverse = ROTARY_BASE ** (-jnp.arange(0, head_width, 2, dtype=jnp.float32) / head_width)
    angles = positions[:, None] * inverse[None, :]
    cosine = jnp.cos(angles)[:, None, :]
    sine = jnp.sin(angles)[:, None, :]
    half_width = head_width // 2
    first_half = values[..., :half_width]
    second_half = values[..., half_width:]
    return jnp.concatenate([first_half * cosine - second_half * sine, second_half * cosine + first_half * sine], axis=-1)

def head_norm(values, gains):
    normed = values * lax.rsqrt(lax.optimization_barrier(jnp.mean(values * values, axis=-1, keepdims=True)) + EPSILON)
    return normed * gains[None, :, :]

def dilated_branch(query, key_all, value_all, dilation_step):
    sequence_rows, head_count, head_width = query.shape
    class_rows = sequence_rows // dilation_step
    block_count = -(-class_rows // KEYS_BEHIND)
    padded_rows = block_count * KEYS_BEHIND

    def by_class(values):
        return values.reshape(class_rows, dilation_step, head_count, head_width).transpose(1, 0, 2, 3).astype(jnp.float32)
    query_blocks = jnp.pad(by_class(query), ((0, 0), (0, padded_rows - class_rows), (0, 0), (0, 0)))
    query_blocks = query_blocks.reshape(dilation_step, block_count, KEYS_BEHIND, head_count, head_width)

    def windows(values):
        padded = jnp.pad(by_class(values), ((0, 0), (KEYS_BEHIND, padded_rows - class_rows), (0, 0), (0, 0)))
        padded = padded.reshape(dilation_step, block_count + 1, KEYS_BEHIND, head_count, head_width)
        return jnp.concatenate([padded[:, :-1], padded[:, 1:]], axis=2)
    key_windows = windows(key_all)
    value_windows = windows(value_all)
    scores = jnp.einsum('rnqhd,rnkhd->rnhqk', query_blocks, key_windows) * head_width ** (-0.5)
    row_index = jnp.arange(KEYS_BEHIND, dtype=jnp.int32)[:, None]
    col_index = jnp.arange(2 * KEYS_BEHIND, dtype=jnp.int32)[None, :]
    distance = row_index + KEYS_BEHIND - col_index
    in_band = (distance >= 0) & (distance <= KEYS_BEHIND)
    class_index = jnp.arange(block_count, dtype=jnp.int32)[:, None] * KEYS_BEHIND + col_index - KEYS_BEHIND
    allowed = in_band[None, :, :] & (class_index >= 0)[:, None, :]
    scores = jnp.where(allowed[None, :, None, :, :], scores, -jnp.inf)
    row_max = lax.optimization_barrier(jnp.max(scores, axis=-1, keepdims=True))
    weights = jnp.exp(scores - row_max)
    weight_sum = lax.optimization_barrier(jnp.sum(weights, axis=-1))
    rounded = lax.optimization_barrier(weights.astype(jnp.bfloat16)).astype(jnp.float32)
    weighted = jnp.einsum('rnhqk,rnkhd->rnqhd', rounded, value_windows)
    branch_out = weighted / jnp.transpose(weight_sum, (0, 1, 3, 2))[..., None]
    branch_out = branch_out.reshape(dilation_step, padded_rows, head_count, head_width)[:, :class_rows]
    branch_out = branch_out.transpose(1, 0, 2, 3).reshape(sequence_rows, head_count, head_width)
    log_sum = jnp.transpose(row_max[..., 0] + jnp.log(weight_sum), (0, 1, 3, 2))
    log_sum = log_sum.reshape(dilation_step, padded_rows, head_count)[:, :class_rows]
    log_sum = log_sum.transpose(1, 0, 2).reshape(sequence_rows, head_count)
    return (branch_out, log_sum)

def reference(hidden, norm_gain, w_query, w_key, w_value, query_gain, key_gain, w_out):
    sequence_rows = hidden.shape[0]
    hidden_float = hidden.astype(jnp.float32)
    row_scale = lax.rsqrt(lax.optimization_barrier(jnp.mean(hidden_float * hidden_float, axis=1, keepdims=True)) + EPSILON)
    scaled = (hidden_float * norm_gain.astype(jnp.float32)[None, :]).astype(jnp.bfloat16)
    query_raw = jnp.dot(scaled, w_query, preferred_element_type=jnp.float32) * row_scale
    key_raw = jnp.dot(scaled, w_key, preferred_element_type=jnp.float32) * row_scale
    value_raw = jnp.dot(scaled, w_value, preferred_element_type=jnp.float32) * row_scale
    positions = jnp.arange(sequence_rows, dtype=jnp.int32).astype(jnp.float32)
    query = rotate(head_norm(query_raw.reshape(sequence_rows, HEADS, HEAD_DIM), query_gain), positions).astype(jnp.bfloat16)
    key_all = rotate(head_norm(key_raw.reshape(sequence_rows, HEADS, HEAD_DIM), key_gain), positions).astype(jnp.bfloat16)
    value_all = value_raw.astype(jnp.bfloat16).reshape(sequence_rows, HEADS, HEAD_DIM)
    branch_outs = []
    branch_logs = []
    for dilation_step in (1, MIDDLE_DILATION, WIDEST_DILATION):
        branch_out, log_sum = dilated_branch(query, key_all, value_all, dilation_step)
        branch_outs.append(branch_out)
        branch_logs.append(log_sum)
    stacked_logs = jnp.stack(branch_logs, axis=0)
    peak = lax.optimization_barrier(jnp.max(stacked_logs, axis=0))
    log_total = peak + jnp.log(lax.optimization_barrier(jnp.sum(jnp.exp(stacked_logs - peak[None]), axis=0)))
    shares = jnp.exp(stacked_logs - log_total[None])
    attended = lax.optimization_barrier(jnp.sum(shares[..., None] * jnp.stack(branch_outs, axis=0), axis=0))
    attended = attended.astype(jnp.bfloat16).reshape(sequence_rows, HEADS * HEAD_DIM)
    mixed = jnp.dot(attended, w_out, preferred_element_type=jnp.float32).astype(jnp.bfloat16)
    return (mixed, log_total)
```

```python
import functools

import jax
import jax.numpy as jnp
import numpy as np
from jax import lax
from jax.experimental import pallas as pl
from jax.experimental.pallas import tpu as pltpu
from jax.sharding import PartitionSpec as P

KEYS_BEHIND = 128
MIDDLE = 4
WIDEST = 16
EPSILON = 1e-06
ROTARY_BASE = 500000.0
NEG = -1e30

NC = MIDDLE
NI = WIDEST // MIDDLE
BF = jnp.bfloat16
F32 = jnp.float32
MESH = pl.DeviceIdType.MESH


def dot(a, b):
    return jnp.dot(a, b, preferred_element_type=F32)


def dot_nt(a, b):
    return lax.dot_general(a, b, (((1,), (1,)), ((), ())), preferred_element_type=F32)


def iota(shape, dim):
    return lax.broadcasted_iota(jnp.int32, shape, dim)


def kernel(
    n_tp, n_sp,
    hid_h, ngain, wq_h, wk_h, wv_h, qg_ref, kg_ref, wo_h, tabc_h, tabs_h, basec, bases,
    out_ref, log_ref,
    hid_v, hx, w_v, tabc, tabs, wcol, sbuf, fbuf, qb, kv, bias1, bias1e, bias4, bias16,
    o1, o4, o16, e1, e4, e16, attb, attl, attx, ag, lt, mm, macc,
    lsem, xs_own, xr_own, xs_fwd, xr_fwd, ds_q, dr_q, zs, zr, ws, wr, wds, wdr,
    ds_a, dr_a, ds_l, dr_l, as_own, ar_own, as_fwd, ar_fwd,
):
    tok, width = hid_v.shape
    rows = tok // NC
    half = rows // 2
    nj = tok // WIDEST
    cj = 2 * nj
    hd = KEYS_BEHIND
    depth = n_tp * width
    wo_rows = wo_h.shape[0]
    own0 = kv.shape[2] - cj
    n_near = own0 - cj
    n_far = n_near - cj
    last = n_far

    me = lax.axis_index("tp")
    sp = lax.axis_index("sp")
    core = lax.rem(sp, 2)
    other = 1 - core
    z = lax.div(sp, 2)
    lf = lax.rem(me + n_tp - 1, n_tp)
    rt = lax.rem(me + 1, n_tp)
    op = lax.rem(me + 2, n_tp)
    partner = sp + 1 - 2 * core
    up = lax.rem(sp + 2, n_sp)
    down = lax.rem(sp + n_sp - 2, n_sp)
    to_rt, to_lf, to_op = {"tp": rt}, {"tp": lf}, {"tp": op}
    to_partner, to_up, to_down = {"sp": partner}, {"sp": up}, {"sp": down}
    joff = pl.multiple_of(core * nj, 8)
    poff = pl.multiple_of(other * nj, 8)

    pending = []

    def send(src, dst, ssem, rsem, dev):
        copy = pltpu.make_async_remote_copy(
            src_ref=src, dst_ref=dst, send_sem=ssem, recv_sem=rsem, device_id=dev, device_id_type=MESH
        )
        copy.start()
        pending.append(copy)
        return copy

    def load(src, dst, k):
        copy = pltpu.make_async_copy(src, dst, lsem.at[k])
        copy.start()
        return copy

    c_hid = load(hid_h, hid_v, 0)
    for stage, (lo, hi) in enumerate(((n_near, own0), (n_far, n_near), (0, n_far))):
        @pl.when(z <= stage)
        def _():
            kv[:, :, lo:hi, :] = jnp.zeros((2, WIDEST, hi - lo, hd), BF)
    barrier = pltpu.get_barrier_semaphore()
    for dev in (to_rt, to_lf, to_op, to_partner):
        pl.semaphore_signal(barrier, inc=1, device_id=dev, device_id_type=MESH)
    has_up, has_down = z < n_sp // 2 - 1, z > 0

    @pl.when(has_up)
    def _():
        pl.semaphore_signal(barrier, inc=1, device_id=to_up, device_id_type=MESH)

    @pl.when(has_down)
    def _():
        pl.semaphore_signal(barrier, inc=1, device_id=to_down, device_id_type=MESH)

    own_col = pl.ds(pl.multiple_of(core * hd, hd), hd)
    oth_col = pl.ds(pl.multiple_of(other * hd, hd), hd)
    c_w = []
    for n, w in enumerate((wq_h, wk_h, wv_h)):
        c_w.append(load(w.at[:, own_col], w_v.at[:, pl.ds(n * hd, hd)], 1 + 2 * n))
        c_w.append(load(w.at[:, oth_col], w_v.at[:, pl.ds((3 + n) * hd, hd)], 2 + 2 * n))
    c_t = [load(tabc_h, tabc, 7), load(tabs_h, tabs, 8)]
    my_cols = pl.ds(pl.multiple_of(me * width, width), width)
    my_rows = pl.ds(pl.multiple_of(me * wo_rows, wo_rows), wo_rows)
    c_wo = load(wo_h.at[:, my_cols], wcol.at[my_rows, :], 9)

    prow = iota((tok, tok), 0)
    pcol = iota((tok, tok), 1)
    place = (pcol & (NC - 1)) * rows + ((pcol >> 2) & (NI - 1)) * nj + (pcol >> 4)
    perm = jnp.where(prow == place, 1.0, 0.0).astype(BF)
    c_hid.wait()
    mine = dot(perm, hid_v[...]).astype(BF)
    hx[me] = mine
    pl.semaphore_wait(barrier, 4 + has_up.astype(jnp.int32) + has_down.astype(jnp.int32))

    def x_own(c):
        part = hx.at[me, pl.ds(c * rows, rows), :]
        return (
            send(part, part, xs_own.at[c, 0], xr_own.at[c, 0], to_rt),
            send(part, part, xs_own.at[c, 1], xr_own.at[c, 1], to_lf),
        )

    x_sent = {0: x_own(0), 1: x_own(1)}

    for c in c_t:
        c.wait()
    bc, bs = basec[pl.ds(sp, 1), :], bases[pl.ds(sp, 1), :]
    oc, os_ = tabc[...], tabs[...]
    sign = jnp.where(iota((1, hd), 1) < hd // 2, -1.0, 1.0)
    tabc[...] = bc * oc - bs * os_
    tabs[...] = (bs * oc + bc * os_) * sign

    first_j = own0 - cj * z
    jq = iota((cj, own0 + cj), 0)
    jk = iota((cj, own0 + cj), 1)
    ok = (jk >= jq) & (jk <= jq + KEYS_BEHIND) & (jk >= first_j)
    bias16[...] = jnp.where(ok, 0.0, NEG)
    w4 = bias4.shape[1] // NI
    row = iota(bias4.shape, 0)
    col = iota(bias4.shape, 1)
    iq = (row * (65536 // cj + 1)) >> 16
    ik = (col * (65536 // w4 + 1)) >> 16
    j4 = own0 + cj - w4
    jk = j4 + col - ik * w4
    dist = NI * (own0 + (row - iq * cj) - jk) + iq - ik
    ok = (dist >= 0) & (dist <= KEYS_BEHIND) & (jk >= first_j)
    bias4[...] = jnp.where(ok, 0.0, NEG)
    row = iota(bias1.shape, 0)
    col = iota(bias1.shape, 1)
    uq = row >> 4
    uk = col >> 5
    rq = (uq >> 2) + NC * (uq & (NI - 1))
    rk = (uk >> 2) + NC * (uk & (NI - 1))
    dist = WIDEST * ((row & 15) + 16 - (col & 31)) + rq - rk
    ok = (dist >= 0) & (dist <= KEYS_BEHIND)
    bias1[...] = jnp.where(ok, 0.0, NEG)
    bias1e[...] = jnp.where(ok & ((col & 31) + own0 - 16 >= first_j), 0.0, NEG)

    def partial(c, s, acc, sq):
        h = hx[s, c * rows : (c + 1) * rows, :].astype(F32)
        sc = (h * ngain[s]).astype(BF)
        sq = sq + jnp.sum(h * h, axis=1, keepdims=True)
        acc = acc + dot(sc, w_v[pl.ds(pl.multiple_of(s * width, width), width), :])
        return acc, sq

    def head_rows(x, gain, cos, sin):
        x = x * lax.rsqrt(jnp.mean(x * x, axis=1, keepdims=True) + EPSILON) * gain
        return x * cos + pltpu.roll(x, hd // 2, 1) * sin

    def epilogue(c, acc, sq):
        rs = lax.rsqrt(sq / depth + EPSILON)
        cos = tabc[c * rows : (c + 1) * rows, :]
        sin = tabs[c * rows : (c + 1) * rows, :]
        parts = []
        for side, hidx in ((1, other), (0, core)):
            x = [acc[:, (3 * side + n) * hd : (3 * side + n + 1) * hd] * rs for n in range(3)]
            q = head_rows(x[0], qg_ref[hidx], cos, sin)
            k = head_rows(x[1], kg_ref[hidx], cos, sin)
            parts = [v.reshape(NI, nj, hd) for v in (q, k, x[2])]
            for n in range(3):
                if side == 1:
                    sbuf[n, c * NI : (c + 1) * NI, :, :] = parts[n]
                else:
                    fbuf[n, c * NI : (c + 1) * NI, pl.ds(joff, nj), :] = parts[n]
        return send(
            sbuf.at[:, pl.ds(c * NI, NI), :, :],
            fbuf.at[:, pl.ds(c * NI, NI), pl.ds(joff, nj), :],
            ds_q.at[c], dr_q.at[c], to_partner,
        )

    z_copies = {}
    for stage, (start, count, to) in enumerate(
        ((own0, cj, n_near), (n_near, cj, n_far), (n_far + cj - last, last, 0))
    ):
        for c in range(NC):
            u = pl.ds(c * NI, NI)
            z_copies[stage, c] = pltpu.make_async_remote_copy(
                src_ref=kv.at[:, u, pl.ds(start, count), :], dst_ref=kv.at[:, u, pl.ds(to, count), :],
                send_sem=zs.at[stage, c], recv_sem=zr.at[stage, c], device_id=to_up, device_id_type=MESH,
            )

    def z_send(stage, c):
        @pl.when((z >= stage) & has_up)
        def _():
            z_copies[stage, c].start()

    def z_wait(stage, c):
        @pl.when(z > stage)
        def _():
            z_copies[stage, c].wait_recv()

    def z_pass(stage, c):
        z_wait(stage, c)
        z_send(stage + 1, c)

    def own_pair(c, copy):
        copy.wait_recv()
        u = slice(c * NI, (c + 1) * NI)
        kv[0, u, own0:, :] = fbuf[1, u].astype(BF)
        kv[1, u, own0:, :] = fbuf[2, u].astype(BF)
        z_send(0, c)
        qb[u] = fbuf[0, u].astype(BF)

    for c in c_w:
        c.wait()
    for c in range(NC):
        right, left = x_sent[c]
        right.wait_recv()
        h0 = hx.at[lf, pl.ds(c * rows, half), :]
        f0 = send(h0, h0, xs_fwd.at[c, 0], xr_fwd.at[c, 0], to_rt)
        left.wait_recv()
        h1 = hx.at[rt, pl.ds(c * rows + half, half), :]
        f1 = send(h1, h1, xs_fwd.at[c, 1], xr_fwd.at[c, 1], to_lf)
        if c + 2 < NC:
            x_sent[c + 2] = x_own(c + 2)
        acc = jnp.zeros((rows, 6 * hd), F32)
        sq = jnp.zeros((rows, 1), F32)
        for s in (me, lf, rt):
            acc, sq = partial(c, s, acc, sq)
        if c >= 2:
            z_pass(0, c - 2)
        f0.wait_recv()
        f1.wait_recv()
        acc, sq = partial(c, op, acc, sq)
        own_pair(c, epilogue(c, acc, sq))

    wh = wo_rows // 2
    w_sent = []
    for n, dst in ((1, rt), (3, lf), (2, op)):
        src = wo_h.at[pl.ds(pl.multiple_of(core * wh, wh), wh), pl.ds(pl.multiple_of(dst * width, width), width)]
        to = wcol.at[pl.ds(pl.multiple_of(me * wo_rows + core * wh, wh), wh), :]
        w_sent.append(send(src, to, ws.at[n - 1], wr.at[n - 1], {"tp": dst}))

    def w_pass():
        fwd = []
        for k, (n, src) in enumerate(((1, lf), (3, rt), (2, op))):
            w_sent[k].wait_recv()
            part = wcol.at[pl.ds(pl.multiple_of(src * wo_rows + core * wh, wh), wh), :]
            fwd.append(send(part, part, wds.at[n - 1], wdr.at[n - 1], to_partner))
        return fwd

    def softmax(s, bias):
        s = s * (hd ** -0.5) + bias
        m = jnp.max(s, axis=1, keepdims=True)
        w = jnp.exp(s - m)
        l = jnp.sum(w, axis=1, keepdims=True)
        return w.astype(BF), m, l

    def wide(x):
        return jnp.broadcast_to(x, (x.shape[0], hd))

    def branch1(b):
        q = qb[:, 16 * b : 16 * b + 16, :].reshape(WIDEST * 16, hd)
        lo = own0 - 16 + 16 * b
        k = kv[0, :, lo : lo + 32, :].reshape(WIDEST * 32, hd)
        v = kv[1, :, lo : lo + 32, :].reshape(WIDEST * 32, hd)
        w, m, l = softmax(dot_nt(q, k), (bias1e if b == 0 else bias1)[...])
        o1[:, 16 * b : 16 * b + 16, :] = (dot(w, v) / l).reshape(WIDEST, 16, hd)
        e1[:, 16 * b : 16 * b + 16, :] = wide(m + jnp.log(l)).reshape(WIDEST, 16, hd)

    def branch4(c):
        u = slice(c * NI, (c + 1) * NI)
        q = qb[u].reshape(NI * cj, hd)
        k = kv[0, u, j4:, :].reshape(NI * w4, hd)
        v = kv[1, u, j4:, :].reshape(NI * w4, hd)
        w, m, l = softmax(dot_nt(q, k), bias4[...])
        o4[u] = (dot(w, v) / l).reshape(NI, cj, hd)
        e4[u] = wide(m + jnp.log(l)).reshape(NI, cj, hd)

    def branch16(c):
        for u in range(c * NI, (c + 1) * NI):
            w, m, l = softmax(dot_nt(qb[u], kv[0, u]), bias16[...])
            o16[u] = dot(w, kv[1, u]) / l
            e16[u] = wide(m + jnp.log(l))

    def finish(c):
        u = slice(c * NI, (c + 1) * NI)
        a, b, d = e1[u], e4[u], e16[u]
        top = jnp.maximum(jnp.maximum(a, b), d)
        total = top + jnp.log(jnp.exp(a - top) + jnp.exp(b - top) + jnp.exp(d - top))
        att = jnp.exp(a - total) * o1[u] + jnp.exp(b - total) * o4[u] + jnp.exp(d - total) * o16[u]
        attb[c] = att
        attl[c] = total
        attx[c] = attb[c, :, pl.ds(poff, nj), :].reshape(rows, hd).astype(BF)
        ag[me, c, core] = attb[c, :, pl.ds(joff, nj), :].reshape(rows, hd).astype(BF)
        lt[core, c] = attl[c, :, pl.ds(joff, nj), :]
        return (
            send(attx.at[c], ag.at[me, c, core], ds_a.at[c], dr_a.at[c], to_partner),
            send(attl.at[c, :, pl.ds(poff, nj), :], lt.at[core, c], ds_l.at[c], dr_l.at[c], to_partner),
        )

    def a_own(c, copies):
        copies[0].wait_recv()
        part = ag.at[me, c]
        return (
            send(part, part, as_own.at[c, 0], ar_own.at[c, 0], to_rt),
            send(part, part, as_own.at[c, 1], ar_own.at[c, 1], to_lf),
        )

    def a_fwd(c, copies):
        copies[0].wait_recv()
        p0 = ag.at[lf, c, 0]
        f0 = send(p0, p0, as_fwd.at[c, 0], ar_fwd.at[c, 0], to_rt)
        copies[1].wait_recv()
        p1 = ag.at[rt, c, 1]
        f1 = send(p1, p1, as_fwd.at[c, 1], ar_fwd.at[c, 1], to_lf)
        return f0, f1

    def a_mix(c, copies):
        for f in copies:
            f.wait_recv()
        lhs = jnp.concatenate([ag[s, c, h] for s in range(n_tp) for h in range(2)], axis=1)
        mm[c * rows : (c + 1) * rows, :] = dot(lhs, wcol[...]).astype(BF)

    t0 = iota((tok, rows), 0)
    q0 = iota((tok, rows), 1)

    def back(c):
        there = ((t0 & (NC - 1)) == c) & (q0 == ((t0 >> 2) & (NI - 1)) * nj + (t0 >> 4))
        return jnp.where(there, 1.0, 0.0).astype(BF)

    z_pass(1, 0)
    z_pass(0, 2)
    branch4(0)
    z_pass(1, 1)
    branch4(1)
    z_pass(0, 3)
    branch4(2)
    z_wait(2, 0)
    branch16(0)
    z_pass(1, 2)
    branch1(0)
    branch1(1)
    branch1(2)
    branch4(3)
    d0 = finish(0)
    z_wait(2, 1)
    branch16(1)
    z_pass(1, 3)
    d1 = finish(1)
    w_fwd = w_pass()
    a0 = a_own(0, d0)
    a1 = a_own(1, d1)
    f_0 = a_fwd(0, a0)
    c_wo.wait()
    for f in w_fwd:
        f.wait_recv()
    a_mix(0, f_0)
    z_wait(2, 2)
    branch16(2)
    d2 = finish(2)
    f_1 = a_fwd(1, a1)
    a_mix(1, f_1)
    a2 = a_own(2, d2)
    z_wait(2, 3)
    branch16(3)
    d3 = finish(3)
    f_2 = a_fwd(2, a2)
    a3 = a_own(3, d3)
    a_mix(2, f_2)
    macc[...] = sum(dot(back(c), mm[c * rows : (c + 1) * rows, :]) for c in range(3))
    for d in (d0, d1, d2, d3):
        d[1].wait_recv()
    lane = iota((1, hd), 1)
    acc = jnp.zeros((tok, hd), F32)
    for c in range(NC):
        x = jnp.where(lane == 0, lt[0, c].reshape(rows, hd), lt[1, c].reshape(rows, hd))
        hi = x.astype(BF)
        rest = x - hi.astype(F32)
        mid = rest.astype(BF)
        low = (rest - mid.astype(F32)).astype(BF)
        p = back(c)
        acc = acc + (dot(p, hi) + dot(p, mid) + dot(p, low))
    log_ref[...] = acc[:, :2]
    f_3 = a_fwd(3, a3)
    a_mix(3, f_3)
    out_ref[...] = (macc[...] + dot(back(3), mm[3 * rows :, :])).astype(BF)
    for copy in pending:
        copy.wait_send()
    for stage in range(3):
        @pl.when((z >= stage) & has_up)
        def _():
            for c in range(NC):
                z_copies[stage, c].wait_send()


def tables(tok, n_sp, hd):
    inv = ROTARY_BASE ** (-np.arange(0, hd, 2, dtype=np.float64) / hd)
    inv = np.concatenate([inv, inv]).astype(np.float32).astype(np.float64)
    nj = tok // WIDEST
    c, i, j = np.meshgrid(np.arange(NC), np.arange(NI), np.arange(nj), indexing="ij")
    off = (WIDEST * j + c + NC * i).reshape(-1).astype(np.float64)
    base = np.arange(n_sp, dtype=np.float64) * tok
    out = []
    for p in (off, base):
        a = p[:, None] * inv[None, :]
        out += [np.cos(a).astype(np.float32), np.sin(a).astype(np.float32)]
    return out


def local(n_tp, n_sp, hidden, norm_gain, w_query, w_key, w_value, query_gain, key_gain, w_out):
    tok, width = hidden.shape
    heads, hd = query_gain.shape
    rows = tok // NC
    nj = tok // WIDEST
    cj = 2 * nj
    keys = cj + KEYS_BEHIND
    w4 = cj + KEYS_BEHIND // NI
    tabc, tabs, basec, bases = tables(tok, n_sp, hd)
    dma = pltpu.SemaphoreType.DMA
    vm = pltpu.VMEM
    scratch = [
        vm((tok, width), BF),
        vm((n_tp, tok, width), BF),
        vm((n_tp * width, 6 * hd), BF),
        vm((tok, hd), F32), vm((tok, hd), F32),
        vm((n_tp * heads * hd, width), BF),
        vm((3, WIDEST, nj, hd), F32),
        vm((3, WIDEST, cj, hd), F32),
        vm((WIDEST, cj, hd), BF),
        vm((2, WIDEST, keys, hd), BF),
        vm((WIDEST * 16, WIDEST * 32), F32), vm((WIDEST * 16, WIDEST * 32), F32),
        vm((NI * cj, NI * w4), F32),
        vm((cj, keys), F32),
        vm((WIDEST, cj, hd), F32), vm((WIDEST, cj, hd), F32), vm((WIDEST, cj, hd), F32),
        vm((WIDEST, cj, hd), F32), vm((WIDEST, cj, hd), F32), vm((WIDEST, cj, hd), F32),
        vm((NC, NI, cj, hd), F32),
        vm((NC, NI, cj, hd), F32),
        vm((NC, rows, hd), BF),
        vm((n_tp, NC, 2, rows, hd), BF),
        vm((2, NC, NI, nj, hd), F32),
        vm((tok, width), BF),
        vm((tok, width), F32),
        dma((10,)),
        dma((NC, 2)), dma((NC, 2)), dma((NC, 2)), dma((NC, 2)),
        dma((NC,)), dma((NC,)),
        dma((3, NC)), dma((3, NC)),
        dma((3,)), dma((3,)), dma((3,)), dma((3,)),
        dma((NC,)), dma((NC,)), dma((NC,)), dma((NC,)),
        dma((NC, 2)), dma((NC, 2)), dma((NC, 2)), dma((NC, 2)),
    ]
    hbm = pl.BlockSpec(memory_space=pl.ANY)
    vmem = pl.BlockSpec(memory_space=pltpu.VMEM)
    return pl.pallas_call(
        functools.partial(kernel, n_tp, n_sp),
        out_shape=(
            jax.ShapeDtypeStruct((tok, width), BF),
            jax.ShapeDtypeStruct((tok, heads), F32),
        ),
        in_specs=[hbm, vmem, hbm, hbm, hbm, vmem, vmem, hbm, hbm, hbm, vmem, vmem],
        out_specs=(vmem, vmem),
        scratch_shapes=scratch,
        compiler_params=pltpu.CompilerParams(
            collective_id=0, has_side_effects=True, vmem_limit_bytes=62 * 1024 * 1024
        ),
    )(
        hidden, norm_gain.astype(F32).reshape(n_tp, 1, width), w_query, w_key, w_value,
        query_gain.reshape(heads, 1, hd), key_gain.reshape(heads, 1, hd), w_out,
        jnp.asarray(tabc), jnp.asarray(tabs), jnp.asarray(basec), jnp.asarray(bases),
    )


def solution(mesh):
    placed = (
        P(("grp", "sp"), "tp"),
        P(),
        P(None, "tp"),
        P(None, "tp"),
        P(None, "tp"),
        P("tp", None),
        P("tp", None),
        P("tp", None),
    )
    return jax.shard_map(
        functools.partial(local, mesh.shape["tp"], mesh.shape["sp"]),
        mesh=mesh,
        in_specs=placed,
        out_specs=(P(("grp", "sp"), "tp"), P(("grp", "sp"), "tp")),
        check_vma=False,
    )
```

```python
import functools

import jax
import jax.numpy as jnp
import numpy as np
from jax import lax
from jax.experimental import pallas as pl
from jax.experimental.pallas import tpu as pltpu
from jax.sharding import PartitionSpec as P

KEYS_BEHIND = 128
MIDDLE = 4
WIDEST = 16
EPSILON = 1e-06
ROTARY_BASE = 500000.0
NEG = -1e30

NC = MIDDLE
NI = WIDEST // MIDDLE
BF = jnp.bfloat16
F32 = jnp.float32
MESH = pl.DeviceIdType.MESH


def dot(a, b):
    return jnp.dot(a, b, preferred_element_type=F32)


def dot_nt(a, b):
    return lax.dot_general(a, b, (((1,), (1,)), ((), ())), preferred_element_type=F32)


def dot_tn(a, b):
    return lax.dot_general(a, b, (((0,), (0,)), ((), ())), preferred_element_type=F32)


def iota(shape, dim):
    return lax.broadcasted_iota(jnp.int32, shape, dim)


def kernel(
    n_tp, n_sp,
    hid_h, ng_h, wq_h, wk_h, wv_h, qg_h, kg_h, wo_h, tabc_h, tabs_h, basec_h, bases_h,
    out_ref, log_ref,
    hid_v, ng_v, ngain, qg_ref, kg_ref, basec, bases, hx, w_v, tabc, tabs, wcol, sbuf, fbuf, qb, kv, bias1, bias1e, bias4, bias16,
    o1, o4, o16, e1, e4, e16, attb, attl, attx, ag, lt, mm, macc,
    lsem, xs_own, xr_own, xs_fwd, xr_fwd, ds_q, dr_q, zs, zr, ws, wr, wds, wdr,
    ds_a, dr_a, ds_l, dr_l, as_own, ar_own, as_fwd, ar_fwd,
):
    tok, width = hid_v.shape
    rows = tok // NC
    half = rows // 2
    nj = tok // WIDEST
    cj = 2 * nj
    hd = KEYS_BEHIND
    depth = n_tp * width
    wo_rows = wo_h.shape[0]
    own0 = kv.shape[2] - cj
    n_near = own0 - cj
    n_far = n_near - cj
    last = n_far

    me = lax.axis_index("tp")
    sp = lax.axis_index("sp")
    core = lax.rem(sp, 2)
    other = 1 - core
    z = lax.div(sp, 2)
    lf = lax.rem(me + n_tp - 1, n_tp)
    rt = lax.rem(me + 1, n_tp)
    op = lax.rem(me + 2, n_tp)
    partner = sp + 1 - 2 * core
    up = lax.rem(sp + 2, n_sp)
    down = lax.rem(sp + n_sp - 2, n_sp)
    to_rt, to_lf, to_op = {"tp": rt}, {"tp": lf}, {"tp": op}
    to_partner, to_up, to_down = {"sp": partner}, {"sp": up}, {"sp": down}
    joff = pl.multiple_of(core * nj, 8)
    poff = pl.multiple_of(other * nj, 8)

    pending = []

    def send(src, dst, ssem, rsem, dev):
        copy = pltpu.make_async_remote_copy(
            src_ref=src, dst_ref=dst, send_sem=ssem, recv_sem=rsem, device_id=dev, device_id_type=MESH
        )
        copy.start()
        pending.append(copy)
        return copy

    def load(src, dst, k):
        copy = pltpu.make_async_copy(src, dst, lsem.at[k])
        copy.start()
        return copy

    c_hid = load(hid_h, hid_v, 0)
    for stage, (lo, hi) in enumerate(((n_near, own0), (n_far, n_near), (0, n_far))):
        @pl.when(z <= stage)
        def _():
            kv[:, :, lo:hi, :] = jnp.zeros((2, WIDEST, hi - lo, hd), BF)
    barrier = pltpu.get_barrier_semaphore()
    for dev in (to_rt, to_lf, to_op, to_partner):
        pl.semaphore_signal(barrier, inc=1, device_id=dev, device_id_type=MESH)
    has_up, has_down = z < n_sp // 2 - 1, z > 0

    @pl.when(has_up)
    def _():
        pl.semaphore_signal(barrier, inc=1, device_id=to_up, device_id_type=MESH)

    @pl.when(has_down)
    def _():
        pl.semaphore_signal(barrier, inc=1, device_id=to_down, device_id_type=MESH)

    own_col = pl.ds(pl.multiple_of(core * hd, hd), hd)
    oth_col = pl.ds(pl.multiple_of(other * hd, hd), hd)
    c_w = []
    for n, w in enumerate((wq_h, wk_h, wv_h)):
        c_w.append(load(w.at[:, own_col], w_v.at[:, pl.ds(n * hd, hd)], 1 + 2 * n))
        c_w.append(load(w.at[:, oth_col], w_v.at[:, pl.ds((3 + n) * hd, hd)], 2 + 2 * n))
    c_t = [load(tabc_h, tabc, 7), load(tabs_h, tabs, 8)]
    for n, (src, dst) in enumerate(
        ((ng_h, ng_v), (qg_h, qg_ref), (kg_h, kg_ref), (basec_h.at[pl.ds(sp, 1)], basec), (bases_h.at[pl.ds(sp, 1)], bases))
    ):
        c_t.append(load(src, dst, 10 + n))
    my_cols = pl.ds(pl.multiple_of(me * width, width), width)
    my_rows = pl.ds(pl.multiple_of(me * wo_rows, wo_rows), wo_rows)
    c_wo = load(wo_h.at[:, my_cols], wcol.at[my_rows, :], 9)

    prow = iota((tok, tok), 0)
    pcol = iota((tok, tok), 1)
    place = (pcol & (NC - 1)) * rows + ((pcol >> 2) & (NI - 1)) * nj + (pcol >> 4)
    perm = jnp.where(prow == place, 1.0, 0.0).astype(BF)
    with jax.named_scope("hid_wait"):
        c_hid.wait()
    mine = dot(perm, hid_v[...]).astype(BF)
    hx[me] = mine
    with jax.named_scope("barrier_wait"):
        pl.semaphore_wait(barrier, 4 + has_up.astype(jnp.int32) + has_down.astype(jnp.int32))

    def x_own(c):
        part = hx.at[me, pl.ds(c * rows, rows), :]
        return (
            send(part, part, xs_own.at[c, 0], xr_own.at[c, 0], to_rt),
            send(part, part, xs_own.at[c, 1], xr_own.at[c, 1], to_lf),
        )

    x_sent = {0: x_own(0), 1: x_own(1)}

    for c in c_t:
        c.wait()
    bc, bs = basec[0], bases[0]
    oc, os_ = tabc[...], tabs[...]
    sign = jnp.where(iota((1, hd), 1) < hd // 2, -1.0, 1.0)
    tabc[...] = bc * oc - bs * os_
    tabs[...] = (bs * oc + bc * os_) * sign

    gains = ng_v[...].astype(F32)
    for s in range(n_tp):
        for k in range(width // hd):
            r = s * (width // hd) + k
            ngain[s, :, k * hd : (k + 1) * hd] = gains[r : r + 1, :]
    first_j = own0 - cj * z
    jq = iota((cj, own0 + cj), 0)
    jk = iota((cj, own0 + cj), 1)
    ok = (jk >= jq) & (jk <= jq + KEYS_BEHIND) & (jk >= first_j)
    bias16[...] = jnp.where(ok, 0.0, NEG)
    w4 = bias4.shape[1] // NI
    row = iota(bias4.shape, 0)
    col = iota(bias4.shape, 1)
    iq = (row * (65536 // cj + 1)) >> 16
    ik = (col * (65536 // w4 + 1)) >> 16
    j4 = own0 + cj - w4
    jk = j4 + col - ik * w4
    dist = NI * (own0 + (row - iq * cj) - jk) + iq - ik
    ok = (dist >= 0) & (dist <= KEYS_BEHIND) & (jk >= first_j)
    bias4[...] = jnp.where(ok, 0.0, NEG)
    row = iota(bias1.shape, 0)
    col = iota(bias1.shape, 1)
    uq = row >> 4
    uk = col >> 5
    rq = (uq >> 2) + NC * (uq & (NI - 1))
    rk = (uk >> 2) + NC * (uk & (NI - 1))
    dist = WIDEST * ((row & 15) + 16 - (col & 31)) + rq - rk
    ok = (dist >= 0) & (dist <= KEYS_BEHIND)
    bias1[...] = jnp.where(ok, 0.0, NEG)
    bias1e[...] = jnp.where(ok & ((col & 31) + own0 - 16 >= first_j), 0.0, NEG)

    @jax.named_scope('partial')
    def partial(c, s, acc, sq):
        h = hx[s, c * rows : (c + 1) * rows, :].astype(F32)
        sc = (h * ngain[s]).astype(BF)
        sq = sq + jnp.sum(h * h, axis=1, keepdims=True)
        acc = acc + dot(sc, w_v[pl.ds(pl.multiple_of(s * width, width), width), :])
        return acc, sq

    def head_rows(x, gain, cos, sin):
        x = x * lax.rsqrt(jnp.mean(x * x, axis=1, keepdims=True) + EPSILON) * gain
        return x * cos + pltpu.roll(x, hd // 2, 1) * sin

    @jax.named_scope('epilogue')
    def epilogue(c, acc, sq):
        rs = lax.rsqrt(sq / depth + EPSILON)
        cos = tabc[c * rows : (c + 1) * rows, :]
        sin = tabs[c * rows : (c + 1) * rows, :]
        parts = []
        for side, hidx in ((1, other), (0, core)):
            x = [acc[:, (3 * side + n) * hd : (3 * side + n + 1) * hd] * rs for n in range(3)]
            q = head_rows(x[0], qg_ref[pl.ds(hidx, 1), :], cos, sin)
            k = head_rows(x[1], kg_ref[pl.ds(hidx, 1), :], cos, sin)
            parts = [v.reshape(NI, nj, hd) for v in (q, k, x[2])]
            for n in range(3):
                if side == 1:
                    sbuf[n, c * NI : (c + 1) * NI, :, :] = parts[n]
                else:
                    fbuf[n, c * NI : (c + 1) * NI, pl.ds(joff, nj), :] = parts[n]
        return send(
            sbuf.at[:, pl.ds(c * NI, NI), :, :],
            fbuf.at[:, pl.ds(c * NI, NI), pl.ds(joff, nj), :],
            ds_q.at[c], dr_q.at[c], to_partner,
        )

    z_copies = {}
    for stage, (start, count, to) in enumerate(
        ((own0, cj, n_near), (n_near, cj, n_far), (n_far + cj - last, last, 0))
    ):
        for c in range(NC):
            u = pl.ds(c * NI, NI)
            z_copies[stage, c] = pltpu.make_async_remote_copy(
                src_ref=kv.at[:, u, pl.ds(start, count), :], dst_ref=kv.at[:, u, pl.ds(to, count), :],
                send_sem=zs.at[stage, c], recv_sem=zr.at[stage, c], device_id=to_up, device_id_type=MESH,
            )

    def z_send(stage, c):
        @pl.when((z >= stage) & has_up)
        def _():
            z_copies[stage, c].start()

    @jax.named_scope('z_wait')
    def z_wait(stage, c):
        @pl.when(z > stage)
        def _():
            z_copies[stage, c].wait_recv()

    @jax.named_scope('z_pass')
    def z_pass(stage, c):
        z_wait(stage, c)
        z_send(stage + 1, c)

    @jax.named_scope('own_pair')
    def own_pair(c, copy):
        with jax.named_scope("pair_wait"):
            copy.wait_recv()
        u = slice(c * NI, (c + 1) * NI)
        kv[0, u, own0:, :] = fbuf[1, u].astype(BF)
        kv[1, u, own0:, :] = fbuf[2, u].astype(BF)
        z_send(0, c)
        qb[u] = fbuf[0, u].astype(BF)

    for c in c_w:
        c.wait()
    def x_step(c):
        right, left = x_sent[c]
        with jax.named_scope("x_wait"):
            right.wait_recv()
        h0 = hx.at[lf, pl.ds(c * rows, half), :]
        f0 = send(h0, h0, xs_fwd.at[c, 0], xr_fwd.at[c, 0], to_rt)
        with jax.named_scope("x_wait"):
            left.wait_recv()
        h1 = hx.at[rt, pl.ds(c * rows + half, half), :]
        f1 = send(h1, h1, xs_fwd.at[c, 1], xr_fwd.at[c, 1], to_lf)
        if c + 2 < NC:
            x_sent[c + 2] = x_own(c + 2)
        acc = jnp.zeros((rows, 6 * hd), F32)
        sq = jnp.zeros((rows, 1), F32)
        for s in (me, lf, rt):
            acc, sq = partial(c, s, acc, sq)
        return acc, sq, f0, f1

    def x_end(c, state):
        acc, sq, f0, f1 = state
        with jax.named_scope("xf_wait"):
            f0.wait_recv()
            f1.wait_recv()
        acc, sq = partial(c, op, acc, sq)
        return epilogue(c, acc, sq)

    state, pairs = {}, {}
    for c in range(NC):
        state[c] = x_step(c)
        if c >= 2:
            own_pair(c - 2, pairs[c - 2])
        if c >= 3:
            z_pass(0, c - 3)
        if c >= 1:
            pairs[c - 1] = x_end(c - 1, state[c - 1])

    wh = wo_rows // 2
    w_sent = []

    def w_start():
        for n, dst in ((1, rt), (3, lf), (2, op)):
            src = wo_h.at[pl.ds(pl.multiple_of(core * wh, wh), wh), pl.ds(pl.multiple_of(dst * width, width), width)]
            to = wcol.at[pl.ds(pl.multiple_of(me * wo_rows + core * wh, wh), wh), :]
            w_sent.append(send(src, to, ws.at[n - 1], wr.at[n - 1], {"tp": dst}))

    @jax.named_scope('w_pass')
    def w_pass():
        fwd = []
        for k, (n, src) in enumerate(((1, lf), (3, rt), (2, op))):
            w_sent[k].wait_recv()
            part = wcol.at[pl.ds(pl.multiple_of(src * wo_rows + core * wh, wh), wh), :]
            fwd.append(send(part, part, wds.at[n - 1], wdr.at[n - 1], to_partner))
        return fwd

    def softmax(s, bias):
        s = s * (hd ** -0.5) + bias
        m = jnp.max(s, axis=1, keepdims=True)
        w = jnp.exp(s - m)
        l = jnp.sum(w, axis=1, keepdims=True)
        return w.astype(BF), m, l

    def wide(x):
        return jnp.broadcast_to(x, (x.shape[0], hd))

    @jax.named_scope('branch1')
    def branch1(b):
        q = qb[:, 16 * b : 16 * b + 16, :].reshape(WIDEST * 16, hd)
        lo = own0 - 16 + 16 * b
        k = kv[0, :, lo : lo + 32, :].reshape(WIDEST * 32, hd)
        v = kv[1, :, lo : lo + 32, :].reshape(WIDEST * 32, hd)
        w, m, l = softmax(dot_nt(q, k), (bias1e if b == 0 else bias1)[...])
        o1[:, 16 * b : 16 * b + 16, :] = (dot(w, v) / l).reshape(WIDEST, 16, hd)
        e1[:, 16 * b : 16 * b + 16, :] = wide(m + jnp.log(l)).reshape(WIDEST, 16, hd)

    @jax.named_scope('branch4')
    def branch4(c):
        u = slice(c * NI, (c + 1) * NI)
        q = qb[u].reshape(NI * cj, hd)
        k = kv[0, u, j4:, :].reshape(NI * w4, hd)
        v = kv[1, u, j4:, :].reshape(NI * w4, hd)
        w, m, l = softmax(dot_nt(q, k), bias4[...])
        o4[u] = (dot(w, v) / l).reshape(NI, cj, hd)
        e4[u] = wide(m + jnp.log(l)).reshape(NI, cj, hd)

    @jax.named_scope('branch16')
    def branch16(c):
        us = range(c * NI, (c + 1) * NI)
        s = jnp.concatenate([dot_nt(qb[u], kv[0, u]) for u in us], axis=0)
        w, m, l = softmax(s, jnp.concatenate([bias16[...]] * NI, axis=0))
        e16[c * NI : (c + 1) * NI] = wide(m + jnp.log(l)).reshape(NI, cj, hd)
        for n, u in enumerate(us):
            part = slice(n * cj, (n + 1) * cj)
            o16[u] = dot(w[part], kv[1, u]) / l[part]

    @jax.named_scope('finish')
    def finish(c):
        u = slice(c * NI, (c + 1) * NI)
        a, b, d = e1[u], e4[u], e16[u]
        top = jnp.maximum(jnp.maximum(a, b), d)
        total = top + jnp.log(jnp.exp(a - top) + jnp.exp(b - top) + jnp.exp(d - top))
        att = jnp.exp(a - total) * o1[u] + jnp.exp(b - total) * o4[u] + jnp.exp(d - total) * o16[u]
        attb[c] = att
        attl[c] = total
        attx[c] = attb[c, :, pl.ds(poff, nj), :].reshape(rows, hd).astype(BF)
        ag[me, c, core] = attb[c, :, pl.ds(joff, nj), :].reshape(rows, hd).astype(BF)
        lt[core, c] = attl[c, :, pl.ds(joff, nj), :]
        return (
            send(attx.at[c], ag.at[me, c, core], ds_a.at[c], dr_a.at[c], to_partner),
            send(attl.at[c, :, pl.ds(poff, nj), :], lt.at[core, c], ds_l.at[c], dr_l.at[c], to_partner),
        )

    @jax.named_scope('a_own')
    def a_own(c, copies):
        copies[0].wait_recv()
        part = ag.at[me, c]
        return (
            send(part, part, as_own.at[c, 0], ar_own.at[c, 0], to_rt),
            send(part, part, as_own.at[c, 1], ar_own.at[c, 1], to_lf),
        )

    @jax.named_scope('a_fwd')
    def a_fwd(c, copies):
        copies[0].wait_recv()
        p0 = ag.at[lf, c, 0]
        f0 = send(p0, p0, as_fwd.at[c, 0], ar_fwd.at[c, 0], to_rt)
        copies[1].wait_recv()
        p1 = ag.at[rt, c, 1]
        f1 = send(p1, p1, as_fwd.at[c, 1], ar_fwd.at[c, 1], to_lf)
        return f0, f1

    @jax.named_scope('a_mix')
    def a_mix(c, copies):
        with jax.named_scope("af_wait"):
            for f in copies:
                f.wait_recv()
        lhs = jnp.concatenate([ag[s, c, h] for s in range(n_tp) for h in range(2)], axis=1)
        mm[c * rows : (c + 1) * rows, :] = dot(lhs, wcol[...]).astype(BF)

    t0 = iota((tok, rows), 0)
    q0 = iota((tok, rows), 1)

    def back(c):
        there = ((t0 & (NC - 1)) == c) & (q0 == ((t0 >> 2) & (NI - 1)) * nj + (t0 >> 4))
        return jnp.where(there, 1.0, 0.0).astype(BF)

    own_pair(2, pairs[2])
    branch4(0)
    pairs[3] = x_end(3, state[3])
    w_start()
    z_pass(0, 1)
    z_pass(1, 0)
    branch4(1)
    own_pair(3, pairs[3])
    z_pass(0, 2)
    z_pass(1, 1)
    branch4(2)
    z_wait(2, 0)
    branch16(0)
    z_pass(0, 3)
    z_pass(1, 2)
    for b in range(cj // 16):
        branch1(b)
    w_fwd = w_pass()
    sent, own, fwd = {}, {}, {}
    sent[0] = finish(0)
    branch4(3)
    z_wait(2, 1)
    branch16(1)
    sent[1] = finish(1)
    own[0] = a_own(0, sent[0])
    z_pass(1, 3)
    z_wait(2, 2)
    branch16(2)
    sent[2] = finish(2)
    own[1] = a_own(1, sent[1])
    fwd[0] = a_fwd(0, own[0])
    z_wait(2, 3)
    branch16(3)
    sent[3] = finish(3)
    own[2] = a_own(2, sent[2])
    fwd[1] = a_fwd(1, own[1])
    own[3] = a_own(3, sent[3])
    c_wo.wait()
    for f in w_fwd:
        f.wait_recv()
    a_mix(0, fwd[0])
    fwd[2] = a_fwd(2, own[2])
    a_mix(1, fwd[1])
    fwd[3] = a_fwd(3, own[3])
    a_mix(2, fwd[2])
    macc[...] = sum(dot(back(c), mm[c * rows : (c + 1) * rows, :]) for c in range(3))
    for d in sent.values():
        d[1].wait_recv()
    lane = iota((1, hd), 1)
    acc = jnp.zeros((hd, tok), F32)
    for c in range(NC):
        x = jnp.where(lane == 0, lt[0, c].reshape(rows, hd), lt[1, c].reshape(rows, hd))
        hi = x.astype(BF)
        rest = x - hi.astype(F32)
        mid = rest.astype(BF)
        low = (rest - mid.astype(F32)).astype(BF)
        p = perm[c * rows : (c + 1) * rows, :]
        acc = acc + (dot_tn(hi, p) + dot_tn(mid, p) + dot_tn(low, p))
    log_ref[...] = acc[:2, :]
    a_mix(3, fwd[3])
    out_ref[...] = (macc[...] + dot(back(3), mm[3 * rows :, :])).astype(BF)
    with jax.named_scope("drain"):
        for copy in pending:
            copy.wait_send()
    for stage in range(3):
        @pl.when((z >= stage) & has_up)
        def _():
            for c in range(NC):
                z_copies[stage, c].wait_send()


def tables(tok, n_sp, hd):
    inv = ROTARY_BASE ** (-np.arange(0, hd, 2, dtype=np.float64) / hd)
    inv = np.concatenate([inv, inv]).astype(np.float32).astype(np.float64)
    nj = tok // WIDEST
    c, i, j = np.meshgrid(np.arange(NC), np.arange(NI), np.arange(nj), indexing="ij")
    off = (WIDEST * j + c + NC * i).reshape(-1).astype(np.float64)
    base = np.arange(n_sp, dtype=np.float64) * tok
    out = []
    for p in (off, base):
        a = p[:, None] * inv[None, :]
        out += [np.cos(a).astype(np.float32), np.sin(a).astype(np.float32)]
    return out


def local(n_tp, n_sp, hidden, norm_gain, w_query, w_key, w_value, query_gain, key_gain, w_out):
    tok, width = hidden.shape
    heads, hd = query_gain.shape
    rows = tok // NC
    nj = tok // WIDEST
    cj = 2 * nj
    keys = cj + KEYS_BEHIND
    w4 = cj + KEYS_BEHIND // NI
    tabc, tabs, basec, bases = tables(tok, n_sp, hd)
    dma = pltpu.SemaphoreType.DMA
    vm = pltpu.VMEM
    scratch = [
        vm((tok, width), BF),
        vm((n_tp * width // hd, hd), BF),
        vm((n_tp, 1, width), F32),
        vm((heads, hd), F32), vm((heads, hd), F32),
        vm((1, 1, hd), F32), vm((1, 1, hd), F32),
        vm((n_tp, tok, width), BF),
        vm((n_tp * width, 6 * hd), BF),
        vm((tok, hd), F32), vm((tok, hd), F32),
        vm((n_tp * heads * hd, width), BF),
        vm((3, WIDEST, nj, hd), F32),
        vm((3, WIDEST, cj, hd), F32),
        vm((WIDEST, cj, hd), BF),
        vm((2, WIDEST, keys, hd), BF),
        vm((WIDEST * 16, WIDEST * 32), F32), vm((WIDEST * 16, WIDEST * 32), F32),
        vm((NI * cj, NI * w4), F32),
        vm((cj, keys), F32),
        vm((WIDEST, cj, hd), F32), vm((WIDEST, cj, hd), F32), vm((WIDEST, cj, hd), F32),
        vm((WIDEST, cj, hd), F32), vm((WIDEST, cj, hd), F32), vm((WIDEST, cj, hd), F32),
        vm((NC, NI, cj, hd), F32),
        vm((NC, NI, cj, hd), F32),
        vm((NC, rows, hd), BF),
        vm((n_tp, NC, 2, rows, hd), BF),
        vm((2, NC, NI, nj, hd), F32),
        vm((tok, width), BF),
        vm((tok, width), F32),
        dma((15,)),
        dma((NC, 2)), dma((NC, 2)), dma((NC, 2)), dma((NC, 2)),
        dma((NC,)), dma((NC,)),
        dma((3, NC)), dma((3, NC)),
        dma((3,)), dma((3,)), dma((3,)), dma((3,)),
        dma((NC,)), dma((NC,)), dma((NC,)), dma((NC,)),
        dma((NC, 2)), dma((NC, 2)), dma((NC, 2)), dma((NC, 2)),
    ]
    hbm = pl.BlockSpec(memory_space=pltpu.HBM)
    vmem = pl.BlockSpec(memory_space=pltpu.VMEM)
    mixed, logs = pl.pallas_call(
        functools.partial(kernel, n_tp, n_sp),
        out_shape=(
            jax.ShapeDtypeStruct((tok, width), BF),
            jax.ShapeDtypeStruct((heads, tok), F32),
        ),
        in_specs=[hbm] * 12,
        out_specs=(vmem, vmem),
        scratch_shapes=scratch,
        compiler_params=pltpu.CompilerParams(
            collective_id=0, has_side_effects=True, vmem_limit_bytes=63 * 1024 * 1024
        ),
    )(
        hidden, norm_gain.reshape(n_tp * width // hd, hd), w_query, w_key, w_value,
        query_gain, key_gain, w_out,
        jnp.asarray(tabc), jnp.asarray(tabs), jnp.asarray(basec)[:, None], jnp.asarray(bases)[:, None],
    )
    return mixed, logs.T


def solution(mesh):
    placed = (
        P(("grp", "sp"), "tp"),
        P(),
        P(None, "tp"),
        P(None, "tp"),
        P(None, "tp"),
        P("tp", None),
        P("tp", None),
        P("tp", None),
    )
    return jax.shard_map(
        functools.partial(local, mesh.shape["tp"], mesh.shape["sp"]),
        mesh=mesh,
        in_specs=placed,
        out_specs=(P(("grp", "sp"), "tp"), P(("grp", "sp"), "tp")),
        check_vma=False,
    )
```

```python
import functools

import jax
import jax.numpy as jnp
import numpy as np
from jax import lax
from jax.experimental import pallas as pl
from jax.experimental.pallas import tpu as pltpu
from jax.sharding import PartitionSpec as P

KEYS_BEHIND = 128
MIDDLE = 4
WIDEST = 16
EPSILON = 1e-06
ROTARY_BASE = 500000.0
NEG = -1e30

NC = MIDDLE
NI = WIDEST // MIDDLE
BF = jnp.bfloat16
F32 = jnp.float32
MESH = pl.DeviceIdType.MESH


def dot(a, b):
    return jnp.dot(a, b, preferred_element_type=F32)


def dot_nt(a, b):
    return lax.dot_general(a, b, (((1,), (1,)), ((), ())), preferred_element_type=F32)


def dot_tn(a, b):
    return lax.dot_general(a, b, (((0,), (0,)), ((), ())), preferred_element_type=F32)


def iota(shape, dim):
    return lax.broadcasted_iota(jnp.int32, shape, dim)


def early_kernel(
    n_tp, hid_h, wo_h, hx_out, wc_out,
    hid_v, hx, wcol, relay, lsem, xs_own, xr_own, xs_fwd, xr_fwd, ws, wr, osem,
):
    tok, width = hid_v.shape
    half = tok // 2
    wo_rows = wo_h.shape[0]
    me = lax.axis_index("tp")
    lf = lax.rem(me + n_tp - 1, n_tp)
    rt = lax.rem(me + 1, n_tp)
    op = lax.rem(me + 2, n_tp)

    def remote(src, dst, ssem, rsem, to):
        return pltpu.make_async_remote_copy(
            src_ref=src, dst_ref=dst, send_sem=ssem, recv_sem=rsem,
            device_id={"tp": to}, device_id_type=MESH,
        )

    def rows_of(ref, dev):
        return ref.at[pl.ds(pl.multiple_of(dev * wo_rows, wo_rows), wo_rows), :]

    def cols_of(dev):
        return wo_h.at[:, pl.ds(pl.multiple_of(dev * width, width), width)]

    @pl.when(lax.rem(lax.axis_index("sp"), 2) == 1)
    def _():
        c_hid = pltpu.make_async_copy(hid_h, hid_v, lsem.at[0])
        c_hid.start()
        barrier = pltpu.get_barrier_semaphore()
        for dev in (rt, lf, op):
            pl.semaphore_signal(barrier, inc=1, device_id={"tp": dev}, device_id_type=MESH)
        c_wo = pltpu.make_async_copy(cols_of(me), rows_of(wcol, me), lsem.at[1])
        c_wo.start()
        perm = placement(tok)
        c_hid.wait()
        hx[me] = dot(perm, hid_v[...]).astype(BF)
        pl.semaphore_wait(barrier, n_tp - 1)
        own, fwd = [], []
        for h in range(2):
            part = hx.at[me, pl.ds(h * half, half), :]
            own.append(remote(part, part, xs_own.at[h, 0], xr_own.at[h, 0], rt))
            own.append(remote(part, part, xs_own.at[h, 1], xr_own.at[h, 1], lf))
        for copy in own:
            copy.start()
        out = [remote(cols_of(dev), rows_of(wcol, me), ws.at[n], wr.at[n], dev) for n, dev in enumerate((rt, lf))]
        wh = wo_rows // 2
        turn, relayed = [], []
        for n, (dev, src) in enumerate(((rt, lf), (lf, rt))):
            part = wo_h.at[pl.ds(n * wh, wh), pl.ds(pl.multiple_of(op * width, width), width)]
            turn.append(remote(part, relay.at[n], ws.at[2 + n], wr.at[2 + n], dev))
            to = wcol.at[pl.ds(pl.multiple_of(src * wo_rows + n * wh, wh), wh), :]
            relayed.append(remote(relay.at[n], to, ws.at[4 + n], wr.at[4 + n], dev))
        for h in range(2):
            lo = pl.ds(h * half, half // 2)
            hi = pl.ds(h * half + half // 2, half // 2)
            own[2 * h].wait_recv()
            fwd.append(remote(hx.at[lf, lo, :], hx.at[lf, lo, :], xs_fwd.at[h, 0], xr_fwd.at[h, 0], rt))
            fwd[-1].start()
            own[2 * h + 1].wait_recv()
            fwd.append(remote(hx.at[rt, hi, :], hx.at[rt, hi, :], xs_fwd.at[h, 1], xr_fwd.at[h, 1], lf))
            fwd[-1].start()
        for copy in turn + out:
            copy.start()
        for n in range(2):
            turn[n].wait_recv()
            relayed[n].start()
        out = out + relayed
        for copy in fwd:
            copy.wait_recv()
        o_hx = pltpu.make_async_copy(hx, hx_out, osem.at[0])
        o_hx.start()
        c_wo.wait()
        for copy in out:
            copy.wait_recv()
        o_wc = pltpu.make_async_copy(wcol, wc_out, osem.at[1])
        o_wc.start()
        for copy in own + fwd + turn + out:
            copy.wait_send()
        o_hx.wait()
        o_wc.wait()


def placement(tok):
    prow = iota((tok, tok), 0)
    pcol = iota((tok, tok), 1)
    place = (pcol & (NC - 1)) * (tok // NC) + ((pcol >> 2) & (NI - 1)) * (tok // WIDEST) + (pcol >> 4)
    return jnp.where(prow == place, 1.0, 0.0).astype(BF)


def kernel(
    n_tp, n_sp, hxe_h, wce_h,
    hid_h, ng_h, wq_h, wk_h, wv_h, qg_h, kg_h, tabc_h, tabs_h, basec_h, bases_h,
    out_ref, log_ref,
    hid_v, ng_v, ngain, qg_ref, kg_ref, basec, bases, hx, w_v, tabc, tabs, wcol, sbuf, fbuf, qb, kv, bias1, bias1e, bias4, bias16,
    o1, o4, o16, e1, e4, e16, attb, attl, attx, ag, lt, mm, macc,
    lsem, xs_own, xr_own, xs_fwd, xr_fwd, ds_q, dr_q, zs, zr, ws, wr,
    ds_a, dr_a, ds_l, dr_l, as_own, ar_own, as_fwd, ar_fwd,
):
    tok, width = hid_v.shape
    rows = tok // NC
    half = rows // 2
    nj = tok // WIDEST
    cj = 2 * nj
    hd = KEYS_BEHIND
    depth = n_tp * width
    own0 = kv.shape[2] - cj
    n_near = own0 - cj
    n_far = n_near - cj
    last = n_far

    me = lax.axis_index("tp")
    sp = lax.axis_index("sp")
    core = lax.rem(sp, 2)
    other = 1 - core
    z = lax.div(sp, 2)
    lf = lax.rem(me + n_tp - 1, n_tp)
    rt = lax.rem(me + 1, n_tp)
    op = lax.rem(me + 2, n_tp)
    partner = sp + 1 - 2 * core
    up = lax.rem(sp + 2, n_sp)
    down = lax.rem(sp + n_sp - 2, n_sp)
    to_rt, to_lf, to_op = {"tp": rt}, {"tp": lf}, {"tp": op}
    to_partner, to_up, to_down = {"sp": partner}, {"sp": up}, {"sp": down}
    joff = pl.multiple_of(core * nj, 8)
    poff = pl.multiple_of(other * nj, 8)

    first, second = core == 0, core == 1
    pending = []

    def when(cond, f):
        if cond is None:
            f()
        else:
            pl.when(cond)(f)

    def send(src, dst, ssem, rsem, dev, cond=None):
        copy = pltpu.make_async_remote_copy(
            src_ref=src, dst_ref=dst, send_sem=ssem, recv_sem=rsem, device_id=dev, device_id_type=MESH
        )
        when(cond, copy.start)
        pending.append((cond, copy))
        return copy

    def load(src, dst, k):
        copy = pltpu.make_async_copy(src, dst, lsem.at[k])
        copy.start()
        return copy

    c_hid = pltpu.make_async_copy(hid_h, hid_v, lsem.at[0])
    c_hx = pltpu.make_async_copy(hxe_h, hx, lsem.at[0])
    c_wc = pltpu.make_async_copy(wce_h, wcol, lsem.at[9])
    when(first, c_hid.start)
    when(second, c_hx.start)
    for stage, (lo, hi) in enumerate(((n_near, own0), (n_far, n_near), (0, n_far))):
        @pl.when(z <= stage)
        def _():
            kv[:, :, lo:hi, :] = jnp.zeros((2, WIDEST, hi - lo, hd), BF)
    barrier = pltpu.get_barrier_semaphore()
    peers = [to_rt, to_lf, to_op, to_partner, {"tp": rt, "sp": partner}, {"tp": lf, "sp": partner}]
    for dev in peers:
        pl.semaphore_signal(barrier, inc=1, device_id=dev, device_id_type=MESH)
    has_up, has_down = z < n_sp // 2 - 1, z > 0

    @pl.when(has_down)
    def _():
        pl.semaphore_signal(barrier, inc=1, device_id=to_down, device_id_type=MESH)

    own_col = pl.ds(pl.multiple_of(core * hd, hd), hd)
    oth_col = pl.ds(pl.multiple_of(other * hd, hd), hd)
    c_w = []
    for n, w in enumerate((wq_h, wk_h, wv_h)):
        c_w.append(load(w.at[:, own_col], w_v.at[:, pl.ds(n * hd, hd)], 1 + 2 * n))
        c_w.append(load(w.at[:, oth_col], w_v.at[:, pl.ds((3 + n) * hd, hd)], 2 + 2 * n))
    c_t = [load(tabc_h, tabc, 7), load(tabs_h, tabs, 8)]
    for n, (src, dst) in enumerate(
        ((ng_h, ng_v), (qg_h, qg_ref), (kg_h, kg_ref), (basec_h.at[pl.ds(sp, 1)], basec), (bases_h.at[pl.ds(sp, 1)], bases))
    ):
        c_t.append(load(src, dst, 10 + n))
    when(second, c_wc.start)

    perm = placement(tok)

    @pl.when(first)
    def _():
        with jax.named_scope("hid_wait"):
            c_hid.wait()
        hx[me] = dot(perm, hid_v[...]).astype(BF)

    with jax.named_scope("barrier_wait"):
        pl.semaphore_wait(barrier, len(peers) + has_up.astype(jnp.int32))

    def x_own(c):
        part = hx.at[me, pl.ds(c * rows, rows), :]
        return (
            send(part, part, xs_own.at[c, 0], xr_own.at[c, 0], to_rt, first),
            send(part, part, xs_own.at[c, 1], xr_own.at[c, 1], to_lf, first),
        )

    x_sent = {c: x_own(c) for c in range(NC)}

    for c in c_t:
        c.wait()
    bc, bs = basec[0], bases[0]
    oc, os_ = tabc[...], tabs[...]
    sign = jnp.where(iota((1, hd), 1) < hd // 2, -1.0, 1.0)
    tabc[...] = bc * oc - bs * os_
    tabs[...] = (bs * oc + bc * os_) * sign

    gains = ng_v[...].astype(F32)
    for s in range(n_tp):
        for k in range(width // hd):
            r = s * (width // hd) + k
            ngain[s, :, k * hd : (k + 1) * hd] = gains[r : r + 1, :]
    first_j = own0 - cj * z
    jq = iota((cj, own0 + cj), 0)
    jk = iota((cj, own0 + cj), 1)
    ok = (jk >= jq) & (jk <= jq + KEYS_BEHIND) & (jk >= first_j)
    bias16[...] = jnp.where(ok, 0.0, NEG)
    w4 = bias4.shape[1] // NI
    row = iota(bias4.shape, 0)
    col = iota(bias4.shape, 1)
    iq = (row * (65536 // cj + 1)) >> 16
    ik = (col * (65536 // w4 + 1)) >> 16
    j4 = own0 + cj - w4
    jk = j4 + col - ik * w4
    dist = NI * (own0 + (row - iq * cj) - jk) + iq - ik
    ok = (dist >= 0) & (dist <= KEYS_BEHIND) & (jk >= first_j)
    bias4[...] = jnp.where(ok, 0.0, NEG)
    row = iota(bias1.shape, 0)
    col = iota(bias1.shape, 1)
    uq = row >> 4
    uk = col >> 5
    rq = (uq >> 2) + NC * (uq & (NI - 1))
    rk = (uk >> 2) + NC * (uk & (NI - 1))
    dist = WIDEST * ((row & 15) + 16 - (col & 31)) + rq - rk
    ok = (dist >= 0) & (dist <= KEYS_BEHIND)
    bias1[...] = jnp.where(ok, 0.0, NEG)
    bias1e[...] = jnp.where(ok & ((col & 31) + own0 - 16 >= first_j), 0.0, NEG)

    @jax.named_scope('partial')
    def partial(c, s, acc, sq):
        h = hx[s, c * rows : (c + 1) * rows, :].astype(F32)
        sc = (h * ngain[s]).astype(BF)
        sq = sq + jnp.sum(h * h, axis=1, keepdims=True)
        acc = acc + dot(sc, w_v[pl.ds(pl.multiple_of(s * width, width), width), :])
        return acc, sq

    def head_rows(x, gain, cos, sin):
        x = x * lax.rsqrt(jnp.mean(x * x, axis=1, keepdims=True) + EPSILON) * gain
        return x * cos + pltpu.roll(x, hd // 2, 1) * sin

    @jax.named_scope('epilogue')
    def epilogue(c, acc, sq):
        rs = lax.rsqrt(sq / depth + EPSILON)
        cos = tabc[c * rows : (c + 1) * rows, :]
        sin = tabs[c * rows : (c + 1) * rows, :]
        parts = []
        for side, hidx in ((1, other), (0, core)):
            x = [acc[:, (3 * side + n) * hd : (3 * side + n + 1) * hd] * rs for n in range(3)]
            q = head_rows(x[0], qg_ref[pl.ds(hidx, 1), :], cos, sin)
            k = head_rows(x[1], kg_ref[pl.ds(hidx, 1), :], cos, sin)
            parts = [v.reshape(NI, nj, hd) for v in (q, k, x[2])]
            for n in range(3):
                if side == 1:
                    sbuf[n, c * NI : (c + 1) * NI, :, :] = parts[n]
                else:
                    fbuf[n, c * NI : (c + 1) * NI, pl.ds(joff, nj), :] = parts[n]
        return send(
            sbuf.at[:, pl.ds(c * NI, NI), :, :],
            fbuf.at[:, pl.ds(c * NI, NI), pl.ds(joff, nj), :],
            ds_q.at[c], dr_q.at[c], to_partner,
        )

    z_copies = {}
    for stage, (start, count, to) in enumerate(
        ((own0, cj, n_near), (n_near, cj, n_far), (n_far + cj - last, last, 0))
    ):
        for c in range(NC):
            u = pl.ds(c * NI, NI)
            z_copies[stage, c] = pltpu.make_async_remote_copy(
                src_ref=kv.at[:, u, pl.ds(start, count), :], dst_ref=kv.at[:, u, pl.ds(to, count), :],
                send_sem=zs.at[stage, c], recv_sem=zr.at[stage, c], device_id=to_up, device_id_type=MESH,
            )

    def z_send(stage, c):
        @pl.when((z >= stage) & has_up)
        def _():
            z_copies[stage, c].start()

    @jax.named_scope('z_wait')
    def z_wait(stage, c):
        @pl.when(z > stage)
        def _():
            z_copies[stage, c].wait_recv()

    @jax.named_scope('z_pass')
    def z_pass(stage, c):
        z_wait(stage, c)
        z_send(stage + 1, c)

    @jax.named_scope('own_pair')
    def own_pair(c, copy):
        with jax.named_scope("pair_wait"):
            copy.wait_recv()
        u = slice(c * NI, (c + 1) * NI)
        kv[0, u, own0:, :] = fbuf[1, u].astype(BF)
        kv[1, u, own0:, :] = fbuf[2, u].astype(BF)
        z_send(0, c)
        qb[u] = fbuf[0, u].astype(BF)

    for c in c_w:
        c.wait()
    def x_step(c):
        right, left = x_sent[c]
        with jax.named_scope("x_wait"):
            when(first, right.wait_recv)
        h0 = hx.at[lf, pl.ds(c * rows, half), :]
        f0 = send(h0, h0, xs_fwd.at[c, 0], xr_fwd.at[c, 0], to_rt, first)
        with jax.named_scope("x_wait"):
            when(first, left.wait_recv)
        h1 = hx.at[rt, pl.ds(c * rows + half, half), :]
        f1 = send(h1, h1, xs_fwd.at[c, 1], xr_fwd.at[c, 1], to_lf, first)
        acc = jnp.zeros((rows, 6 * hd), F32)
        sq = jnp.zeros((rows, 1), F32)
        for s in (me, lf, rt):
            acc, sq = partial(c, s, acc, sq)
        return acc, sq, f0, f1

    def x_end(c, state):
        acc, sq, f0, f1 = state
        with jax.named_scope("xf_wait"):
            when(first, f0.wait_recv)
            when(first, f1.wait_recv)
        acc, sq = partial(c, op, acc, sq)
        return epilogue(c, acc, sq)

    with jax.named_scope("hx_wait"):
        when(second, c_hx.wait)
    def softmax(s, bias):
        s = s * (hd ** -0.5) + bias
        m = jnp.max(s, axis=1, keepdims=True)
        w = jnp.exp(s - m)
        l = jnp.sum(w, axis=1, keepdims=True)
        return w.astype(BF), m, l

    def wide(x):
        return jnp.broadcast_to(x, (x.shape[0], hd))

    @jax.named_scope('branch1')
    def branch1(b):
        q = qb[:, 16 * b : 16 * b + 16, :].reshape(WIDEST * 16, hd)
        lo = own0 - 16 + 16 * b
        k = kv[0, :, lo : lo + 32, :].reshape(WIDEST * 32, hd)
        v = kv[1, :, lo : lo + 32, :].reshape(WIDEST * 32, hd)
        w, m, l = softmax(dot_nt(q, k), (bias1e if b == 0 else bias1)[...])
        o1[:, 16 * b : 16 * b + 16, :] = (dot(w, v) / l).reshape(WIDEST, 16, hd)
        e1[:, 16 * b : 16 * b + 16, :] = wide(m + jnp.log(l)).reshape(WIDEST, 16, hd)

    @jax.named_scope('branch4')
    def branch4(c):
        u = slice(c * NI, (c + 1) * NI)
        q = qb[u].reshape(NI * cj, hd)
        k = kv[0, u, j4:, :].reshape(NI * w4, hd)
        v = kv[1, u, j4:, :].reshape(NI * w4, hd)
        w, m, l = softmax(dot_nt(q, k), bias4[...])
        o4[u] = (dot(w, v) / l).reshape(NI, cj, hd)
        e4[u] = wide(m + jnp.log(l)).reshape(NI, cj, hd)

    @jax.named_scope('branch16')
    def branch16(c):
        us = range(c * NI, (c + 1) * NI)
        s = jnp.concatenate([dot_nt(qb[u], kv[0, u]) for u in us], axis=0)
        w, m, l = softmax(s, jnp.concatenate([bias16[...]] * NI, axis=0))
        e16[c * NI : (c + 1) * NI] = wide(m + jnp.log(l)).reshape(NI, cj, hd)
        for n, u in enumerate(us):
            part = slice(n * cj, (n + 1) * cj)
            o16[u] = dot(w[part], kv[1, u]) / l[part]

    @jax.named_scope('finish')
    def finish(c):
        u = slice(c * NI, (c + 1) * NI)
        a, b, d = e1[u], e4[u], e16[u]
        top = jnp.maximum(jnp.maximum(a, b), d)
        total = top + jnp.log(jnp.exp(a - top) + jnp.exp(b - top) + jnp.exp(d - top))
        att = jnp.exp(a - total) * o1[u] + jnp.exp(b - total) * o4[u] + jnp.exp(d - total) * o16[u]
        attb[c] = att
        attl[c] = total
        attx[c] = attb[c, :, pl.ds(poff, nj), :].reshape(rows, hd).astype(BF)
        ag[me, c, core] = attb[c, :, pl.ds(joff, nj), :].reshape(rows, hd).astype(BF)
        lt[core, c] = attl[c, :, pl.ds(joff, nj), :]
        same, cross = ag.at[me, c, core], attx.at[c]
        for side, dev in ((0, rt), (1, lf)):
            send(same, same, as_own.at[c, side, 0], ar_own.at[c, side, core], {"tp": dev})
            send(cross, same, as_own.at[c, side, 1], ar_own.at[c, side, core], {"tp": dev, "sp": partner})
        send(cross, same, ds_a.at[c], dr_a.at[c], to_partner)
        return send(attl.at[c, :, pl.ds(poff, nj), :], lt.at[core, c], ds_l.at[c], dr_l.at[c], to_partner)

    def arrived(ref, sem):
        pltpu.make_async_remote_copy(
            src_ref=ref, dst_ref=ref, send_sem=sem, recv_sem=sem, device_id=to_partner, device_id_type=MESH
        ).wait_recv()

    @jax.named_scope('a_fwd')
    def a_fwd(c):
        p0, p1 = ag.at[lf, c, 0], ag.at[rt, c, 1]
        arrived(p0, ar_own.at[c, 0, 0])
        f0 = send(p0, p0, as_fwd.at[c, 0], ar_fwd.at[c, 0], to_rt)
        arrived(p1, ar_own.at[c, 1, 1])
        f1 = send(p1, p1, as_fwd.at[c, 1], ar_fwd.at[c, 1], to_lf)
        return f0, f1

    @jax.named_scope('a_mix')
    def a_mix(c, copies):
        with jax.named_scope("af_wait"):
            arrived(ag.at[lf, c, 1], ar_own.at[c, 0, 1])
            arrived(ag.at[rt, c, 0], ar_own.at[c, 1, 0])
            arrived(ag.at[me, c, other], dr_a.at[c])
            for f in copies:
                f.wait_recv()
        lhs = jnp.concatenate([ag[s, c, h] for s in range(n_tp) for h in range(2)], axis=1)
        mm[c * rows : (c + 1) * rows, :] = dot(lhs, wcol[...]).astype(BF)

    t0 = iota((tok, rows), 0)
    q0 = iota((tok, rows), 1)

    def back(c):
        there = ((t0 & (NC - 1)) == c) & (q0 == ((t0 >> 2) & (NI - 1)) * nj + (t0 >> 4))
        return jnp.where(there, 1.0, 0.0).astype(BF)

    state, pairs = {}, {}
    edge = z == 0

    def early(c):
        @pl.when(edge & first)
        def _():
            branch16(c)
            branch4(c)

    for c in range(NC):
        state[c] = x_step(c)
        if c >= 2:
            pl.when(first)(functools.partial(own_pair, c - 2, pairs[c - 2]))
        if c >= 3:
            early(c - 3)
        if c >= 1:
            pairs[c - 1] = x_end(c - 1, state[c - 1])
    pl.when(first)(functools.partial(own_pair, 2, pairs[2]))
    early(1)
    pairs[3] = x_end(3, state[3])
    when(second, c_wc.wait)
    c_w = send(wcol, wcol, ws.at[0], wr.at[0], to_partner, second)
    early(2)
    for c in range(3):
        pl.when(second)(functools.partial(own_pair, c, pairs[c]))

        @pl.when(edge & second)
        def _():
            branch16(c)
            branch4(c)

    own_pair(3, pairs[3])
    z_pass(0, 0)
    z_pass(0, 1)
    for c in range(3):
        pl.when(~edge)(functools.partial(branch4, c))
        if c + 2 < NC:
            z_pass(0, c + 2)
    for b in range(cj // 16):
        branch1(b)
    for c in range(NC):
        z_pass(1, c)
    branch4(3)
    logs_sent, fwd = {}, {}
    for c in range(NC):
        z_wait(2, c)
        if c == 3:
            branch16(c)
        else:
            pl.when(~edge)(functools.partial(branch16, c))
        logs_sent[c] = finish(c)
    for c in range(NC):
        fwd[c] = a_fwd(c)
    with jax.named_scope("w_wait"):
        when(first, c_w.wait_recv)
    for c in range(3):
        a_mix(c, fwd[c])
    macc[...] = sum(dot(back(c), mm[c * rows : (c + 1) * rows, :]) for c in range(3))
    for copy in logs_sent.values():
        copy.wait_recv()
    lane = iota((1, hd), 1)
    acc = jnp.zeros((hd, tok), F32)
    for c in range(NC):
        x = jnp.where(lane == 0, lt[0, c].reshape(rows, hd), lt[1, c].reshape(rows, hd))
        hi = x.astype(BF)
        rest = x - hi.astype(F32)
        mid = rest.astype(BF)
        low = (rest - mid.astype(F32)).astype(BF)
        p = perm[c * rows : (c + 1) * rows, :]
        acc = acc + (dot_tn(hi, p) + dot_tn(mid, p) + dot_tn(low, p))
    log_ref[...] = acc[:2, :]
    a_mix(3, fwd[3])
    out_ref[...] = (macc[...] + dot(back(3), mm[3 * rows :, :])).astype(BF)
    with jax.named_scope("drain"):
        for cond, copy in pending:
            when(cond, copy.wait_send)
    for stage in range(3):
        @pl.when((z >= stage) & has_up)
        def _():
            for c in range(NC):
                z_copies[stage, c].wait_send()


def tables(tok, n_sp, hd):
    inv = ROTARY_BASE ** (-np.arange(0, hd, 2, dtype=np.float64) / hd)
    inv = np.concatenate([inv, inv]).astype(np.float32).astype(np.float64)
    nj = tok // WIDEST
    c, i, j = np.meshgrid(np.arange(NC), np.arange(NI), np.arange(nj), indexing="ij")
    off = (WIDEST * j + c + NC * i).reshape(-1).astype(np.float64)
    base = np.arange(n_sp, dtype=np.float64) * tok
    out = []
    for p in (off, base):
        a = p[:, None] * inv[None, :]
        out += [np.cos(a).astype(np.float32), np.sin(a).astype(np.float32)]
    return out


def local(n_tp, n_sp, hidden, norm_gain, w_query, w_key, w_value, query_gain, key_gain, w_out):
    tok, width = hidden.shape
    heads, hd = query_gain.shape
    rows = tok // NC
    nj = tok // WIDEST
    cj = 2 * nj
    keys = cj + KEYS_BEHIND
    w4 = cj + KEYS_BEHIND // NI
    tabc, tabs, basec, bases = tables(tok, n_sp, hd)
    dma = pltpu.SemaphoreType.DMA
    vm = pltpu.VMEM
    scratch = [
        vm((tok, width), BF),
        vm((n_tp * width // hd, hd), BF),
        vm((n_tp, 1, width), F32),
        vm((heads, hd), F32), vm((heads, hd), F32),
        vm((1, 1, hd), F32), vm((1, 1, hd), F32),
        vm((n_tp, tok, width), BF),
        vm((n_tp * width, 6 * hd), BF),
        vm((tok, hd), F32), vm((tok, hd), F32),
        vm((n_tp * heads * hd, width), BF),
        vm((3, WIDEST, nj, hd), F32),
        vm((3, WIDEST, cj, hd), F32),
        vm((WIDEST, cj, hd), BF),
        vm((2, WIDEST, keys, hd), BF),
        vm((WIDEST * 16, WIDEST * 32), F32), vm((WIDEST * 16, WIDEST * 32), F32),
        vm((NI * cj, NI * w4), F32),
        vm((cj, keys), F32),
        vm((WIDEST, cj, hd), F32), vm((WIDEST, cj, hd), F32), vm((WIDEST, cj, hd), F32),
        vm((WIDEST, cj, hd), F32), vm((WIDEST, cj, hd), F32), vm((WIDEST, cj, hd), F32),
        vm((NC, NI, cj, hd), F32),
        vm((NC, NI, cj, hd), F32),
        vm((NC, rows, hd), BF),
        vm((n_tp, NC, 2, rows, hd), BF),
        vm((2, NC, NI, nj, hd), F32),
        vm((tok, width), BF),
        vm((tok, width), F32),
        dma((15,)),
        dma((NC, 2)), dma((NC, 2)), dma((NC, 2)), dma((NC, 2)),
        dma((NC,)), dma((NC,)),
        dma((3, NC)), dma((3, NC)),
        dma((1,)), dma((1,)),
        dma((NC,)), dma((NC,)), dma((NC,)), dma((NC,)),
        dma((NC, 2, 2)), dma((NC, 2, 2)), dma((NC, 2)), dma((NC, 2)),
    ]
    hbm = pl.BlockSpec(memory_space=pltpu.HBM)
    vmem = pl.BlockSpec(memory_space=pltpu.VMEM)
    early_hx, early_wc = pl.pallas_call(
        functools.partial(early_kernel, n_tp),
        out_shape=(
            jax.ShapeDtypeStruct((n_tp, tok, width), BF),
            jax.ShapeDtypeStruct((n_tp * heads * hd, width), BF),
        ),
        in_specs=[hbm] * 2,
        out_specs=(hbm, hbm),
        scratch_shapes=[
            vm((tok, width), BF), vm((n_tp, tok, width), BF), vm((n_tp * heads * hd, width), BF),
            vm((2, heads * hd // 2, width), BF),
            dma((2,)), dma((2, 2)), dma((2, 2)), dma((2, 2)), dma((2, 2)), dma((6,)), dma((6,)), dma((2,)),
        ],
        compiler_params=pltpu.CompilerParams(
            collective_id=1, has_side_effects=True, vmem_limit_bytes=63 * 1024 * 1024
        ),
    )(hidden, w_out)
    mixed, logs = pl.pallas_call(
        functools.partial(kernel, n_tp, n_sp),
        out_shape=(
            jax.ShapeDtypeStruct((tok, width), BF),
            jax.ShapeDtypeStruct((heads, tok), F32),
        ),
        in_specs=[hbm] * 13,
        out_specs=(vmem, vmem),
        scratch_shapes=scratch,
        compiler_params=pltpu.CompilerParams(
            collective_id=0, has_side_effects=True, vmem_limit_bytes=63 * 1024 * 1024
        ),
    )(
        early_hx, early_wc, hidden, norm_gain.reshape(n_tp * width // hd, hd), w_query, w_key, w_value,
        query_gain, key_gain,
        jnp.asarray(tabc), jnp.asarray(tabs), jnp.asarray(basec)[:, None], jnp.asarray(bases)[:, None],
    )
    return mixed, logs.T


def solution(mesh):
    placed = (
        P(("grp", "sp"), "tp"),
        P(),
        P(None, "tp"),
        P(None, "tp"),
        P(None, "tp"),
        P("tp", None),
        P("tp", None),
        P("tp", None),
    )
    return jax.shard_map(
        functools.partial(local, mesh.shape["tp"], mesh.shape["sp"]),
        mesh=mesh,
        in_specs=placed,
        out_specs=(P(("grp", "sp"), "tp"), P(("grp", "sp"), "tp")),
        check_vma=False,
    )
```

```python
import functools

import jax
import jax.numpy as jnp
import numpy as np
from jax import lax
from jax.experimental import pallas as pl
from jax.experimental.pallas import tpu as pltpu
from jax.sharding import PartitionSpec as P

KEYS_BEHIND = 128
MIDDLE = 4
WIDEST = 16
EPSILON = 1e-06
ROTARY_BASE = 500000.0
NEG = -1e30

NC = MIDDLE
NI = WIDEST // MIDDLE
BF = jnp.bfloat16
F32 = jnp.float32
MESH = pl.DeviceIdType.MESH


def dot(a, b):
    return jnp.dot(a, b, preferred_element_type=F32)


def dot_nt(a, b):
    return lax.dot_general(a, b, (((1,), (1,)), ((), ())), preferred_element_type=F32)


def dot_tn(a, b):
    return lax.dot_general(a, b, (((0,), (0,)), ((), ())), preferred_element_type=F32)


def iota(shape, dim):
    return lax.broadcasted_iota(jnp.int32, shape, dim)


def early_kernel(
    n_tp, hid_h, wo_h, hx_out, wc_out,
    hid_v, hx, wcol, relay, lsem, xs_own, xr_own, xs_fwd, xr_fwd, ws, wr, osem,
):
    tok, width = hid_v.shape
    half = tok // 2
    wo_rows = wo_h.shape[0]
    me = lax.axis_index("tp")
    lf = lax.rem(me + n_tp - 1, n_tp)
    rt = lax.rem(me + 1, n_tp)
    op = lax.rem(me + 2, n_tp)

    def remote(src, dst, ssem, rsem, to):
        return pltpu.make_async_remote_copy(
            src_ref=src, dst_ref=dst, send_sem=ssem, recv_sem=rsem,
            device_id={"tp": to}, device_id_type=MESH,
        )

    def rows_of(ref, dev):
        return ref.at[pl.ds(pl.multiple_of(dev * wo_rows, wo_rows), wo_rows), :]

    def cols_of(dev):
        return wo_h.at[:, pl.ds(pl.multiple_of(dev * width, width), width)]

    @pl.when(lax.rem(lax.axis_index("sp"), 2) == 1)
    def _():
        c_hid = pltpu.make_async_copy(hid_h, hid_v, lsem.at[0])
        c_hid.start()
        barrier = pltpu.get_barrier_semaphore()
        for dev in (rt, lf, op):
            pl.semaphore_signal(barrier, inc=1, device_id={"tp": dev}, device_id_type=MESH)
        c_wo = pltpu.make_async_copy(cols_of(me), rows_of(wcol, me), lsem.at[1])
        c_wo.start()
        perm = placement(tok)
        c_hid.wait()
        hx[me] = dot(perm, hid_v[...]).astype(BF)
        pl.semaphore_wait(barrier, n_tp - 1)
        own, fwd = [], []
        for h in range(2):
            part = hx.at[me, pl.ds(h * half, half), :]
            own.append(remote(part, part, xs_own.at[h, 0], xr_own.at[h, 0], rt))
            own.append(remote(part, part, xs_own.at[h, 1], xr_own.at[h, 1], lf))
        for copy in own:
            copy.start()
        out = [remote(cols_of(dev), rows_of(wcol, me), ws.at[n], wr.at[n], dev) for n, dev in enumerate((rt, lf))]
        wh = wo_rows // 2
        turn, relayed = [], []
        for n, (dev, src) in enumerate(((rt, lf), (lf, rt))):
            part = wo_h.at[pl.ds(n * wh, wh), pl.ds(pl.multiple_of(op * width, width), width)]
            turn.append(remote(part, relay.at[n], ws.at[2 + n], wr.at[2 + n], dev))
            to = wcol.at[pl.ds(pl.multiple_of(src * wo_rows + n * wh, wh), wh), :]
            relayed.append(remote(relay.at[n], to, ws.at[4 + n], wr.at[4 + n], dev))
        for h in range(2):
            lo = pl.ds(h * half, half // 2)
            hi = pl.ds(h * half + half // 2, half // 2)
            own[2 * h].wait_recv()
            fwd.append(remote(hx.at[lf, lo, :], hx.at[lf, lo, :], xs_fwd.at[h, 0], xr_fwd.at[h, 0], rt))
            fwd[-1].start()
            own[2 * h + 1].wait_recv()
            fwd.append(remote(hx.at[rt, hi, :], hx.at[rt, hi, :], xs_fwd.at[h, 1], xr_fwd.at[h, 1], lf))
            fwd[-1].start()
        for copy in turn + out:
            copy.start()
        for n in range(2):
            turn[n].wait_recv()
            relayed[n].start()
        out = out + relayed
        for copy in fwd:
            copy.wait_recv()
        o_hx = pltpu.make_async_copy(hx, hx_out, osem.at[0])
        o_hx.start()
        c_wo.wait()
        for copy in out:
            copy.wait_recv()
        o_wc = pltpu.make_async_copy(wcol, wc_out, osem.at[1])
        o_wc.start()
        for copy in own + fwd + turn + out:
            copy.wait_send()
        o_hx.wait()
        o_wc.wait()


def placement(tok):
    prow = iota((tok, tok), 0)
    pcol = iota((tok, tok), 1)
    place = (pcol & (NC - 1)) * (tok // NC) + ((pcol >> 2) & (NI - 1)) * (tok // WIDEST) + (pcol >> 4)
    return jnp.where(prow == place, 1.0, 0.0).astype(BF)


def kernel(
    n_tp, n_sp, hxe_h, wce_h,
    hid_h, ng_h, wq_h, wk_h, wv_h, qg_h, kg_h, tabc_h, tabs_h, basec_h, bases_h,
    out_ref, log_ref,
    hid_v, ng_v, ngain, qg_ref, kg_ref, basec, bases, hx, w_v, tabc, tabs, wcol, sbuf, fbuf, qb, kv, bias1, bias1e, bias4, bias16,
    o1, o4, o16, e1, e4, e16, attb, attl, attx, ag, lt, mm, macc,
    lsem, xs_own, xr_own, xs_fwd, xr_fwd, ds_q, dr_q, zs, zr, ws, wr,
    ds_a, dr_a, ds_l, dr_l, as_own, ar_own, as_fwd, ar_fwd, as_op, ar_op,
):
    tok, width = hid_v.shape
    rows = tok // NC
    half = rows // 2
    nj = tok // WIDEST
    cj = 2 * nj
    hd = KEYS_BEHIND
    depth = n_tp * width
    own0 = kv.shape[2] - cj
    n_near = own0 - cj
    n_far = n_near - cj
    last = n_far

    me = lax.axis_index("tp")
    sp = lax.axis_index("sp")
    core = lax.rem(sp, 2)
    other = 1 - core
    z = lax.div(sp, 2)
    lf = lax.rem(me + n_tp - 1, n_tp)
    rt = lax.rem(me + 1, n_tp)
    op = lax.rem(me + 2, n_tp)
    partner = sp + 1 - 2 * core
    up = lax.rem(sp + 2, n_sp)
    down = lax.rem(sp + n_sp - 2, n_sp)
    to_rt, to_lf, to_op = {"tp": rt}, {"tp": lf}, {"tp": op}
    to_partner, to_up, to_down = {"sp": partner}, {"sp": up}, {"sp": down}
    joff = pl.multiple_of(core * nj, 8)
    poff = pl.multiple_of(other * nj, 8)

    first, second = core == 0, core == 1
    pending = []

    def when(cond, f):
        if cond is None:
            f()
        else:
            pl.when(cond)(f)

    def send(src, dst, ssem, rsem, dev, cond=None):
        copy = pltpu.make_async_remote_copy(
            src_ref=src, dst_ref=dst, send_sem=ssem, recv_sem=rsem, device_id=dev, device_id_type=MESH
        )
        when(cond, copy.start)
        pending.append((cond, copy))
        return copy

    def load(src, dst, k):
        copy = pltpu.make_async_copy(src, dst, lsem.at[k])
        copy.start()
        return copy

    c_hid = pltpu.make_async_copy(hid_h, hid_v, lsem.at[0])
    c_hx = pltpu.make_async_copy(hxe_h, hx, lsem.at[0])
    c_wc = pltpu.make_async_copy(wce_h, wcol, lsem.at[9])
    barrier = pltpu.get_barrier_semaphore()
    peers = [
        to_rt, to_lf, to_op, to_partner,
        {"tp": rt, "sp": partner}, {"tp": lf, "sp": partner}, {"tp": op, "sp": partner},
    ]
    for dev in peers:
        pl.semaphore_signal(barrier, inc=1, device_id=dev, device_id_type=MESH)
    has_up, has_down = z < n_sp // 2 - 1, z > 0

    @pl.when(has_down)
    def _():
        pl.semaphore_signal(barrier, inc=1, device_id=to_down, device_id_type=MESH)

    when(first, c_hid.start)
    when(second, c_hx.start)
    own_col = pl.ds(pl.multiple_of(core * hd, hd), hd)
    oth_col = pl.ds(pl.multiple_of(other * hd, hd), hd)
    c_w = []
    for n, w in enumerate((wq_h, wk_h, wv_h)):
        c_w.append(load(w.at[:, own_col], w_v.at[:, pl.ds(n * hd, hd)], 1 + 2 * n))
        c_w.append(load(w.at[:, oth_col], w_v.at[:, pl.ds((3 + n) * hd, hd)], 2 + 2 * n))
    c_t = [load(tabc_h, tabc, 7), load(tabs_h, tabs, 8)]
    for n, (src, dst) in enumerate(
        ((ng_h, ng_v), (qg_h, qg_ref), (kg_h, kg_ref), (basec_h.at[pl.ds(sp, 1)], basec), (bases_h.at[pl.ds(sp, 1)], bases))
    ):
        c_t.append(load(src, dst, 10 + n))
    when(second, c_wc.start)

    perm = placement(tok)

    @pl.when(first)
    def _():
        with jax.named_scope("hid_wait"):
            c_hid.wait()
        hx[me] = dot(perm, hid_v[...]).astype(BF)

    with jax.named_scope("barrier_wait"):
        pl.semaphore_wait(barrier, len(peers) + has_up.astype(jnp.int32))

    def x_own(c):
        part = hx.at[me, pl.ds(c * rows, rows), :]
        return (
            send(part, part, xs_own.at[c, 0], xr_own.at[c, 0], to_rt, first),
            send(part, part, xs_own.at[c, 1], xr_own.at[c, 1], to_lf, first),
        )

    x_sent = {c: x_own(c) for c in range(NC)}

    for stage, (lo, hi) in enumerate(((n_near, own0), (n_far, n_near), (0, n_far))):
        @pl.when(z <= stage)
        def _():
            kv[:, :, lo:hi, :] = jnp.zeros((2, WIDEST, hi - lo, hd), BF)

    for c in c_t:
        c.wait()
    bc, bs = basec[0], bases[0]
    oc, os_ = tabc[...], tabs[...]
    sign = jnp.where(iota((1, hd), 1) < hd // 2, -1.0, 1.0)
    tabc[...] = bc * oc - bs * os_
    tabs[...] = (bs * oc + bc * os_) * sign

    gains = ng_v[...].astype(F32)
    for s in range(n_tp):
        for k in range(width // hd):
            r = s * (width // hd) + k
            ngain[s, :, k * hd : (k + 1) * hd] = gains[r : r + 1, :]
    first_j = own0 - cj * z
    jq = iota((cj, own0 + cj), 0)
    jk = iota((cj, own0 + cj), 1)
    ok = (jk >= jq) & (jk <= jq + KEYS_BEHIND) & (jk >= first_j)
    bias16[...] = jnp.where(ok, 0.0, NEG)
    w4 = bias4.shape[1] // NI
    row = iota(bias4.shape, 0)
    col = iota(bias4.shape, 1)
    iq = (row * (65536 // cj + 1)) >> 16
    ik = (col * (65536 // w4 + 1)) >> 16
    j4 = own0 + cj - w4
    jk = j4 + col - ik * w4
    dist = NI * (own0 + (row - iq * cj) - jk) + iq - ik
    ok = (dist >= 0) & (dist <= KEYS_BEHIND) & (jk >= first_j)
    bias4[...] = jnp.where(ok, 0.0, NEG)
    row = iota(bias1.shape, 0)
    col = iota(bias1.shape, 1)
    uq = row >> 4
    uk = col >> 5
    rq = (uq >> 2) + NC * (uq & (NI - 1))
    rk = (uk >> 2) + NC * (uk & (NI - 1))
    dist = WIDEST * ((row & 15) + 16 - (col & 31)) + rq - rk
    ok = (dist >= 0) & (dist <= KEYS_BEHIND)
    bias1[...] = jnp.where(ok, 0.0, NEG)
    bias1e[...] = jnp.where(ok & ((col & 31) + own0 - 16 >= first_j), 0.0, NEG)

    @jax.named_scope('partial')
    def partial(c, s, acc, sq):
        h = hx[s, c * rows : (c + 1) * rows, :].astype(F32)
        sc = (h * ngain[s]).astype(BF)
        sq = sq + jnp.sum(h * h, axis=1, keepdims=True)
        acc = acc + dot(sc, w_v[pl.ds(pl.multiple_of(s * width, width), width), :])
        return acc, sq

    def head_rows(x, gain, cos, sin):
        x = x * lax.rsqrt(jnp.mean(x * x, axis=1, keepdims=True) + EPSILON) * gain
        return x * cos + pltpu.roll(x, hd // 2, 1) * sin

    @jax.named_scope('epilogue')
    def epilogue(c, acc, sq):
        rs = lax.rsqrt(sq / depth + EPSILON)
        cos = tabc[c * rows : (c + 1) * rows, :]
        sin = tabs[c * rows : (c + 1) * rows, :]
        parts = []
        for side, hidx in ((1, other), (0, core)):
            x = [acc[:, (3 * side + n) * hd : (3 * side + n + 1) * hd] * rs for n in range(3)]
            q = head_rows(x[0], qg_ref[pl.ds(hidx, 1), :], cos, sin)
            k = head_rows(x[1], kg_ref[pl.ds(hidx, 1), :], cos, sin)
            parts = [v.reshape(NI, nj, hd) for v in (q, k, x[2])]
            for n in range(3):
                if side == 1:
                    sbuf[n, c * NI : (c + 1) * NI, :, :] = parts[n]
                else:
                    fbuf[n, c * NI : (c + 1) * NI, pl.ds(joff, nj), :] = parts[n]
        return send(
            sbuf.at[:, pl.ds(c * NI, NI), :, :],
            fbuf.at[:, pl.ds(c * NI, NI), pl.ds(joff, nj), :],
            ds_q.at[c], dr_q.at[c], to_partner,
        )

    z_copies = {}
    for stage, (start, count, to) in enumerate(
        ((own0, cj, n_near), (n_near, cj, n_far), (n_far + cj - last, last, 0))
    ):
        for c in range(NC):
            u = pl.ds(c * NI, NI)
            z_copies[stage, c] = [
                pltpu.make_async_remote_copy(
                    src_ref=kv.at[n, u, pl.ds(start, count), :], dst_ref=kv.at[n, u, pl.ds(to, count), :],
                    send_sem=zs.at[stage, c, n], recv_sem=zr.at[stage, c, n],
                    device_id=to_up, device_id_type=MESH,
                )
                for n in range(2)
            ]

    def z_send(stage, c, n):
        when((z >= stage) & has_up, z_copies[stage, c][n].start)

    @jax.named_scope('z_wait')
    def z_wait(stage, c):
        for n in range(2):
            when(z > stage, z_copies[stage, c][n].wait_recv)

    @jax.named_scope('z_pass')
    def z_pass(stage, c):
        for n in range(2):
            when(z > stage, z_copies[stage, c][n].wait_recv)
            z_send(stage + 1, c, n)

    @jax.named_scope('own_pair')
    def own_pair(c, copy):
        with jax.named_scope("pair_wait"):
            copy.wait_recv()
        u = slice(c * NI, (c + 1) * NI)
        for n in range(2):
            kv[n, u, own0:, :] = fbuf[1 + n, u].astype(BF)
            z_send(0, c, n)
        qb[u] = fbuf[0, u].astype(BF)

    for c in c_w:
        c.wait()
    def x_pass(c):
        right, left = x_sent[c]
        with jax.named_scope("x_wait"):
            when(first, right.wait_recv)
        h0 = hx.at[lf, pl.ds(c * rows, half), :]
        f0 = send(h0, h0, xs_fwd.at[c, 0], xr_fwd.at[c, 0], to_rt, first)
        with jax.named_scope("x_wait"):
            when(first, left.wait_recv)
        h1 = hx.at[rt, pl.ds(c * rows + half, half), :]
        f1 = send(h1, h1, xs_fwd.at[c, 1], xr_fwd.at[c, 1], to_lf, first)
        return f0, f1

    def x_near(c, passed):
        acc = jnp.zeros((rows, 6 * hd), F32)
        sq = jnp.zeros((rows, 1), F32)
        for s in (me, lf, rt):
            acc, sq = partial(c, s, acc, sq)
        return acc, sq, *passed

    def x_end(c, state):
        acc, sq, f0, f1 = state
        with jax.named_scope("xf_wait"):
            when(first, f0.wait_recv)
            when(first, f1.wait_recv)
        acc, sq = partial(c, op, acc, sq)
        return epilogue(c, acc, sq)

    with jax.named_scope("hx_wait"):
        when(second, c_hx.wait)
    def softmax(s, bias):
        s = s * (hd ** -0.5) + bias
        m = jnp.max(s, axis=1, keepdims=True)
        w = jnp.exp(s - m)
        l = jnp.sum(w, axis=1, keepdims=True)
        return w.astype(BF), m, l

    def wide(x):
        return jnp.broadcast_to(x, (x.shape[0], hd))

    @jax.named_scope('branch1')
    def branch1(b):
        q = qb[:, 16 * b : 16 * b + 16, :].reshape(WIDEST * 16, hd)
        lo = own0 - 16 + 16 * b
        k = kv[0, :, lo : lo + 32, :].reshape(WIDEST * 32, hd)
        v = kv[1, :, lo : lo + 32, :].reshape(WIDEST * 32, hd)
        w, m, l = softmax(dot_nt(q, k), (bias1e if b == 0 else bias1)[...])
        o1[:, 16 * b : 16 * b + 16, :] = (dot(w, v) / l).reshape(WIDEST, 16, hd)
        e1[:, 16 * b : 16 * b + 16, :] = wide(m + jnp.log(l)).reshape(WIDEST, 16, hd)

    @jax.named_scope('branch4')
    def branch4(c):
        u = slice(c * NI, (c + 1) * NI)
        q = qb[u].reshape(NI * cj, hd)
        k = kv[0, u, j4:, :].reshape(NI * w4, hd)
        v = kv[1, u, j4:, :].reshape(NI * w4, hd)
        w, m, l = softmax(dot_nt(q, k), bias4[...])
        o4[u] = (dot(w, v) / l).reshape(NI, cj, hd)
        e4[u] = wide(m + jnp.log(l)).reshape(NI, cj, hd)

    @jax.named_scope('branch16')
    def branch16(c):
        us = range(c * NI, (c + 1) * NI)
        s = jnp.concatenate([dot_nt(qb[u], kv[0, u]) for u in us], axis=0)
        w, m, l = softmax(s, jnp.concatenate([bias16[...]] * NI, axis=0))
        e16[c * NI : (c + 1) * NI] = wide(m + jnp.log(l)).reshape(NI, cj, hd)
        for n, u in enumerate(us):
            part = slice(n * cj, (n + 1) * cj)
            o16[u] = dot(w[part], kv[1, u]) / l[part]

    @jax.named_scope('finish')
    def finish(c):
        u = slice(c * NI, (c + 1) * NI)
        a, b, d = e1[u], e4[u], e16[u]
        top = jnp.maximum(jnp.maximum(a, b), d)
        total = top + jnp.log(jnp.exp(a - top) + jnp.exp(b - top) + jnp.exp(d - top))
        att = jnp.exp(a - total) * o1[u] + jnp.exp(b - total) * o4[u] + jnp.exp(d - total) * o16[u]
        attb[c] = att
        attl[c] = total
        attx[c] = attb[c, :, pl.ds(poff, nj), :].reshape(rows, hd).astype(BF)
        ag[me, c, core] = attb[c, :, pl.ds(joff, nj), :].reshape(rows, hd).astype(BF)
        lt[core, c] = attl[c, :, pl.ds(joff, nj), :]
        same, cross = ag.at[me, c, core], attx.at[c]
        for side, dev in ((0, rt), (1, lf)):
            send(same, same, as_own.at[c, side, 0], ar_own.at[c, side, core], {"tp": dev})
            send(cross, same, as_own.at[c, side, 1], ar_own.at[c, side, core], {"tp": dev, "sp": partner})
        if c == NC - 1:
            send(same, same, as_op.at[0], ar_op.at[core], to_op)
            send(cross, same, as_op.at[1], ar_op.at[core], {"tp": op, "sp": partner})
        send(cross, same, ds_a.at[c], dr_a.at[c], to_partner)
        return send(attl.at[c, :, pl.ds(poff, nj), :], lt.at[core, c], ds_l.at[c], dr_l.at[c], to_partner)

    def arrived(ref, sem):
        pltpu.make_async_remote_copy(
            src_ref=ref, dst_ref=ref, send_sem=sem, recv_sem=sem, device_id=to_partner, device_id_type=MESH
        ).wait_recv()

    @jax.named_scope('a_fwd')
    def a_fwd(c):
        p0, p1 = ag.at[lf, c, 0], ag.at[rt, c, 1]
        arrived(p0, ar_own.at[c, 0, 0])
        f0 = send(p0, p0, as_fwd.at[c, 0], ar_fwd.at[c, 0], to_rt)
        arrived(p1, ar_own.at[c, 1, 1])
        f1 = send(p1, p1, as_fwd.at[c, 1], ar_fwd.at[c, 1], to_lf)
        return f0, f1

    @jax.named_scope('a_mix')
    def a_mix(c, copies):
        with jax.named_scope("af_wait"):
            arrived(ag.at[lf, c, 1], ar_own.at[c, 0, 1])
            arrived(ag.at[rt, c, 0], ar_own.at[c, 1, 0])
            arrived(ag.at[me, c, other], dr_a.at[c])
            if c < NC - 1:
                for f in copies:
                    f.wait_recv()
            else:
                arrived(ag.at[lf, c, 0], ar_own.at[c, 0, 0])
                arrived(ag.at[rt, c, 1], ar_own.at[c, 1, 1])
                for h in range(2):
                    arrived(ag.at[op, c, h], ar_op.at[h])
        lhs = jnp.concatenate([ag[s, c, h] for s in range(n_tp) for h in range(2)], axis=1)
        mm[c * rows : (c + 1) * rows, :] = dot(lhs, wcol[...]).astype(BF)

    t0 = iota((tok, rows), 0)
    q0 = iota((tok, rows), 1)

    def back(c):
        there = ((t0 & (NC - 1)) == c) & (q0 == ((t0 >> 2) & (NI - 1)) * nj + (t0 >> 4))
        return jnp.where(there, 1.0, 0.0).astype(BF)

    state, pairs = {}, {}
    edge = z == 0

    def early(c):
        @pl.when(edge & first)
        def _():
            branch16(c)
            branch4(c)

    def pair_first(c):
        pl.when(first)(functools.partial(own_pair, c, pairs[c]))

    passed = {0: x_pass(0), 1: x_pass(1)}
    state[0] = x_near(0, passed[0])
    passed[2] = x_pass(2)
    state[1] = x_near(1, passed[1])
    passed[3] = x_pass(3)
    pairs[0] = x_end(0, state[0])
    state[2] = x_near(2, passed[2])
    pair_first(0)
    pairs[1] = x_end(1, state[1])
    state[3] = x_near(3, passed[3])
    pair_first(1)
    pairs[2] = x_end(2, state[2])
    pairs[3] = x_end(3, state[3])
    pair_first(2)
    when(second, c_wc.wait)
    c_w = send(wcol, wcol, ws.at[0], wr.at[0], to_partner, second)
    early(0)
    for c in range(3):
        pl.when(second)(functools.partial(own_pair, c, pairs[c]))

    pl.when(edge & second)(functools.partial(branch4, 0))
    own_pair(3, pairs[3])
    z_pass(0, 0)
    z_pass(0, 1)
    for c in range(2):
        pl.when(~edge)(functools.partial(branch4, c))
        pl.when(z == 1)(functools.partial(branch16, c))
        z_pass(0, c + 2)
    for b in range(cj // 16):
        branch1(b)
    for c in range(NC):
        z_pass(1, c)
        if c < 2:
            pl.when(z == 2)(functools.partial(branch16, c))
    logs_sent, fwd = {}, {}
    for c in range(NC):
        z_wait(2, c)
        if c < 2:
            pl.when((z > 2) | (edge & (second | (c > 0))))(functools.partial(branch16, c))
            if c > 0:
                pl.when(edge)(functools.partial(branch4, c))
        else:
            if c == 2:
                branch4(2)
            branch16(c)
        logs_sent[c] = finish(c)
        if c == 2:
            branch4(3)
    for c in range(NC - 1):
        fwd[c] = a_fwd(c)
    fwd[NC - 1] = ()
    with jax.named_scope("w_wait"):
        when(first, c_w.wait_recv)
    for c in range(3):
        a_mix(c, fwd[c])
    macc[...] = sum(dot(back(c), mm[c * rows : (c + 1) * rows, :]) for c in range(3))
    for copy in logs_sent.values():
        copy.wait_recv()
    lane = iota((1, hd), 1)
    acc = jnp.zeros((hd, tok), F32)
    for c in range(NC):
        x = jnp.where(lane == 0, lt[0, c].reshape(rows, hd), lt[1, c].reshape(rows, hd))
        hi = x.astype(BF)
        rest = x - hi.astype(F32)
        mid = rest.astype(BF)
        low = (rest - mid.astype(F32)).astype(BF)
        p = perm[c * rows : (c + 1) * rows, :]
        acc = acc + (dot_tn(hi, p) + dot_tn(mid, p) + dot_tn(low, p))
    log_ref[...] = acc[:2, :]
    a_mix(3, fwd[3])
    out_ref[...] = (macc[...] + dot(back(3), mm[3 * rows :, :])).astype(BF)
    with jax.named_scope("drain"):
        for cond, copy in pending:
            when(cond, copy.wait_send)
    for stage in range(3):
        @pl.when((z >= stage) & has_up)
        def _():
            for c in range(NC):
                for n in range(2):
                    z_copies[stage, c][n].wait_send()


def tables(tok, n_sp, hd):
    inv = ROTARY_BASE ** (-np.arange(0, hd, 2, dtype=np.float64) / hd)
    inv = np.concatenate([inv, inv]).astype(np.float32).astype(np.float64)
    nj = tok // WIDEST
    c, i, j = np.meshgrid(np.arange(NC), np.arange(NI), np.arange(nj), indexing="ij")
    off = (WIDEST * j + c + NC * i).reshape(-1).astype(np.float64)
    base = np.arange(n_sp, dtype=np.float64) * tok
    out = []
    for p in (off, base):
        a = p[:, None] * inv[None, :]
        out += [np.cos(a).astype(np.float32), np.sin(a).astype(np.float32)]
    return out


def local(n_tp, n_sp, hidden, norm_gain, w_query, w_key, w_value, query_gain, key_gain, w_out):
    tok, width = hidden.shape
    heads, hd = query_gain.shape
    rows = tok // NC
    nj = tok // WIDEST
    cj = 2 * nj
    keys = cj + KEYS_BEHIND
    w4 = cj + KEYS_BEHIND // NI
    tabc, tabs, basec, bases = tables(tok, n_sp, hd)
    dma = pltpu.SemaphoreType.DMA
    vm = pltpu.VMEM
    scratch = [
        vm((tok, width), BF),
        vm((n_tp * width // hd, hd), BF),
        vm((n_tp, 1, width), F32),
        vm((heads, hd), F32), vm((heads, hd), F32),
        vm((1, 1, hd), F32), vm((1, 1, hd), F32),
        vm((n_tp, tok, width), BF),
        vm((n_tp * width, 6 * hd), BF),
        vm((tok, hd), F32), vm((tok, hd), F32),
        vm((n_tp * heads * hd, width), BF),
        vm((3, WIDEST, nj, hd), F32),
        vm((3, WIDEST, cj, hd), F32),
        vm((WIDEST, cj, hd), BF),
        vm((2, WIDEST, keys, hd), BF),
        vm((WIDEST * 16, WIDEST * 32), F32), vm((WIDEST * 16, WIDEST * 32), F32),
        vm((NI * cj, NI * w4), F32),
        vm((cj, keys), F32),
        vm((WIDEST, cj, hd), F32), vm((WIDEST, cj, hd), F32), vm((WIDEST, cj, hd), F32),
        vm((WIDEST, cj, hd), F32), vm((WIDEST, cj, hd), F32), vm((WIDEST, cj, hd), F32),
        vm((NC, NI, cj, hd), F32),
        vm((NC, NI, cj, hd), F32),
        vm((NC, rows, hd), BF),
        vm((n_tp, NC, 2, rows, hd), BF),
        vm((2, NC, NI, nj, hd), F32),
        vm((tok, width), BF),
        vm((tok, width), F32),
        dma((15,)),
        dma((NC, 2)), dma((NC, 2)), dma((NC, 2)), dma((NC, 2)),
        dma((NC,)), dma((NC,)),
        dma((3, NC, 2)), dma((3, NC, 2)),
        dma((1,)), dma((1,)),
        dma((NC,)), dma((NC,)), dma((NC,)), dma((NC,)),
        dma((NC, 2, 2)), dma((NC, 2, 2)), dma((NC - 1, 2)), dma((NC - 1, 2)), dma((2,)), dma((2,)),
    ]
    hbm = pl.BlockSpec(memory_space=pltpu.HBM)
    vmem = pl.BlockSpec(memory_space=pltpu.VMEM)
    early_hx, early_wc = pl.pallas_call(
        functools.partial(early_kernel, n_tp),
        out_shape=(
            jax.ShapeDtypeStruct((n_tp, tok, width), BF),
            jax.ShapeDtypeStruct((n_tp * heads * hd, width), BF),
        ),
        in_specs=[hbm] * 2,
        out_specs=(hbm, hbm),
        scratch_shapes=[
            vm((tok, width), BF), vm((n_tp, tok, width), BF), vm((n_tp * heads * hd, width), BF),
            vm((2, heads * hd // 2, width), BF),
            dma((2,)), dma((2, 2)), dma((2, 2)), dma((2, 2)), dma((2, 2)), dma((6,)), dma((6,)), dma((2,)),
        ],
        compiler_params=pltpu.CompilerParams(
            collective_id=1, has_side_effects=True, vmem_limit_bytes=63 * 1024 * 1024
        ),
    )(hidden, w_out)
    mixed, logs = pl.pallas_call(
        functools.partial(kernel, n_tp, n_sp),
        out_shape=(
            pltpu.VMEM((tok, width), BF),
            pltpu.VMEM((heads, tok), F32),
        ),
        in_specs=[hbm] * 13,
        out_specs=(vmem, vmem),
        scratch_shapes=scratch,
        compiler_params=pltpu.CompilerParams(
            collective_id=0, has_side_effects=True, vmem_limit_bytes=63 * 1024 * 1024
        ),
    )(
        early_hx, early_wc, hidden, norm_gain.reshape(n_tp * width // hd, hd), w_query, w_key, w_value,
        query_gain, key_gain,
        jnp.asarray(tabc), jnp.asarray(tabs), jnp.asarray(basec)[:, None], jnp.asarray(bases)[:, None],
    )
    return mixed, logs.T


def solution(mesh):
    placed = (
        P(("grp", "sp"), "tp"),
        P(),
        P(None, "tp"),
        P(None, "tp"),
        P(None, "tp"),
        P("tp", None),
        P("tp", None),
        P("tp", None),
    )
    return jax.shard_map(
        functools.partial(local, mesh.shape["tp"], mesh.shape["sp"]),
        mesh=mesh,
        in_specs=placed,
        out_specs=(P(("grp", "sp"), "tp"), P(("grp", "sp"), "tp")),
        check_vma=False,
    )
```

```python
import functools

import jax
import jax.numpy as jnp
import numpy as np
from jax import lax
from jax.experimental import pallas as pl
from jax.experimental.pallas import tpu as pltpu
from jax.sharding import PartitionSpec as P

KEYS_BEHIND = 128
MIDDLE = 4
WIDEST = 16
EPSILON = 1e-06
ROTARY_BASE = 500000.0
NEG = -1e30

NC = MIDDLE
NI = WIDEST // MIDDLE
BF = jnp.bfloat16
F32 = jnp.float32
MESH = pl.DeviceIdType.MESH


def dot(a, b):
    return jnp.dot(a, b, preferred_element_type=F32)


def dot_nt(a, b):
    return lax.dot_general(a, b, (((1,), (1,)), ((), ())), preferred_element_type=F32)


def dot_tn(a, b):
    return lax.dot_general(a, b, (((0,), (0,)), ((), ())), preferred_element_type=F32)


def iota(shape, dim):
    return lax.broadcasted_iota(jnp.int32, shape, dim)


def early_kernel(
    n_tp, hid_h, wo_h, hx_out, wc_out,
    hid_v, hx, wcol, relay, lsem, xs_own, xr_own, xs_fwd, xr_fwd, ws, wr, osem,
):
    tok, width = hid_v.shape
    half = tok // 2
    wo_rows = wo_h.shape[0]
    me = lax.axis_index("tp")
    lf = lax.rem(me + n_tp - 1, n_tp)
    rt = lax.rem(me + 1, n_tp)
    op = lax.rem(me + 2, n_tp)

    def remote(src, dst, ssem, rsem, to):
        return pltpu.make_async_remote_copy(
            src_ref=src, dst_ref=dst, send_sem=ssem, recv_sem=rsem,
            device_id={"tp": to}, device_id_type=MESH,
        )

    def rows_of(ref, dev):
        return ref.at[pl.ds(pl.multiple_of(dev * wo_rows, wo_rows), wo_rows), :]

    def cols_of(dev):
        return wo_h.at[:, pl.ds(pl.multiple_of(dev * width, width), width)]

    @pl.when(lax.rem(lax.axis_index("sp"), 2) == 1)
    def _():
        c_hid = pltpu.make_async_copy(hid_h, hid_v, lsem.at[0])
        c_hid.start()
        barrier = pltpu.get_barrier_semaphore()
        for dev in (rt, lf, op):
            pl.semaphore_signal(barrier, inc=1, device_id={"tp": dev}, device_id_type=MESH)
        c_wo = pltpu.make_async_copy(cols_of(me), rows_of(wcol, me), lsem.at[1])
        c_wo.start()
        perm = placement(tok)
        c_hid.wait()
        hx[me] = dot(perm, hid_v[...]).astype(BF)
        pl.semaphore_wait(barrier, n_tp - 1)
        own, fwd = [], []
        for h in range(2):
            part = hx.at[me, pl.ds(h * half, half), :]
            own.append(remote(part, part, xs_own.at[h, 0], xr_own.at[h, 0], rt))
            own.append(remote(part, part, xs_own.at[h, 1], xr_own.at[h, 1], lf))
        for copy in own:
            copy.start()
        out = [remote(cols_of(dev), rows_of(wcol, me), ws.at[n], wr.at[n], dev) for n, dev in enumerate((rt, lf))]
        wh = wo_rows // 2
        turn, relayed = [], []
        for n, (dev, src) in enumerate(((rt, lf), (lf, rt))):
            part = wo_h.at[pl.ds(n * wh, wh), pl.ds(pl.multiple_of(op * width, width), width)]
            turn.append(remote(part, relay.at[n], ws.at[2 + n], wr.at[2 + n], dev))
            to = wcol.at[pl.ds(pl.multiple_of(src * wo_rows + n * wh, wh), wh), :]
            relayed.append(remote(relay.at[n], to, ws.at[4 + n], wr.at[4 + n], dev))
        for h in range(2):
            lo = pl.ds(h * half, half // 2)
            hi = pl.ds(h * half + half // 2, half // 2)
            own[2 * h].wait_recv()
            fwd.append(remote(hx.at[lf, lo, :], hx.at[lf, lo, :], xs_fwd.at[h, 0], xr_fwd.at[h, 0], rt))
            fwd[-1].start()
            own[2 * h + 1].wait_recv()
            fwd.append(remote(hx.at[rt, hi, :], hx.at[rt, hi, :], xs_fwd.at[h, 1], xr_fwd.at[h, 1], lf))
            fwd[-1].start()
        for copy in turn + out:
            copy.start()
        for n in range(2):
            turn[n].wait_recv()
            relayed[n].start()
        out = out + relayed
        for copy in fwd:
            copy.wait_recv()
        o_hx = pltpu.make_async_copy(hx, hx_out, osem.at[0])
        o_hx.start()
        c_wo.wait()
        for copy in out:
            copy.wait_recv()
        o_wc = pltpu.make_async_copy(wcol, wc_out, osem.at[1])
        o_wc.start()
        for copy in own + fwd + turn + out:
            copy.wait_send()
        o_hx.wait()
        o_wc.wait()


def placement(tok):
    prow = iota((tok, tok), 0)
    pcol = iota((tok, tok), 1)
    place = (pcol & (NC - 1)) * (tok // NC) + ((pcol >> 2) & (NI - 1)) * (tok // WIDEST) + (pcol >> 4)
    return jnp.where(prow == place, 1.0, 0.0).astype(BF)


def kernel(
    n_tp, n_sp, hxe_h, wce_h,
    hid_h, ng_h, wq_h, wk_h, wv_h, qg_h, kg_h, tabc_h, tabs_h, basec_h, bases_h,
    out_ref, log_ref,
    hid_v, ng_v, ngain, qg_ref, kg_ref, basec, bases, hx, w_v, tabc, tabs, wcol, sbuf, fbuf, qb, kv, bias1, bias1e, bias4, bias16,
    o1, o4, o16, e1, e4, e16, attb, attl, attx, ag, lt, mm, macc,
    lsem, xs_own, xr_own, xs_fwd, xr_fwd, ds_q, dr_q, zs, zr, ws, wr,
    ds_a, dr_a, ds_l, dr_l, as_own, ar_own, as_fwd, ar_fwd, as_op, ar_op,
):
    tok, width = hid_v.shape
    rows = tok // NC
    half = rows // 2
    nj = tok // WIDEST
    cj = 2 * nj
    hd = KEYS_BEHIND
    depth = n_tp * width
    own0 = kv.shape[2] - cj
    n_near = own0 - cj
    n_far = n_near - cj
    last = n_far

    me = lax.axis_index("tp")
    sp = lax.axis_index("sp")
    core = lax.rem(sp, 2)
    other = 1 - core
    z = lax.div(sp, 2)
    lf = lax.rem(me + n_tp - 1, n_tp)
    rt = lax.rem(me + 1, n_tp)
    op = lax.rem(me + 2, n_tp)
    partner = sp + 1 - 2 * core
    up = lax.rem(sp + 2, n_sp)
    down = lax.rem(sp + n_sp - 2, n_sp)
    to_rt, to_lf, to_op = {"tp": rt}, {"tp": lf}, {"tp": op}
    to_partner, to_up, to_down = {"sp": partner}, {"sp": up}, {"sp": down}
    joff = pl.multiple_of(core * nj, 8)
    poff = pl.multiple_of(other * nj, 8)

    first, second = core == 0, core == 1
    pending = []

    def when(cond, f):
        if cond is None:
            f()
        else:
            pl.when(cond)(f)

    def send(src, dst, ssem, rsem, dev, cond=None):
        copy = pltpu.make_async_remote_copy(
            src_ref=src, dst_ref=dst, send_sem=ssem, recv_sem=rsem, device_id=dev, device_id_type=MESH
        )
        when(cond, copy.start)
        pending.append((cond, copy))
        return copy

    def load(src, dst, k):
        copy = pltpu.make_async_copy(src, dst, lsem.at[k])
        copy.start()
        return copy

    c_hid = pltpu.make_async_copy(hid_h, hid_v, lsem.at[0])
    c_hx = pltpu.make_async_copy(hxe_h, hx, lsem.at[0])
    c_wc = pltpu.make_async_copy(wce_h, wcol, lsem.at[9])
    barrier = pltpu.get_barrier_semaphore()
    peers = [
        to_rt, to_lf, to_op, to_partner,
        {"tp": rt, "sp": partner}, {"tp": lf, "sp": partner}, {"tp": op, "sp": partner},
    ]
    for dev in peers:
        pl.semaphore_signal(barrier, inc=1, device_id=dev, device_id_type=MESH)
    has_up, has_down = z < n_sp // 2 - 1, z > 0

    @pl.when(has_down)
    def _():
        pl.semaphore_signal(barrier, inc=1, device_id=to_down, device_id_type=MESH)

    when(first, c_hid.start)
    when(second, c_hx.start)
    own_col = pl.ds(pl.multiple_of(core * hd, hd), hd)
    oth_col = pl.ds(pl.multiple_of(other * hd, hd), hd)
    c_w = []
    for n, w in enumerate((wq_h, wk_h, wv_h)):
        c_w.append(load(w.at[:, own_col], w_v.at[:, pl.ds(n * hd, hd)], 1 + 2 * n))
        c_w.append(load(w.at[:, oth_col], w_v.at[:, pl.ds((3 + n) * hd, hd)], 2 + 2 * n))
    c_t = [load(tabc_h, tabc, 7), load(tabs_h, tabs, 8)]
    for n, (src, dst) in enumerate(
        ((ng_h, ng_v), (qg_h, qg_ref), (kg_h, kg_ref), (basec_h.at[pl.ds(sp, 1)], basec), (bases_h.at[pl.ds(sp, 1)], bases))
    ):
        c_t.append(load(src, dst, 10 + n))
    when(second, c_wc.start)

    perm = placement(tok)

    @pl.when(first)
    def _():
        with jax.named_scope("hid_wait"):
            c_hid.wait()
        hx[me] = dot(perm, hid_v[...]).astype(BF)

    with jax.named_scope("barrier_wait"):
        pl.semaphore_wait(barrier, len(peers) + has_up.astype(jnp.int32))

    def x_own(c):
        part = hx.at[me, pl.ds(c * rows, rows), :]
        return (
            send(part, part, xs_own.at[c, 0], xr_own.at[c, 0], to_rt, first),
            send(part, part, xs_own.at[c, 1], xr_own.at[c, 1], to_lf, first),
        )

    x_sent = {c: x_own(c) for c in range(NC)}

    for stage, (lo, hi) in enumerate(((n_near, own0), (n_far, n_near), (0, n_far))):
        @pl.when(z <= stage)
        def _():
            kv[:, :, lo:hi, :] = jnp.zeros((2, WIDEST, hi - lo, hd), BF)

    for c in c_t:
        c.wait()
    bc, bs = basec[0], bases[0]
    oc, os_ = tabc[...], tabs[...]
    sign = jnp.where(iota((1, hd), 1) < hd // 2, -1.0, 1.0)
    tabc[...] = bc * oc - bs * os_
    tabs[...] = (bs * oc + bc * os_) * sign

    gains = ng_v[...].astype(F32)
    for s in range(n_tp):
        for k in range(width // hd):
            r = s * (width // hd) + k
            ngain[s, :, k * hd : (k + 1) * hd] = gains[r : r + 1, :]
    first_j = own0 - cj * z
    jq = iota((cj, own0 + cj), 0)
    jk = iota((cj, own0 + cj), 1)
    ok = (jk >= jq) & (jk <= jq + KEYS_BEHIND) & (jk >= first_j)
    bias16[...] = jnp.where(ok, 0.0, NEG)
    w4 = bias4.shape[1] // NI
    row = iota(bias4.shape, 0)
    col = iota(bias4.shape, 1)
    iq = (row * (65536 // cj + 1)) >> 16
    ik = (col * (65536 // w4 + 1)) >> 16
    j4 = own0 + cj - w4
    jk = j4 + col - ik * w4
    dist = NI * (own0 + (row - iq * cj) - jk) + iq - ik
    ok = (dist >= 0) & (dist <= KEYS_BEHIND) & (jk >= first_j)
    bias4[...] = jnp.where(ok, 0.0, NEG)
    row = iota(bias1.shape, 0)
    col = iota(bias1.shape, 1)
    uq = row >> 4
    uk = col >> 5
    rq = (uq >> 2) + NC * (uq & (NI - 1))
    rk = (uk >> 2) + NC * (uk & (NI - 1))
    dist = WIDEST * ((row & 15) + 16 - (col & 31)) + rq - rk
    ok = (dist >= 0) & (dist <= KEYS_BEHIND)
    bias1[...] = jnp.where(ok, 0.0, NEG)
    bias1e[...] = jnp.where(ok & ((col & 31) + own0 - 16 >= first_j), 0.0, NEG)

    @jax.named_scope('partial')
    def partial(c, s, acc, sq):
        h = hx[s, c * rows : (c + 1) * rows, :].astype(F32)
        sc = (h * ngain[s]).astype(BF)
        sq = sq + jnp.sum(h * h, axis=1, keepdims=True)
        acc = acc + dot(sc, w_v[pl.ds(pl.multiple_of(s * width, width), width), :])
        return acc, sq

    def head_rows(x, gain, cos, sin):
        x = x * lax.rsqrt(jnp.mean(x * x, axis=1, keepdims=True) + EPSILON) * gain
        return x * cos + pltpu.roll(x, hd // 2, 1) * sin

    @jax.named_scope('epilogue')
    def epilogue(c, acc, sq):
        rs = lax.rsqrt(sq / depth + EPSILON)
        cos = tabc[c * rows : (c + 1) * rows, :]
        sin = tabs[c * rows : (c + 1) * rows, :]
        parts = []
        for side, hidx in ((1, other), (0, core)):
            x = [acc[:, (3 * side + n) * hd : (3 * side + n + 1) * hd] * rs for n in range(3)]
            q = head_rows(x[0], qg_ref[pl.ds(hidx, 1), :], cos, sin)
            k = head_rows(x[1], kg_ref[pl.ds(hidx, 1), :], cos, sin)
            parts = [v.reshape(NI, nj, hd) for v in (q, k, x[2])]
            for n in range(3):
                if side == 1:
                    sbuf[n, c * NI : (c + 1) * NI, :, :] = parts[n]
                else:
                    fbuf[n, c * NI : (c + 1) * NI, pl.ds(joff, nj), :] = parts[n]
        return send(
            sbuf.at[:, pl.ds(c * NI, NI), :, :],
            fbuf.at[:, pl.ds(c * NI, NI), pl.ds(joff, nj), :],
            ds_q.at[c], dr_q.at[c], to_partner,
        )

    z_copies = {}
    for stage, (start, count, to) in enumerate(
        ((own0, cj, n_near), (n_near, cj, n_far), (n_far + cj - last, last, 0))
    ):
        for c in range(NC):
            u = pl.ds(c * NI, NI)
            z_copies[stage, c] = [
                pltpu.make_async_remote_copy(
                    src_ref=kv.at[n, u, pl.ds(start, count), :], dst_ref=kv.at[n, u, pl.ds(to, count), :],
                    send_sem=zs.at[stage, c, n], recv_sem=zr.at[stage, c, n],
                    device_id=to_up, device_id_type=MESH,
                )
                for n in range(2)
            ]

    def z_send(stage, c, n):
        when((z >= stage) & has_up, z_copies[stage, c][n].start)

    @jax.named_scope('z_wait')
    def z_wait(stage, c):
        for n in range(2):
            when(z > stage, z_copies[stage, c][n].wait_recv)

    @jax.named_scope('z_pass')
    def z_pass(stage, c):
        for n in range(2):
            when(z > stage, z_copies[stage, c][n].wait_recv)
            z_send(stage + 1, c, n)

    @jax.named_scope('own_pair')
    def own_pair(c, copy):
        with jax.named_scope("pair_wait"):
            copy.wait_recv()
        u = slice(c * NI, (c + 1) * NI)
        for n in range(2):
            kv[n, u, own0:, :] = fbuf[1 + n, u].astype(BF)
            z_send(0, c, n)
        qb[u] = fbuf[0, u].astype(BF)

    for c in c_w:
        c.wait()
    def x_pass(c):
        right, left = x_sent[c]
        with jax.named_scope("x_wait"):
            when(first, right.wait_recv)
        h0 = hx.at[lf, pl.ds(c * rows, half), :]
        f0 = send(h0, h0, xs_fwd.at[c, 0], xr_fwd.at[c, 0], to_rt, first)
        with jax.named_scope("x_wait"):
            when(first, left.wait_recv)
        h1 = hx.at[rt, pl.ds(c * rows + half, half), :]
        f1 = send(h1, h1, xs_fwd.at[c, 1], xr_fwd.at[c, 1], to_lf, first)
        return f0, f1

    def x_near(c, passed):
        acc = jnp.zeros((rows, 6 * hd), F32)
        sq = jnp.zeros((rows, 1), F32)
        for s in (me, lf, rt):
            acc, sq = partial(c, s, acc, sq)
        return acc, sq, *passed

    def x_end(c, state):
        acc, sq, f0, f1 = state
        with jax.named_scope("xf_wait"):
            when(first, f0.wait_recv)
            when(first, f1.wait_recv)
        acc, sq = partial(c, op, acc, sq)
        return epilogue(c, acc, sq)

    with jax.named_scope("hx_wait"):
        when(second, c_hx.wait)
    def softmax(s, bias):
        s = s * (hd ** -0.5) + bias
        m = jnp.max(s, axis=1, keepdims=True)
        w = jnp.exp(s - m)
        l = jnp.sum(w, axis=1, keepdims=True)
        return w.astype(BF), m, l

    def wide(x):
        return jnp.broadcast_to(x, (x.shape[0], hd))

    @jax.named_scope('branch1')
    def branch1(b):
        q = qb[:, 16 * b : 16 * b + 16, :].reshape(WIDEST * 16, hd)
        lo = own0 - 16 + 16 * b
        k = kv[0, :, lo : lo + 32, :].reshape(WIDEST * 32, hd)
        v = kv[1, :, lo : lo + 32, :].reshape(WIDEST * 32, hd)
        w, m, l = softmax(dot_nt(q, k), (bias1e if b == 0 else bias1)[...])
        o1[:, 16 * b : 16 * b + 16, :] = (dot(w, v) / l).reshape(WIDEST, 16, hd)
        e1[:, 16 * b : 16 * b + 16, :] = wide(m + jnp.log(l)).reshape(WIDEST, 16, hd)

    @jax.named_scope('branch4')
    def branch4(c):
        u = slice(c * NI, (c + 1) * NI)
        q = qb[u].reshape(NI * cj, hd)
        k = kv[0, u, j4:, :].reshape(NI * w4, hd)
        v = kv[1, u, j4:, :].reshape(NI * w4, hd)
        w, m, l = softmax(dot_nt(q, k), bias4[...])
        o4[u] = (dot(w, v) / l).reshape(NI, cj, hd)
        e4[u] = wide(m + jnp.log(l)).reshape(NI, cj, hd)

    @jax.named_scope('branch16')
    def branch16(c):
        us = range(c * NI, (c + 1) * NI)
        s = jnp.concatenate([dot_nt(qb[u], kv[0, u]) for u in us], axis=0)
        w, m, l = softmax(s, jnp.concatenate([bias16[...]] * NI, axis=0))
        e16[c * NI : (c + 1) * NI] = wide(m + jnp.log(l)).reshape(NI, cj, hd)
        for n, u in enumerate(us):
            part = slice(n * cj, (n + 1) * cj)
            o16[u] = dot(w[part], kv[1, u]) / l[part]

    @jax.named_scope('finish')
    def finish(c):
        u = slice(c * NI, (c + 1) * NI)
        a, b, d = e1[u], e4[u], e16[u]
        top = jnp.maximum(jnp.maximum(a, b), d)
        total = top + jnp.log(jnp.exp(a - top) + jnp.exp(b - top) + jnp.exp(d - top))
        att = jnp.exp(a - total) * o1[u] + jnp.exp(b - total) * o4[u] + jnp.exp(d - total) * o16[u]
        attb[c] = att
        attl[c] = total
        attx[c] = attb[c, :, pl.ds(poff, nj), :].reshape(rows, hd).astype(BF)
        ag[me, c, core] = attb[c, :, pl.ds(joff, nj), :].reshape(rows, hd).astype(BF)
        lt[core, c] = attl[c, :, pl.ds(joff, nj), :]
        for copy in plans[c]:
            copy.start()

    def finish_plan(c):
        same, cross = ag.at[me, c, core], attx.at[c]
        copies = []

        def add(src, dst, ssem, rsem, dev):
            copies.append(
                pltpu.make_async_remote_copy(
                    src_ref=src, dst_ref=dst, send_sem=ssem, recv_sem=rsem, device_id=dev, device_id_type=MESH
                )
            )
            pending.append((None, copies[-1]))

        for side, dev in ((0, rt), (1, lf)):
            add(same, same, as_own.at[c, side, 0], ar_own.at[c, side, core], {"tp": dev})
            add(cross, same, as_own.at[c, side, 1], ar_own.at[c, side, core], {"tp": dev, "sp": partner})
        if c == NC - 1:
            add(same, same, as_op.at[0], ar_op.at[core], to_op)
            add(cross, same, as_op.at[1], ar_op.at[core], {"tp": op, "sp": partner})
        add(cross, same, ds_a.at[c], dr_a.at[c], to_partner)
        add(attl.at[c, :, pl.ds(poff, nj), :], lt.at[core, c], ds_l.at[c], dr_l.at[c], to_partner)
        return copies

    def arrived(ref, sem):
        pltpu.make_async_remote_copy(
            src_ref=ref, dst_ref=ref, send_sem=sem, recv_sem=sem, device_id=to_partner, device_id_type=MESH
        ).wait_recv()

    def a_plan(c):
        p0, p1 = ag.at[lf, c, 0], ag.at[rt, c, 1]
        f0 = pltpu.make_async_remote_copy(
            src_ref=p0, dst_ref=p0, send_sem=as_fwd.at[c, 0], recv_sem=ar_fwd.at[c, 0],
            device_id=to_rt, device_id_type=MESH,
        )
        f1 = pltpu.make_async_remote_copy(
            src_ref=p1, dst_ref=p1, send_sem=as_fwd.at[c, 1], recv_sem=ar_fwd.at[c, 1],
            device_id=to_lf, device_id_type=MESH,
        )
        pending.extend([(None, f0), (None, f1)])
        return f0, f1

    @jax.named_scope('a_fwd')
    def a_fwd(c, copies):
        arrived(ag.at[lf, c, 0], ar_own.at[c, 0, 0])
        copies[0].start()
        arrived(ag.at[rt, c, 1], ar_own.at[c, 1, 1])
        copies[1].start()

    @jax.named_scope('a_mix')
    def a_mix(c, copies):
        with jax.named_scope("af_wait"):
            arrived(ag.at[lf, c, 1], ar_own.at[c, 0, 1])
            arrived(ag.at[rt, c, 0], ar_own.at[c, 1, 0])
            arrived(ag.at[me, c, other], dr_a.at[c])
            if c < NC - 1:
                for f in copies:
                    f.wait_recv()
            else:
                arrived(ag.at[lf, c, 0], ar_own.at[c, 0, 0])
                arrived(ag.at[rt, c, 1], ar_own.at[c, 1, 1])
                for h in range(2):
                    arrived(ag.at[op, c, h], ar_op.at[h])
        lhs = jnp.concatenate([ag[s, c, h] for s in range(n_tp) for h in range(2)], axis=1)
        mm[c * rows : (c + 1) * rows, :] = dot(lhs, wcol[...]).astype(BF)

    t0 = iota((tok, rows), 0)
    q0 = iota((tok, rows), 1)

    def back(c):
        there = ((t0 & (NC - 1)) == c) & (q0 == ((t0 >> 2) & (NI - 1)) * nj + (t0 >> 4))
        return jnp.where(there, 1.0, 0.0).astype(BF)

    state, pairs = {}, {}
    edge = z == 0

    def early(c):
        @pl.when(edge & first)
        def _():
            branch16(c)
            branch4(c)

    def pair_first(c):
        pl.when(first)(functools.partial(own_pair, c, pairs[c]))

    for c in range(NC):
        state[c] = x_near(c, x_pass(c))
    pairs[0] = x_end(0, state[0])
    pairs[1] = x_end(1, state[1])
    pair_first(0)
    pairs[2] = x_end(2, state[2])
    pair_first(1)
    pairs[3] = x_end(3, state[3])
    pair_first(2)
    when(second, c_wc.wait)
    c_w = send(wcol, wcol, ws.at[0], wr.at[0], to_partner, second)
    early(0)
    for c in range(3):
        pl.when(second)(functools.partial(own_pair, c, pairs[c]))

    pl.when(edge & second)(functools.partial(branch4, 0))
    own_pair(3, pairs[3])
    for b in range(1, cj // 16):
        branch1(b)
    plans = [finish_plan(c) for c in range(NC)]
    fwd = {c: a_plan(c) for c in range(NC - 1)}
    for c in range(3):
        z_pass(0, c)
        pl.when(~edge)(functools.partial(branch4, c))
        pl.when(z == 1)(functools.partial(branch16, c))
    z_pass(0, 3)
    branch1(0)
    pl.when(z >= 2)(functools.partial(branch4, 3))
    for c in range(NC):
        z_pass(1, c)

        @pl.when(z == 2)
        def _():
            branch16(c)
            finish(c)

    @pl.when(z != 2)
    def _():
        for c in range(NC):
            z_wait(2, c)

            @pl.when((z > 2) | (edge & (second | (c > 0))) | (c == 3))
            def _():
                branch16(c)

            if c == 3:
                pl.when(z < 2)(functools.partial(branch4, c))
            elif c > 0:
                pl.when(edge)(functools.partial(branch4, c))
            finish(c)
            if c == 2:
                pl.when(z > 2)(functools.partial(a_fwd, 0, fwd[0]))

    pl.when(z <= 2)(functools.partial(a_fwd, 0, fwd[0]))
    for c in range(1, NC - 1):
        a_fwd(c, fwd[c])
    fwd[NC - 1] = ()
    with jax.named_scope("w_wait"):
        when(first, c_w.wait_recv)
    for c in range(3):
        a_mix(c, fwd[c])
    macc[...] = sum(dot(back(c), mm[c * rows : (c + 1) * rows, :]) for c in range(3))
    for c in range(NC):
        plans[c][-1].wait_recv()
    lane = iota((1, hd), 1)
    acc = jnp.zeros((hd, tok), F32)
    for c in range(NC):
        x = jnp.where(lane == 0, lt[0, c].reshape(rows, hd), lt[1, c].reshape(rows, hd))
        hi = x.astype(BF)
        rest = x - hi.astype(F32)
        mid = rest.astype(BF)
        low = (rest - mid.astype(F32)).astype(BF)
        p = perm[c * rows : (c + 1) * rows, :]
        acc = acc + (dot_tn(hi, p) + dot_tn(mid, p) + dot_tn(low, p))
    log_ref[...] = acc[:2, :]
    a_mix(3, fwd[3])
    out_ref[...] = (macc[...] + dot(back(3), mm[3 * rows :, :])).astype(BF)
    with jax.named_scope("drain"):
        for cond, copy in pending:
            when(cond, copy.wait_send)
    for stage in range(3):
        @pl.when((z >= stage) & has_up)
        def _():
            for c in range(NC):
                for n in range(2):
                    z_copies[stage, c][n].wait_send()


def tables(tok, n_sp, hd):
    inv = ROTARY_BASE ** (-np.arange(0, hd, 2, dtype=np.float64) / hd)
    inv = np.concatenate([inv, inv]).astype(np.float32).astype(np.float64)
    nj = tok // WIDEST
    c, i, j = np.meshgrid(np.arange(NC), np.arange(NI), np.arange(nj), indexing="ij")
    off = (WIDEST * j + c + NC * i).reshape(-1).astype(np.float64)
    base = np.arange(n_sp, dtype=np.float64) * tok
    out = []
    for p in (off, base):
        a = p[:, None] * inv[None, :]
        out += [np.cos(a).astype(np.float32), np.sin(a).astype(np.float32)]
    return out


def local(n_tp, n_sp, hidden, norm_gain, w_query, w_key, w_value, query_gain, key_gain, w_out):
    tok, width = hidden.shape
    heads, hd = query_gain.shape
    rows = tok // NC
    nj = tok // WIDEST
    cj = 2 * nj
    keys = cj + KEYS_BEHIND
    w4 = cj + KEYS_BEHIND // NI
    tabc, tabs, basec, bases = tables(tok, n_sp, hd)
    dma = pltpu.SemaphoreType.DMA
    vm = pltpu.VMEM
    scratch = [
        vm((tok, width), BF),
        vm((n_tp * width // hd, hd), BF),
        vm((n_tp, 1, width), F32),
        vm((heads, hd), F32), vm((heads, hd), F32),
        vm((1, 1, hd), F32), vm((1, 1, hd), F32),
        vm((n_tp, tok, width), BF),
        vm((n_tp * width, 6 * hd), BF),
        vm((tok, hd), F32), vm((tok, hd), F32),
        vm((n_tp * heads * hd, width), BF),
        vm((3, WIDEST, nj, hd), F32),
        vm((3, WIDEST, cj, hd), F32),
        vm((WIDEST, cj, hd), BF),
        vm((2, WIDEST, keys, hd), BF),
        vm((WIDEST * 16, WIDEST * 32), F32), vm((WIDEST * 16, WIDEST * 32), F32),
        vm((NI * cj, NI * w4), F32),
        vm((cj, keys), F32),
        vm((WIDEST, cj, hd), F32), vm((WIDEST, cj, hd), F32), vm((WIDEST, cj, hd), F32),
        vm((WIDEST, cj, hd), F32), vm((WIDEST, cj, hd), F32), vm((WIDEST, cj, hd), F32),
        vm((NC, NI, cj, hd), F32),
        vm((NC, NI, cj, hd), F32),
        vm((NC, rows, hd), BF),
        vm((n_tp, NC, 2, rows, hd), BF),
        vm((2, NC, NI, nj, hd), F32),
        vm((tok, width), BF),
        vm((tok, width), F32),
        dma((15,)),
        dma((NC, 2)), dma((NC, 2)), dma((NC, 2)), dma((NC, 2)),
        dma((NC,)), dma((NC,)),
        dma((3, NC, 2)), dma((3, NC, 2)),
        dma((1,)), dma((1,)),
        dma((NC,)), dma((NC,)), dma((NC,)), dma((NC,)),
        dma((NC, 2, 2)), dma((NC, 2, 2)), dma((NC - 1, 2)), dma((NC - 1, 2)), dma((2,)), dma((2,)),
    ]
    hbm = pl.BlockSpec(memory_space=pltpu.HBM)
    vmem = pl.BlockSpec(memory_space=pltpu.VMEM)
    early_hx, early_wc = pl.pallas_call(
        functools.partial(early_kernel, n_tp),
        out_shape=(
            jax.ShapeDtypeStruct((n_tp, tok, width), BF),
            jax.ShapeDtypeStruct((n_tp * heads * hd, width), BF),
        ),
        in_specs=[hbm] * 2,
        out_specs=(hbm, hbm),
        scratch_shapes=[
            vm((tok, width), BF), vm((n_tp, tok, width), BF), vm((n_tp * heads * hd, width), BF),
            vm((2, heads * hd // 2, width), BF),
            dma((2,)), dma((2, 2)), dma((2, 2)), dma((2, 2)), dma((2, 2)), dma((6,)), dma((6,)), dma((2,)),
        ],
        compiler_params=pltpu.CompilerParams(
            collective_id=1, has_side_effects=True, vmem_limit_bytes=63 * 1024 * 1024
        ),
    )(hidden, w_out)
    mixed, logs = pl.pallas_call(
        functools.partial(kernel, n_tp, n_sp),
        out_shape=(
            pltpu.VMEM((tok, width), BF),
            pltpu.VMEM((heads, tok), F32),
        ),
        in_specs=[hbm] * 13,
        out_specs=(vmem, vmem),
        scratch_shapes=scratch,
        compiler_params=pltpu.CompilerParams(
            collective_id=0, has_side_effects=True, vmem_limit_bytes=63 * 1024 * 1024
        ),
    )(
        early_hx, early_wc, hidden, norm_gain.reshape(n_tp * width // hd, hd), w_query, w_key, w_value,
        query_gain, key_gain,
        jnp.asarray(tabc), jnp.asarray(tabs), jnp.asarray(basec)[:, None], jnp.asarray(bases)[:, None],
    )
    return mixed, logs.T


def solution(mesh):
    placed = (
        P(("grp", "sp"), "tp"),
        P(),
        P(None, "tp"),
        P(None, "tp"),
        P(None, "tp"),
        P("tp", None),
        P("tp", None),
        P("tp", None),
    )
    return jax.shard_map(
        functools.partial(local, mesh.shape["tp"], mesh.shape["sp"]),
        mesh=mesh,
        in_specs=placed,
        out_specs=(P(("grp", "sp"), "tp"), P(("grp", "sp"), "tp")),
        check_vma=False,
    )
```

```python
import functools

import jax
import jax.numpy as jnp
import numpy as np
from jax import lax
from jax.experimental import pallas as pl
from jax.experimental.pallas import tpu as pltpu
from jax.sharding import PartitionSpec as P

KEYS_BEHIND = 128
MIDDLE = 4
WIDEST = 16
EPSILON = 1e-06
ROTARY_BASE = 500000.0
NEG = -1e30

NC = MIDDLE
NI = WIDEST // MIDDLE
BF = jnp.bfloat16
F32 = jnp.float32
MESH = pl.DeviceIdType.MESH


def dot(a, b):
    return jnp.dot(a, b, preferred_element_type=F32)


def dot_nt(a, b):
    return lax.dot_general(a, b, (((1,), (1,)), ((), ())), preferred_element_type=F32)


def dot_tn(a, b):
    return lax.dot_general(a, b, (((0,), (0,)), ((), ())), preferred_element_type=F32)


def iota(shape, dim):
    return lax.broadcasted_iota(jnp.int32, shape, dim)


def early_kernel(
    n_tp, hid_h, wo_h, hx_out, wc_out,
    hid_v, hx, wcol, relay, lsem, xs_own, xr_own, xs_fwd, xr_fwd, ws, wr, osem,
):
    tok, width = hid_v.shape
    half = tok // 2
    wo_rows = wo_h.shape[0]
    me = lax.axis_index("tp")
    lf = lax.rem(me + n_tp - 1, n_tp)
    rt = lax.rem(me + 1, n_tp)
    op = lax.rem(me + 2, n_tp)

    def remote(src, dst, ssem, rsem, to):
        return pltpu.make_async_remote_copy(
            src_ref=src, dst_ref=dst, send_sem=ssem, recv_sem=rsem,
            device_id={"tp": to}, device_id_type=MESH,
        )

    def rows_of(ref, dev):
        return ref.at[pl.ds(pl.multiple_of(dev * wo_rows, wo_rows), wo_rows), :]

    def cols_of(dev):
        return wo_h.at[:, pl.ds(pl.multiple_of(dev * width, width), width)]

    @pl.when(lax.rem(lax.axis_index("sp"), 2) == 1)
    def _():
        c_hid = pltpu.make_async_copy(hid_h, hid_v, lsem.at[0])
        c_hid.start()
        barrier = pltpu.get_barrier_semaphore()
        for dev in (rt, lf, op):
            pl.semaphore_signal(barrier, inc=1, device_id={"tp": dev}, device_id_type=MESH)
        c_wo = pltpu.make_async_copy(cols_of(me), rows_of(wcol, me), lsem.at[1])
        c_wo.start()
        perm = placement(tok)
        c_hid.wait()
        hx[me] = dot(perm, hid_v[...]).astype(BF)
        pl.semaphore_wait(barrier, n_tp - 1)
        own, fwd = [], []
        for h in range(2):
            part = hx.at[me, pl.ds(h * half, half), :]
            own.append(remote(part, part, xs_own.at[h, 0], xr_own.at[h, 0], rt))
            own.append(remote(part, part, xs_own.at[h, 1], xr_own.at[h, 1], lf))
        for copy in own:
            copy.start()
        out = [remote(cols_of(dev), rows_of(wcol, me), ws.at[n], wr.at[n], dev) for n, dev in enumerate((rt, lf))]
        wh = wo_rows // 2
        turn, relayed = [], []
        for n, (dev, src) in enumerate(((rt, lf), (lf, rt))):
            part = wo_h.at[pl.ds(n * wh, wh), pl.ds(pl.multiple_of(op * width, width), width)]
            turn.append(remote(part, relay.at[n], ws.at[2 + n], wr.at[2 + n], dev))
            to = wcol.at[pl.ds(pl.multiple_of(src * wo_rows + n * wh, wh), wh), :]
            relayed.append(remote(relay.at[n], to, ws.at[4 + n], wr.at[4 + n], dev))
        for h in range(2):
            lo = pl.ds(h * half, half // 2)
            hi = pl.ds(h * half + half // 2, half // 2)
            own[2 * h].wait_recv()
            fwd.append(remote(hx.at[lf, lo, :], hx.at[lf, lo, :], xs_fwd.at[h, 0], xr_fwd.at[h, 0], rt))
            fwd[-1].start()
            own[2 * h + 1].wait_recv()
            fwd.append(remote(hx.at[rt, hi, :], hx.at[rt, hi, :], xs_fwd.at[h, 1], xr_fwd.at[h, 1], lf))
            fwd[-1].start()
        for copy in turn + out:
            copy.start()
        for n in range(2):
            turn[n].wait_recv()
            relayed[n].start()
        out = out + relayed
        for copy in fwd:
            copy.wait_recv()
        o_hx = pltpu.make_async_copy(hx, hx_out, osem.at[0])
        o_hx.start()
        c_wo.wait()
        for copy in out:
            copy.wait_recv()
        o_wc = pltpu.make_async_copy(wcol, wc_out, osem.at[1])
        o_wc.start()
        for copy in own + fwd + turn + out:
            copy.wait_send()
        o_hx.wait()
        o_wc.wait()


def placement(tok):
    prow = iota((tok, tok), 0)
    pcol = iota((tok, tok), 1)
    place = (pcol & (NC - 1)) * (tok // NC) + ((pcol >> 2) & (NI - 1)) * (tok // WIDEST) + (pcol >> 4)
    return jnp.where(prow == place, 1.0, 0.0).astype(BF)


def kernel(
    n_tp, n_sp, hxe_h, wce_h,
    hid_h, ng_h, wq_h, wk_h, wv_h, qg_h, kg_h, tabc_h, tabs_h, basec_h, bases_h,
    out_ref, log_ref,
    hid_v, ng_v, ngain, qg_ref, kg_ref, basec, bases, hx, w_v, tabc, tabs, wcol, sbuf, fbuf, qb, kv, bias1, bias1e, bias4, bias16,
    o1, o4, o16, e1, e4, e16, attb, attl, attx, ag, lt, mm, macc,
    lsem, xs_own, xr_own, xs_fwd, xr_fwd, ds_q, dr_q, zs, zr, ws, wr,
    ds_a, dr_a, ds_l, dr_l, as_own, ar_own, as_fwd, ar_fwd, as_op, ar_op,
):
    tok, width = hid_v.shape
    rows = tok // NC
    half = rows // 2
    nj = tok // WIDEST
    cj = 2 * nj
    hd = KEYS_BEHIND
    depth = n_tp * width
    own0 = kv.shape[2] - cj
    n_near = own0 - cj
    n_far = n_near - cj
    last = n_far

    me = lax.axis_index("tp")
    sp = lax.axis_index("sp")
    core = lax.rem(sp, 2)
    other = 1 - core
    z = lax.div(sp, 2)
    lf = lax.rem(me + n_tp - 1, n_tp)
    rt = lax.rem(me + 1, n_tp)
    op = lax.rem(me + 2, n_tp)
    partner = sp + 1 - 2 * core
    up = lax.rem(sp + 2, n_sp)
    down = lax.rem(sp + n_sp - 2, n_sp)
    to_rt, to_lf, to_op = {"tp": rt}, {"tp": lf}, {"tp": op}
    to_partner, to_up, to_down = {"sp": partner}, {"sp": up}, {"sp": down}
    joff = pl.multiple_of(core * nj, 8)
    poff = pl.multiple_of(other * nj, 8)

    first, second = core == 0, core == 1
    pending = []

    def when(cond, f):
        if cond is None:
            f()
        else:
            pl.when(cond)(f)

    def send(src, dst, ssem, rsem, dev, cond=None):
        copy = pltpu.make_async_remote_copy(
            src_ref=src, dst_ref=dst, send_sem=ssem, recv_sem=rsem, device_id=dev, device_id_type=MESH
        )
        when(cond, copy.start)
        pending.append((cond, copy))
        return copy

    def load(src, dst, k):
        copy = pltpu.make_async_copy(src, dst, lsem.at[k])
        copy.start()
        return copy

    c_hid = pltpu.make_async_copy(hid_h, hid_v, lsem.at[0])
    c_hx = pltpu.make_async_copy(hxe_h, hx, lsem.at[0])
    c_wc = pltpu.make_async_copy(wce_h, wcol, lsem.at[9])
    barrier = pltpu.get_barrier_semaphore()
    peers = [
        to_rt, to_lf, to_op, to_partner,
        {"tp": rt, "sp": partner}, {"tp": lf, "sp": partner}, {"tp": op, "sp": partner},
    ]
    for dev in peers:
        pl.semaphore_signal(barrier, inc=1, device_id=dev, device_id_type=MESH)
    has_up, has_down = z < n_sp // 2 - 1, z > 0

    @pl.when(has_down)
    def _():
        pl.semaphore_signal(barrier, inc=1, device_id=to_down, device_id_type=MESH)

    when(first, c_hid.start)
    when(second, c_hx.start)
    own_col = pl.ds(pl.multiple_of(core * hd, hd), hd)
    oth_col = pl.ds(pl.multiple_of(other * hd, hd), hd)
    c_w = []
    for n, w in enumerate((wq_h, wk_h, wv_h)):
        c_w.append(load(w.at[:, own_col], w_v.at[:, pl.ds(n * hd, hd)], 1 + 2 * n))
        c_w.append(load(w.at[:, oth_col], w_v.at[:, pl.ds((3 + n) * hd, hd)], 2 + 2 * n))
    c_t = [load(tabc_h, tabc, 7), load(tabs_h, tabs, 8)]
    for n, (src, dst) in enumerate(
        ((ng_h, ng_v), (qg_h, qg_ref), (kg_h, kg_ref), (basec_h.at[pl.ds(sp, 1)], basec), (bases_h.at[pl.ds(sp, 1)], bases))
    ):
        c_t.append(load(src, dst, 10 + n))
    when(second, c_wc.start)

    perm = placement(tok)

    @pl.when(first)
    def _():
        with jax.named_scope("hid_wait"):
            c_hid.wait()
        hx[me] = dot(perm, hid_v[...]).astype(BF)

    with jax.named_scope("barrier_wait"):
        pl.semaphore_wait(barrier, len(peers) + has_up.astype(jnp.int32))

    def x_own(c):
        part = hx.at[me, pl.ds(c * rows, rows), :]
        return (
            send(part, part, xs_own.at[c, 0], xr_own.at[c, 0], to_rt, first),
            send(part, part, xs_own.at[c, 1], xr_own.at[c, 1], to_lf, first),
        )

    x_sent = {c: x_own(c) for c in range(NC)}

    for stage, (lo, hi) in enumerate(((n_near, own0), (n_far, n_near), (0, n_far))):
        @pl.when(z <= stage)
        def _():
            kv[:, :, lo:hi, :] = jnp.zeros((2, WIDEST, hi - lo, hd), BF)

    for c in c_t:
        c.wait()
    bc, bs = basec[0], bases[0]
    oc, os_ = tabc[...], tabs[...]
    sign = jnp.where(iota((1, hd), 1) < hd // 2, -1.0, 1.0)
    tabc[...] = bc * oc - bs * os_
    tabs[...] = (bs * oc + bc * os_) * sign

    gains = ng_v[...].astype(F32)
    for s in range(n_tp):
        for k in range(width // hd):
            r = s * (width // hd) + k
            ngain[s, :, k * hd : (k + 1) * hd] = gains[r : r + 1, :]
    first_j = own0 - cj * z
    jq = iota((cj, own0 + cj), 0)
    jk = iota((cj, own0 + cj), 1)
    ok = (jk >= jq) & (jk <= jq + KEYS_BEHIND) & (jk >= first_j)
    bias16[...] = jnp.where(ok, 0.0, NEG)
    w4 = bias4.shape[1] // NI
    row = iota(bias4.shape, 0)
    col = iota(bias4.shape, 1)
    iq = (row * (65536 // cj + 1)) >> 16
    ik = (col * (65536 // w4 + 1)) >> 16
    j4 = own0 + cj - w4
    jk = j4 + col - ik * w4
    dist = NI * (own0 + (row - iq * cj) - jk) + iq - ik
    ok = (dist >= 0) & (dist <= KEYS_BEHIND) & (jk >= first_j)
    bias4[...] = jnp.where(ok, 0.0, NEG)
    row = iota(bias1.shape, 0)
    col = iota(bias1.shape, 1)
    uq = row >> 4
    uk = col >> 5
    rq = (uq >> 2) + NC * (uq & (NI - 1))
    rk = (uk >> 2) + NC * (uk & (NI - 1))
    dist = WIDEST * ((row & 15) + 16 - (col & 31)) + rq - rk
    ok = (dist >= 0) & (dist <= KEYS_BEHIND)
    bias1[...] = jnp.where(ok, 0.0, NEG)
    bias1e[...] = jnp.where(ok & ((col & 31) + own0 - 16 >= first_j), 0.0, NEG)

    @jax.named_scope('partial')
    def partial(c, s, acc, sq):
        h = hx[s, c * rows : (c + 1) * rows, :].astype(F32)
        sc = (h * ngain[s]).astype(BF)
        sq = sq + jnp.sum(h * h, axis=1, keepdims=True)
        acc = acc + dot(sc, w_v[pl.ds(pl.multiple_of(s * width, width), width), :])
        return acc, sq

    def head_rows(x, gain, cos, sin):
        x = x * lax.rsqrt(jnp.mean(x * x, axis=1, keepdims=True) + EPSILON) * gain
        return x * cos + pltpu.roll(x, hd // 2, 1) * sin

    @jax.named_scope('epilogue')
    def epilogue(c, acc, sq):
        rs = lax.rsqrt(sq / depth + EPSILON)
        cos = tabc[c * rows : (c + 1) * rows, :]
        sin = tabs[c * rows : (c + 1) * rows, :]
        parts = []
        for side, hidx in ((1, other), (0, core)):
            x = [acc[:, (3 * side + n) * hd : (3 * side + n + 1) * hd] * rs for n in range(3)]
            q = head_rows(x[0], qg_ref[pl.ds(hidx, 1), :], cos, sin)
            k = head_rows(x[1], kg_ref[pl.ds(hidx, 1), :], cos, sin)
            parts = [v.reshape(NI, nj, hd) for v in (q, k, x[2])]
            for n in range(3):
                if side == 1:
                    sbuf[n, c * NI : (c + 1) * NI, :, :] = parts[n]
                else:
                    fbuf[n, c * NI : (c + 1) * NI, pl.ds(joff, nj), :] = parts[n]
        return send(
            sbuf.at[:, pl.ds(c * NI, NI), :, :],
            fbuf.at[:, pl.ds(c * NI, NI), pl.ds(joff, nj), :],
            ds_q.at[c], dr_q.at[c], to_partner,
        )

    z_copies = {}
    for stage, (start, count, to) in enumerate(
        ((own0, cj, n_near), (n_near, cj, n_far), (n_far + cj - last, last, 0))
    ):
        for c in range(NC):
            u = pl.ds(c * NI, NI)
            z_copies[stage, c] = [
                pltpu.make_async_remote_copy(
                    src_ref=kv.at[n, u, pl.ds(start, count), :], dst_ref=kv.at[n, u, pl.ds(to, count), :],
                    send_sem=zs.at[stage, c, n], recv_sem=zr.at[stage, c, n],
                    device_id=to_up, device_id_type=MESH,
                )
                for n in range(2)
            ]

    def z_send(stage, c, n):
        when((z >= stage) & has_up, z_copies[stage, c][n].start)

    @jax.named_scope('z_wait')
    def z_wait(stage, c):
        for n in range(2):
            when(z > stage, z_copies[stage, c][n].wait_recv)

    @jax.named_scope('z_pass')
    def z_pass(stage, c):
        for n in range(2):
            when(z > stage, z_copies[stage, c][n].wait_recv)
            z_send(stage + 1, c, n)

    @jax.named_scope('own_pair')
    def own_pair(c, copy):
        with jax.named_scope("pair_wait"):
            copy.wait_recv()
        u = slice(c * NI, (c + 1) * NI)
        for n in range(2):
            kv[n, u, own0:, :] = fbuf[1 + n, u].astype(BF)
            z_send(0, c, n)
        qb[u] = fbuf[0, u].astype(BF)

    for c in c_w:
        c.wait()
    def x_pass(c):
        right, left = x_sent[c]
        with jax.named_scope("x_wait"):
            when(first, right.wait_recv)
        h0 = hx.at[lf, pl.ds(c * rows, half), :]
        f0 = send(h0, h0, xs_fwd.at[c, 0], xr_fwd.at[c, 0], to_rt, first)
        with jax.named_scope("x_wait"):
            when(first, left.wait_recv)
        h1 = hx.at[rt, pl.ds(c * rows + half, half), :]
        f1 = send(h1, h1, xs_fwd.at[c, 1], xr_fwd.at[c, 1], to_lf, first)
        return f0, f1

    def x_near(c, passed):
        acc = jnp.zeros((rows, 6 * hd), F32)
        sq = jnp.zeros((rows, 1), F32)
        for s in (me, lf, rt):
            acc, sq = partial(c, s, acc, sq)
        return acc, sq, *passed

    def x_end(c, state):
        acc, sq, f0, f1 = state
        with jax.named_scope("xf_wait"):
            when(first, f0.wait_recv)
            when(first, f1.wait_recv)
        acc, sq = partial(c, op, acc, sq)
        return epilogue(c, acc, sq)

    with jax.named_scope("hx_wait"):
        when(second, c_hx.wait)
    def softmax(s, bias):
        s = s * (hd ** -0.5) + bias
        m = jnp.max(s, axis=1, keepdims=True)
        w = jnp.exp(s - m)
        l = jnp.sum(w, axis=1, keepdims=True)
        return w.astype(BF), m, l

    def wide(x):
        return jnp.broadcast_to(x, (x.shape[0], hd))

    @jax.named_scope('branch1')
    def branch1(b):
        q = qb[:, 16 * b : 16 * b + 16, :].reshape(WIDEST * 16, hd)
        lo = own0 - 16 + 16 * b
        k = kv[0, :, lo : lo + 32, :].reshape(WIDEST * 32, hd)
        v = kv[1, :, lo : lo + 32, :].reshape(WIDEST * 32, hd)
        w, m, l = softmax(dot_nt(q, k), (bias1e if b == 0 else bias1)[...])
        o1[:, 16 * b : 16 * b + 16, :] = (dot(w, v) / l).reshape(WIDEST, 16, hd)
        e1[:, 16 * b : 16 * b + 16, :] = wide(m + jnp.log(l)).reshape(WIDEST, 16, hd)

    @jax.named_scope('branch4')
    def branch4(c):
        u = slice(c * NI, (c + 1) * NI)
        q = qb[u].reshape(NI * cj, hd)
        k = kv[0, u, j4:, :].reshape(NI * w4, hd)
        v = kv[1, u, j4:, :].reshape(NI * w4, hd)
        w, m, l = softmax(dot_nt(q, k), bias4[...])
        o4[u] = (dot(w, v) / l).reshape(NI, cj, hd)
        e4[u] = wide(m + jnp.log(l)).reshape(NI, cj, hd)

    @jax.named_scope('branch16')
    def branch16(c):
        us = range(c * NI, (c + 1) * NI)
        s = jnp.concatenate([dot_nt(qb[u], kv[0, u]) for u in us], axis=0)
        w, m, l = softmax(s, jnp.concatenate([bias16[...]] * NI, axis=0))
        e16[c * NI : (c + 1) * NI] = wide(m + jnp.log(l)).reshape(NI, cj, hd)
        for n, u in enumerate(us):
            part = slice(n * cj, (n + 1) * cj)
            o16[u] = dot(w[part], kv[1, u]) / l[part]

    @jax.named_scope('finish')
    def finish(c):
        u = slice(c * NI, (c + 1) * NI)
        a, b, d = e1[u], e4[u], e16[u]
        top = jnp.maximum(jnp.maximum(a, b), d)
        total = top + jnp.log(jnp.exp(a - top) + jnp.exp(b - top) + jnp.exp(d - top))
        att = jnp.exp(a - total) * o1[u] + jnp.exp(b - total) * o4[u] + jnp.exp(d - total) * o16[u]
        attb[c] = att
        attl[c] = total
        attx[c] = attb[c, :, pl.ds(poff, nj), :].reshape(rows, hd).astype(BF)
        ag[me, c, core] = attb[c, :, pl.ds(joff, nj), :].reshape(rows, hd).astype(BF)
        lt[core, c] = attl[c, :, pl.ds(joff, nj), :]
        for copy in plans[c]:
            copy.start()

    def finish_plan(c):
        same, cross = ag.at[me, c, core], attx.at[c]
        copies = []

        def add(src, dst, ssem, rsem, dev):
            copies.append(
                pltpu.make_async_remote_copy(
                    src_ref=src, dst_ref=dst, send_sem=ssem, recv_sem=rsem, device_id=dev, device_id_type=MESH
                )
            )
            pending.append((None, copies[-1]))

        for side, dev in ((0, rt), (1, lf)):
            add(same, same, as_own.at[c, side, 0], ar_own.at[c, side, core], {"tp": dev})
            add(cross, same, as_own.at[c, side, 1], ar_own.at[c, side, core], {"tp": dev, "sp": partner})
        if c == NC - 1:
            add(same, same, as_op.at[0], ar_op.at[core], to_op)
            add(cross, same, as_op.at[1], ar_op.at[core], {"tp": op, "sp": partner})
        add(cross, same, ds_a.at[c], dr_a.at[c], to_partner)
        add(attl.at[c, :, pl.ds(poff, nj), :], lt.at[core, c], ds_l.at[c], dr_l.at[c], to_partner)
        return copies

    def arrived(ref, sem):
        pltpu.make_async_remote_copy(
            src_ref=ref, dst_ref=ref, send_sem=sem, recv_sem=sem, device_id=to_partner, device_id_type=MESH
        ).wait_recv()

    def a_plan(c):
        p0, p1 = ag.at[lf, c, 0], ag.at[rt, c, 1]
        f0 = pltpu.make_async_remote_copy(
            src_ref=p0, dst_ref=p0, send_sem=as_fwd.at[c, 0], recv_sem=ar_fwd.at[c, 0],
            device_id=to_rt, device_id_type=MESH,
        )
        f1 = pltpu.make_async_remote_copy(
            src_ref=p1, dst_ref=p1, send_sem=as_fwd.at[c, 1], recv_sem=ar_fwd.at[c, 1],
            device_id=to_lf, device_id_type=MESH,
        )
        pending.extend([(None, f0), (None, f1)])
        return f0, f1

    @jax.named_scope('a_fwd')
    def a_fwd(c, copies):
        arrived(ag.at[lf, c, 0], ar_own.at[c, 0, 0])
        copies[0].start()
        arrived(ag.at[rt, c, 1], ar_own.at[c, 1, 1])
        copies[1].start()

    @jax.named_scope('a_mix')
    def a_mix(c, copies):
        with jax.named_scope("af_wait"):
            arrived(ag.at[lf, c, 1], ar_own.at[c, 0, 1])
            arrived(ag.at[rt, c, 0], ar_own.at[c, 1, 0])
            arrived(ag.at[me, c, other], dr_a.at[c])
            if c < NC - 1:
                for f in copies:
                    f.wait_recv()
            else:
                arrived(ag.at[lf, c, 0], ar_own.at[c, 0, 0])
                arrived(ag.at[rt, c, 1], ar_own.at[c, 1, 1])
                for h in range(2):
                    arrived(ag.at[op, c, h], ar_op.at[h])
        lhs = jnp.concatenate([ag[s, c, h] for s in range(n_tp) for h in range(2)], axis=1)
        mm[c * rows : (c + 1) * rows, :] = dot(lhs, wcol[...]).astype(BF)

    t0 = iota((tok, rows), 0)
    q0 = iota((tok, rows), 1)

    def back(c):
        there = ((t0 & (NC - 1)) == c) & (q0 == ((t0 >> 2) & (NI - 1)) * nj + (t0 >> 4))
        return jnp.where(there, 1.0, 0.0).astype(BF)

    state, pairs = {}, {}
    edge = z == 0

    def early(c):
        @pl.when(edge & first)
        def _():
            branch16(c)
            branch4(c)

    def pair_first(c):
        pl.when(first)(functools.partial(own_pair, c, pairs[c]))

    for c in range(NC):
        state[c] = x_near(c, x_pass(c))
    for c in range(NC):
        pairs[c] = x_end(c, state[c])
        pair_first(c)
    early(0)
    when(second, c_wc.wait)
    c_w = send(wcol, wcol, ws.at[0], wr.at[0], to_partner, second)
    for c in range(3):
        pl.when(second)(functools.partial(own_pair, c, pairs[c]))

    pl.when(edge & second)(functools.partial(branch4, 0))
    pl.when(second)(functools.partial(own_pair, 3, pairs[3]))
    for b in range(1, cj // 16):
        branch1(b)
    plans = [finish_plan(c) for c in range(NC)]
    fwd = {c: a_plan(c) for c in range(NC - 1)}
    for c in range(3):
        z_pass(0, c)
        pl.when(~edge)(functools.partial(branch4, c))
        pl.when(z == 1)(functools.partial(branch16, c))
    z_pass(0, 3)
    branch1(0)
    pl.when(z >= 2)(functools.partial(branch4, 3))
    for c in range(NC):
        z_pass(1, c)

        @pl.when(z == 2)
        def _():
            branch16(c)
            finish(c)

    @pl.when(z != 2)
    def _():
        for c in range(NC):
            z_wait(2, c)

            @pl.when((z > 2) | (edge & (second | (c > 0))) | (c == 3))
            def _():
                branch16(c)

            if c == 3:
                pl.when(z < 2)(functools.partial(branch4, c))
            elif c > 0:
                pl.when(edge)(functools.partial(branch4, c))
            finish(c)
            if c == 2:
                pl.when(z > 2)(functools.partial(a_fwd, 0, fwd[0]))

    pl.when(z <= 2)(functools.partial(a_fwd, 0, fwd[0]))
    for c in range(1, NC - 1):
        a_fwd(c, fwd[c])
    fwd[NC - 1] = ()
    with jax.named_scope("w_wait"):
        when(first, c_w.wait_recv)
    for c in range(3):
        a_mix(c, fwd[c])
    macc[...] = sum(dot(back(c), mm[c * rows : (c + 1) * rows, :]) for c in range(3))
    for c in range(NC):
        plans[c][-1].wait_recv()
    lane = iota((1, hd), 1)
    acc = jnp.zeros((hd, tok), F32)
    for c in range(NC):
        x = jnp.where(lane == 0, lt[0, c].reshape(rows, hd), lt[1, c].reshape(rows, hd))
        hi = x.astype(BF)
        rest = x - hi.astype(F32)
        mid = rest.astype(BF)
        low = (rest - mid.astype(F32)).astype(BF)
        p = perm[c * rows : (c + 1) * rows, :]
        acc = acc + (dot_tn(hi, p) + dot_tn(mid, p) + dot_tn(low, p))
    log_ref[...] = acc[:2, :]
    a_mix(3, fwd[3])
    out_ref[...] = (macc[...] + dot(back(3), mm[3 * rows :, :])).astype(BF)
    with jax.named_scope("drain"):
        for cond, copy in pending:
            when(cond, copy.wait_send)
    for stage in range(3):
        @pl.when((z >= stage) & has_up)
        def _():
            for c in range(NC):
                for n in range(2):
                    z_copies[stage, c][n].wait_send()


def tables(tok, n_sp, hd):
    inv = ROTARY_BASE ** (-np.arange(0, hd, 2, dtype=np.float64) / hd)
    inv = np.concatenate([inv, inv]).astype(np.float32).astype(np.float64)
    nj = tok // WIDEST
    c, i, j = np.meshgrid(np.arange(NC), np.arange(NI), np.arange(nj), indexing="ij")
    off = (WIDEST * j + c + NC * i).reshape(-1).astype(np.float64)
    base = np.arange(n_sp, dtype=np.float64) * tok
    out = []
    for p in (off, base):
        a = p[:, None] * inv[None, :]
        out += [np.cos(a).astype(np.float32), np.sin(a).astype(np.float32)]
    return out


def local(n_tp, n_sp, hidden, norm_gain, w_query, w_key, w_value, query_gain, key_gain, w_out):
    tok, width = hidden.shape
    heads, hd = query_gain.shape
    rows = tok // NC
    nj = tok // WIDEST
    cj = 2 * nj
    keys = cj + KEYS_BEHIND
    w4 = cj + KEYS_BEHIND // NI
    tabc, tabs, basec, bases = tables(tok, n_sp, hd)
    dma = pltpu.SemaphoreType.DMA
    vm = pltpu.VMEM
    scratch = [
        vm((tok, width), BF),
        vm((n_tp * width // hd, hd), BF),
        vm((n_tp, 1, width), F32),
        vm((heads, hd), F32), vm((heads, hd), F32),
        vm((1, 1, hd), F32), vm((1, 1, hd), F32),
        vm((n_tp, tok, width), BF),
        vm((n_tp * width, 6 * hd), BF),
        vm((tok, hd), F32), vm((tok, hd), F32),
        vm((n_tp * heads * hd, width), BF),
        vm((3, WIDEST, nj, hd), F32),
        vm((3, WIDEST, cj, hd), F32),
        vm((WIDEST, cj, hd), BF),
        vm((2, WIDEST, keys, hd), BF),
        vm((WIDEST * 16, WIDEST * 32), F32), vm((WIDEST * 16, WIDEST * 32), F32),
        vm((NI * cj, NI * w4), F32),
        vm((cj, keys), F32),
        vm((WIDEST, cj, hd), F32), vm((WIDEST, cj, hd), F32), vm((WIDEST, cj, hd), F32),
        vm((WIDEST, cj, hd), F32), vm((WIDEST, cj, hd), F32), vm((WIDEST, cj, hd), F32),
        vm((NC, NI, cj, hd), F32),
        vm((NC, NI, cj, hd), F32),
        vm((NC, rows, hd), BF),
        vm((n_tp, NC, 2, rows, hd), BF),
        vm((2, NC, NI, nj, hd), F32),
        vm((tok, width), BF),
        vm((tok, width), F32),
        dma((15,)),
        dma((NC, 2)), dma((NC, 2)), dma((NC, 2)), dma((NC, 2)),
        dma((NC,)), dma((NC,)),
        dma((3, NC, 2)), dma((3, NC, 2)),
        dma((1,)), dma((1,)),
        dma((NC,)), dma((NC,)), dma((NC,)), dma((NC,)),
        dma((NC, 2, 2)), dma((NC, 2, 2)), dma((NC - 1, 2)), dma((NC - 1, 2)), dma((2,)), dma((2,)),
    ]
    hbm = pl.BlockSpec(memory_space=pltpu.HBM)
    vmem = pl.BlockSpec(memory_space=pltpu.VMEM)
    early_hx, early_wc = pl.pallas_call(
        functools.partial(early_kernel, n_tp),
        out_shape=(
            jax.ShapeDtypeStruct((n_tp, tok, width), BF),
            jax.ShapeDtypeStruct((n_tp * heads * hd, width), BF),
        ),
        in_specs=[hbm] * 2,
        out_specs=(hbm, hbm),
        scratch_shapes=[
            vm((tok, width), BF), vm((n_tp, tok, width), BF), vm((n_tp * heads * hd, width), BF),
            vm((2, heads * hd // 2, width), BF),
            dma((2,)), dma((2, 2)), dma((2, 2)), dma((2, 2)), dma((2, 2)), dma((6,)), dma((6,)), dma((2,)),
        ],
        compiler_params=pltpu.CompilerParams(
            collective_id=1, has_side_effects=True, vmem_limit_bytes=63 * 1024 * 1024
        ),
    )(hidden, w_out)
    mixed, logs = pl.pallas_call(
        functools.partial(kernel, n_tp, n_sp),
        out_shape=(
            pltpu.VMEM((tok, width), BF),
            pltpu.VMEM((heads, tok), F32),
        ),
        in_specs=[hbm] * 13,
        out_specs=(vmem, vmem),
        scratch_shapes=scratch,
        compiler_params=pltpu.CompilerParams(
            collective_id=0, has_side_effects=True, vmem_limit_bytes=63 * 1024 * 1024
        ),
    )(
        early_hx, early_wc, hidden, norm_gain.reshape(n_tp * width // hd, hd), w_query, w_key, w_value,
        query_gain, key_gain,
        jnp.asarray(tabc), jnp.asarray(tabs), jnp.asarray(basec)[:, None], jnp.asarray(bases)[:, None],
    )
    return mixed, logs.T


def solution(mesh):
    placed = (
        P(("grp", "sp"), "tp"),
        P(),
        P(None, "tp"),
        P(None, "tp"),
        P(None, "tp"),
        P("tp", None),
        P("tp", None),
        P("tp", None),
    )
    return jax.shard_map(
        functools.partial(local, mesh.shape["tp"], mesh.shape["sp"]),
        mesh=mesh,
        in_specs=placed,
        out_specs=(P(("grp", "sp"), "tp"), P(("grp", "sp"), "tp")),
        check_vma=False,
    )
```

```python
import functools

import jax
import jax.numpy as jnp
import numpy as np
from jax import lax
from jax.experimental import pallas as pl
from jax.experimental.pallas import tpu as pltpu
from jax.sharding import PartitionSpec as P

KEYS_BEHIND = 128
MIDDLE = 4
WIDEST = 16
EPSILON = 1e-06
ROTARY_BASE = 500000.0
NEG = -1e30

NC = MIDDLE
NI = WIDEST // MIDDLE
BF = jnp.bfloat16
F32 = jnp.float32
MESH = pl.DeviceIdType.MESH


def dot(a, b):
    return jnp.dot(a, b, preferred_element_type=F32)


def dot_nt(a, b):
    return lax.dot_general(a, b, (((1,), (1,)), ((), ())), preferred_element_type=F32)


def dot_tn(a, b):
    return lax.dot_general(a, b, (((0,), (0,)), ((), ())), preferred_element_type=F32)


def iota(shape, dim):
    return lax.broadcasted_iota(jnp.int32, shape, dim)


def early_kernel(
    n_tp, hid_h, wo_h, hx_out, wc_out,
    hid_v, hx, wcol, relay, lsem, xs_own, xr_own, xs_fwd, xr_fwd, ws, wr, osem,
):
    tok, width = hid_v.shape
    half = tok // 2
    wo_rows = wo_h.shape[0]
    me = lax.axis_index("tp")
    lf = lax.rem(me + n_tp - 1, n_tp)
    rt = lax.rem(me + 1, n_tp)
    op = lax.rem(me + 2, n_tp)

    def remote(src, dst, ssem, rsem, to):
        return pltpu.make_async_remote_copy(
            src_ref=src, dst_ref=dst, send_sem=ssem, recv_sem=rsem,
            device_id={"tp": to}, device_id_type=MESH,
        )

    def rows_of(ref, dev):
        return ref.at[pl.ds(pl.multiple_of(dev * wo_rows, wo_rows), wo_rows), :]

    def cols_of(dev):
        return wo_h.at[:, pl.ds(pl.multiple_of(dev * width, width), width)]

    @pl.when(lax.rem(lax.axis_index("sp"), 2) == 1)
    def _():
        c_hid = pltpu.make_async_copy(hid_h, hid_v, lsem.at[0])
        c_hid.start()
        barrier = pltpu.get_barrier_semaphore()
        for dev in (rt, lf, op):
            pl.semaphore_signal(barrier, inc=1, device_id={"tp": dev}, device_id_type=MESH)
        c_wo = pltpu.make_async_copy(cols_of(me), rows_of(wcol, me), lsem.at[1])
        c_wo.start()
        perm = placement(tok)
        c_hid.wait()
        hx[me] = dot(perm, hid_v[...]).astype(BF)
        pl.semaphore_wait(barrier, n_tp - 1)
        own, fwd = [], []
        for h in range(2):
            part = hx.at[me, pl.ds(h * half, half), :]
            own.append(remote(part, part, xs_own.at[h, 0], xr_own.at[h, 0], rt))
            own.append(remote(part, part, xs_own.at[h, 1], xr_own.at[h, 1], lf))
        for copy in own:
            copy.start()
        out = [remote(cols_of(dev), rows_of(wcol, me), ws.at[n], wr.at[n], dev) for n, dev in enumerate((rt, lf))]
        wh = wo_rows // 2
        turn, relayed = [], []
        for n, (dev, src) in enumerate(((rt, lf), (lf, rt))):
            part = wo_h.at[pl.ds(n * wh, wh), pl.ds(pl.multiple_of(op * width, width), width)]
            turn.append(remote(part, relay.at[n], ws.at[2 + n], wr.at[2 + n], dev))
            to = wcol.at[pl.ds(pl.multiple_of(src * wo_rows + n * wh, wh), wh), :]
            relayed.append(remote(relay.at[n], to, ws.at[4 + n], wr.at[4 + n], dev))
        for h in range(2):
            lo = pl.ds(h * half, half // 2)
            hi = pl.ds(h * half + half // 2, half // 2)
            own[2 * h].wait_recv()
            fwd.append(remote(hx.at[lf, lo, :], hx.at[lf, lo, :], xs_fwd.at[h, 0], xr_fwd.at[h, 0], rt))
            fwd[-1].start()
            own[2 * h + 1].wait_recv()
            fwd.append(remote(hx.at[rt, hi, :], hx.at[rt, hi, :], xs_fwd.at[h, 1], xr_fwd.at[h, 1], lf))
            fwd[-1].start()
        for copy in turn + out:
            copy.start()
        for n in range(2):
            turn[n].wait_recv()
            relayed[n].start()
        out = out + relayed
        for copy in fwd:
            copy.wait_recv()
        o_hx = pltpu.make_async_copy(hx, hx_out, osem.at[0])
        o_hx.start()
        c_wo.wait()
        for copy in out:
            copy.wait_recv()
        o_wc = pltpu.make_async_copy(wcol, wc_out, osem.at[1])
        o_wc.start()
        for copy in own + fwd + turn + out:
            copy.wait_send()
        o_hx.wait()
        o_wc.wait()


def placement(tok):
    prow = iota((tok, tok), 0)
    pcol = iota((tok, tok), 1)
    place = (pcol & (NC - 1)) * (tok // NC) + ((pcol >> 2) & (NI - 1)) * (tok // WIDEST) + (pcol >> 4)
    return jnp.where(prow == place, 1.0, 0.0).astype(BF)


def kernel(
    n_tp, n_sp, hxe_h, wce_h,
    hid_h, ng_h, wq_h, wk_h, wv_h, qg_h, kg_h, tabc_h, tabs_h, basec_h, bases_h,
    out_ref, log_ref,
    hid_v, ng_v, ngain, qg_ref, kg_ref, basec, bases, hx, w_v, tabc, tabs, wcol, sbuf, fbuf, qb, kv, bias1, bias1e, bias4, bias16,
    o1, o4, o16, e1, e4, e16, attb, attl, attx, ag, lt, mm, macc,
    lsem, xs_own, xr_own, xs_fwd, xr_fwd, ds_q, dr_q, zs, zr, ws, wr,
    ds_a, dr_a, ds_l, dr_l, as_own, ar_own, as_fwd, ar_fwd, as_op, ar_op,
):
    tok, width = hid_v.shape
    rows = tok // NC
    half = rows // 2
    nj = tok // WIDEST
    cj = 2 * nj
    hd = KEYS_BEHIND
    depth = n_tp * width
    own0 = kv.shape[2] - cj
    n_near = own0 - cj
    n_far = n_near - cj
    last = n_far

    me = lax.axis_index("tp")
    sp = lax.axis_index("sp")
    core = lax.rem(sp, 2)
    other = 1 - core
    z = lax.div(sp, 2)
    lf = lax.rem(me + n_tp - 1, n_tp)
    rt = lax.rem(me + 1, n_tp)
    op = lax.rem(me + 2, n_tp)
    partner = sp + 1 - 2 * core
    up = lax.rem(sp + 2, n_sp)
    down = lax.rem(sp + n_sp - 2, n_sp)
    to_rt, to_lf, to_op = {"tp": rt}, {"tp": lf}, {"tp": op}
    to_partner, to_up, to_down = {"sp": partner}, {"sp": up}, {"sp": down}
    joff = pl.multiple_of(core * nj, 8)
    poff = pl.multiple_of(other * nj, 8)

    first, second = core == 0, core == 1
    pending = []

    def when(cond, f):
        if cond is None:
            f()
        else:
            pl.when(cond)(f)

    def send(src, dst, ssem, rsem, dev, cond=None):
        copy = pltpu.make_async_remote_copy(
            src_ref=src, dst_ref=dst, send_sem=ssem, recv_sem=rsem, device_id=dev, device_id_type=MESH
        )
        when(cond, copy.start)
        pending.append((cond, copy))
        return copy

    def load(src, dst, k):
        copy = pltpu.make_async_copy(src, dst, lsem.at[k])
        copy.start()
        return copy

    c_hid = pltpu.make_async_copy(hid_h, hid_v, lsem.at[0])
    c_hx = pltpu.make_async_copy(hxe_h, hx, lsem.at[0])
    c_wc = pltpu.make_async_copy(wce_h, wcol, lsem.at[9])
    barrier = pltpu.get_barrier_semaphore()
    peers = [
        to_rt, to_lf, to_op, to_partner,
        {"tp": rt, "sp": partner}, {"tp": lf, "sp": partner}, {"tp": op, "sp": partner},
    ]
    for dev in peers:
        pl.semaphore_signal(barrier, inc=1, device_id=dev, device_id_type=MESH)
    has_up, has_down = z < n_sp // 2 - 1, z > 0

    @pl.when(has_down)
    def _():
        pl.semaphore_signal(barrier, inc=1, device_id=to_down, device_id_type=MESH)

    when(first, c_hid.start)
    when(second, c_hx.start)
    own_col = pl.ds(pl.multiple_of(core * hd, hd), hd)
    oth_col = pl.ds(pl.multiple_of(other * hd, hd), hd)
    c_w = []
    for n, w in enumerate((wq_h, wk_h, wv_h)):
        c_w.append(load(w.at[:, own_col], w_v.at[:, pl.ds(n * hd, hd)], 1 + 2 * n))
        c_w.append(load(w.at[:, oth_col], w_v.at[:, pl.ds((3 + n) * hd, hd)], 2 + 2 * n))
    c_t = [load(tabc_h, tabc, 7), load(tabs_h, tabs, 8)]
    for n, (src, dst) in enumerate(
        ((ng_h, ng_v), (qg_h, qg_ref), (kg_h, kg_ref), (basec_h.at[pl.ds(sp, 1)], basec), (bases_h.at[pl.ds(sp, 1)], bases))
    ):
        c_t.append(load(src, dst, 10 + n))
    when(second, c_wc.start)

    perm = placement(tok)

    @pl.when(first)
    def _():
        with jax.named_scope("hid_wait"):
            c_hid.wait()
        hx[me, :rows, :] = dot(perm[:rows], hid_v[...]).astype(BF)

    with jax.named_scope("barrier_wait"):
        pl.semaphore_wait(barrier, len(peers) + has_up.astype(jnp.int32))

    def x_own(c):
        part = hx.at[me, pl.ds(c * rows, rows), :]
        return (
            send(part, part, xs_own.at[c, 0], xr_own.at[c, 0], to_rt, first),
            send(part, part, xs_own.at[c, 1], xr_own.at[c, 1], to_lf, first),
        )

    x_sent = {0: x_own(0)}

    @pl.when(first)
    def _():
        hx[me, rows:, :] = dot(perm[rows:], hid_v[...]).astype(BF)

    x_sent.update({c: x_own(c) for c in range(1, NC)})

    for stage, (lo, hi) in enumerate(((n_near, own0), (n_far, n_near), (0, n_far))):
        @pl.when(z <= stage)
        def _():
            kv[:, :, lo:hi, :] = jnp.zeros((2, WIDEST, hi - lo, hd), BF)

    for c in c_t:
        c.wait()
    bc, bs = basec[0], bases[0]
    oc, os_ = tabc[...], tabs[...]
    sign = jnp.where(iota((1, hd), 1) < hd // 2, -1.0, 1.0)
    tabc[...] = bc * oc - bs * os_
    tabs[...] = (bs * oc + bc * os_) * sign

    gains = ng_v[...].astype(F32)
    for s in range(n_tp):
        for k in range(width // hd):
            r = s * (width // hd) + k
            ngain[s, :, k * hd : (k + 1) * hd] = gains[r : r + 1, :]
    first_j = own0 - cj * z
    jq = iota((cj, own0 + cj), 0)
    jk = iota((cj, own0 + cj), 1)
    ok = (jk >= jq) & (jk <= jq + KEYS_BEHIND) & (jk >= first_j)
    bias16[...] = jnp.where(ok, 0.0, NEG)
    w4 = bias4.shape[1] // NI
    row = iota(bias4.shape, 0)
    col = iota(bias4.shape, 1)
    iq = (row * (65536 // cj + 1)) >> 16
    ik = (col * (65536 // w4 + 1)) >> 16
    j4 = own0 + cj - w4
    jk = j4 + col - ik * w4
    dist = NI * (own0 + (row - iq * cj) - jk) + iq - ik
    ok = (dist >= 0) & (dist <= KEYS_BEHIND) & (jk >= first_j)
    bias4[...] = jnp.where(ok, 0.0, NEG)
    row = iota(bias1.shape, 0)
    col = iota(bias1.shape, 1)
    uq = row >> 4
    uk = col >> 5
    rq = (uq >> 2) + NC * (uq & (NI - 1))
    rk = (uk >> 2) + NC * (uk & (NI - 1))
    dist = WIDEST * ((row & 15) + 16 - (col & 31)) + rq - rk
    ok = (dist >= 0) & (dist <= KEYS_BEHIND)
    bias1[...] = jnp.where(ok, 0.0, NEG)
    bias1e[...] = jnp.where(ok & ((col & 31) + own0 - 16 >= first_j), 0.0, NEG)

    @jax.named_scope('partial')
    def partial(c, s, acc, sq):
        h = hx[s, c * rows : (c + 1) * rows, :].astype(F32)
        sc = (h * ngain[s]).astype(BF)
        sq = sq + jnp.sum(h * h, axis=1, keepdims=True)
        acc = acc + dot(sc, w_v[pl.ds(pl.multiple_of(s * width, width), width), :])
        return acc, sq

    def head_rows(x, gain, cos, sin):
        x = x * lax.rsqrt(jnp.mean(x * x, axis=1, keepdims=True) + EPSILON) * gain
        return x * cos + pltpu.roll(x, hd // 2, 1) * sin

    @jax.named_scope('epilogue')
    def epilogue(c, acc, sq):
        rs = lax.rsqrt(sq / depth + EPSILON)
        cos = tabc[c * rows : (c + 1) * rows, :]
        sin = tabs[c * rows : (c + 1) * rows, :]
        parts = []
        for side, hidx in ((1, other), (0, core)):
            x = [acc[:, (3 * side + n) * hd : (3 * side + n + 1) * hd] * rs for n in range(3)]
            q = head_rows(x[0], qg_ref[pl.ds(hidx, 1), :], cos, sin)
            k = head_rows(x[1], kg_ref[pl.ds(hidx, 1), :], cos, sin)
            parts = [v.reshape(NI, nj, hd) for v in (q, k, x[2])]
            for n in range(3):
                if side == 1:
                    sbuf[n, c * NI : (c + 1) * NI, :, :] = parts[n]
                else:
                    fbuf[n, c * NI : (c + 1) * NI, pl.ds(joff, nj), :] = parts[n]
        return send(
            sbuf.at[:, pl.ds(c * NI, NI), :, :],
            fbuf.at[:, pl.ds(c * NI, NI), pl.ds(joff, nj), :],
            ds_q.at[c], dr_q.at[c], to_partner,
        )

    z_copies = {}
    for stage, (start, count, to) in enumerate(
        ((own0, cj, n_near), (n_near, cj, n_far), (n_far + cj - last, last, 0))
    ):
        for c in range(NC):
            u = pl.ds(c * NI, NI)
            z_copies[stage, c] = [
                pltpu.make_async_remote_copy(
                    src_ref=kv.at[n, u, pl.ds(start, count), :], dst_ref=kv.at[n, u, pl.ds(to, count), :],
                    send_sem=zs.at[stage, c, n], recv_sem=zr.at[stage, c, n],
                    device_id=to_up, device_id_type=MESH,
                )
                for n in range(2)
            ]

    def z_send(stage, c, n):
        when((z >= stage) & has_up, z_copies[stage, c][n].start)

    @jax.named_scope('z_wait')
    def z_wait(stage, c):
        for n in range(2):
            when(z > stage, z_copies[stage, c][n].wait_recv)

    @jax.named_scope('z_pass')
    def z_pass(stage, c):
        for n in range(2):
            when(z > stage, z_copies[stage, c][n].wait_recv)
            z_send(stage + 1, c, n)

    @jax.named_scope('own_pair')
    def own_pair(c, copy):
        with jax.named_scope("pair_wait"):
            copy.wait_recv()
        u = slice(c * NI, (c + 1) * NI)
        for n in range(2):
            kv[n, u, own0:, :] = fbuf[1 + n, u].astype(BF)
            z_send(0, c, n)
        qb[u] = fbuf[0, u].astype(BF)

    for c in c_w:
        c.wait()
    def x_pass(c):
        right, left = x_sent[c]
        with jax.named_scope("x_wait"):
            when(first, right.wait_recv)
        h0 = hx.at[lf, pl.ds(c * rows, half), :]
        f0 = send(h0, h0, xs_fwd.at[c, 0], xr_fwd.at[c, 0], to_rt, first)
        with jax.named_scope("x_wait"):
            when(first, left.wait_recv)
        h1 = hx.at[rt, pl.ds(c * rows + half, half), :]
        f1 = send(h1, h1, xs_fwd.at[c, 1], xr_fwd.at[c, 1], to_lf, first)
        return f0, f1

    def x_near(c, passed):
        acc = jnp.zeros((rows, 6 * hd), F32)
        sq = jnp.zeros((rows, 1), F32)
        for s in (me, lf, rt):
            acc, sq = partial(c, s, acc, sq)
        return acc, sq, *passed

    def x_end(c, state):
        acc, sq, f0, f1 = state
        with jax.named_scope("xf_wait"):
            when(first, f0.wait_recv)
            when(first, f1.wait_recv)
        acc, sq = partial(c, op, acc, sq)
        return epilogue(c, acc, sq)

    with jax.named_scope("hx_wait"):
        when(second, c_hx.wait)
    def softmax(s, bias):
        s = s * (hd ** -0.5) + bias
        m = jnp.max(s, axis=1, keepdims=True)
        w = jnp.exp(s - m)
        l = jnp.sum(w, axis=1, keepdims=True)
        return w.astype(BF), m, l

    def wide(x):
        return jnp.broadcast_to(x, (x.shape[0], hd))

    @jax.named_scope('branch1')
    def branch1(b):
        q = qb[:, 16 * b : 16 * b + 16, :].reshape(WIDEST * 16, hd)
        lo = own0 - 16 + 16 * b
        k = kv[0, :, lo : lo + 32, :].reshape(WIDEST * 32, hd)
        v = kv[1, :, lo : lo + 32, :].reshape(WIDEST * 32, hd)
        w, m, l = softmax(dot_nt(q, k), (bias1e if b == 0 else bias1)[...])
        o1[:, 16 * b : 16 * b + 16, :] = (dot(w, v) / l).reshape(WIDEST, 16, hd)
        e1[:, 16 * b : 16 * b + 16, :] = wide(m + jnp.log(l)).reshape(WIDEST, 16, hd)

    @jax.named_scope('branch4')
    def branch4(c):
        u = slice(c * NI, (c + 1) * NI)
        q = qb[u].reshape(NI * cj, hd)
        k = kv[0, u, j4:, :].reshape(NI * w4, hd)
        v = kv[1, u, j4:, :].reshape(NI * w4, hd)
        w, m, l = softmax(dot_nt(q, k), bias4[...])
        o4[u] = (dot(w, v) / l).reshape(NI, cj, hd)
        e4[u] = wide(m + jnp.log(l)).reshape(NI, cj, hd)

    @jax.named_scope('branch16')
    def branch16(c):
        us = range(c * NI, (c + 1) * NI)
        s = jnp.concatenate([dot_nt(qb[u], kv[0, u]) for u in us], axis=0)
        w, m, l = softmax(s, jnp.concatenate([bias16[...]] * NI, axis=0))
        e16[c * NI : (c + 1) * NI] = wide(m + jnp.log(l)).reshape(NI, cj, hd)
        for n, u in enumerate(us):
            part = slice(n * cj, (n + 1) * cj)
            o16[u] = dot(w[part], kv[1, u]) / l[part]

    @jax.named_scope('finish')
    def finish(c):
        u = slice(c * NI, (c + 1) * NI)
        a, b, d = e1[u], e4[u], e16[u]
        top = jnp.maximum(jnp.maximum(a, b), d)
        total = top + jnp.log(jnp.exp(a - top) + jnp.exp(b - top) + jnp.exp(d - top))
        att = jnp.exp(a - total) * o1[u] + jnp.exp(b - total) * o4[u] + jnp.exp(d - total) * o16[u]
        attb[c] = att
        attl[c] = total
        attx[c] = attb[c, :, pl.ds(poff, nj), :].reshape(rows, hd).astype(BF)
        ag[me, c, core] = attb[c, :, pl.ds(joff, nj), :].reshape(rows, hd).astype(BF)
        lt[core, c] = attl[c, :, pl.ds(joff, nj), :]
        for copy in plans[c]:
            copy.start()

    def finish_plan(c):
        same, cross = ag.at[me, c, core], attx.at[c]
        copies = []

        def add(src, dst, ssem, rsem, dev):
            copies.append(
                pltpu.make_async_remote_copy(
                    src_ref=src, dst_ref=dst, send_sem=ssem, recv_sem=rsem, device_id=dev, device_id_type=MESH
                )
            )
            pending.append((None, copies[-1]))

        for side, dev in ((0, rt), (1, lf)):
            add(same, same, as_own.at[c, side, 0], ar_own.at[c, side, core], {"tp": dev})
            add(cross, same, as_own.at[c, side, 1], ar_own.at[c, side, core], {"tp": dev, "sp": partner})
        if c == NC - 1:
            add(same, same, as_op.at[0], ar_op.at[core], to_op)
            add(cross, same, as_op.at[1], ar_op.at[core], {"tp": op, "sp": partner})
        add(cross, same, ds_a.at[c], dr_a.at[c], to_partner)
        add(attl.at[c, :, pl.ds(poff, nj), :], lt.at[core, c], ds_l.at[c], dr_l.at[c], to_partner)
        return copies

    def arrived(ref, sem):
        pltpu.make_async_remote_copy(
            src_ref=ref, dst_ref=ref, send_sem=sem, recv_sem=sem, device_id=to_partner, device_id_type=MESH
        ).wait_recv()

    def a_plan(c):
        p0, p1 = ag.at[lf, c, 0], ag.at[rt, c, 1]
        f0 = pltpu.make_async_remote_copy(
            src_ref=p0, dst_ref=p0, send_sem=as_fwd.at[c, 0], recv_sem=ar_fwd.at[c, 0],
            device_id=to_rt, device_id_type=MESH,
        )
        f1 = pltpu.make_async_remote_copy(
            src_ref=p1, dst_ref=p1, send_sem=as_fwd.at[c, 1], recv_sem=ar_fwd.at[c, 1],
            device_id=to_lf, device_id_type=MESH,
        )
        pending.extend([(None, f0), (None, f1)])
        return f0, f1

    @jax.named_scope('a_fwd')
    def a_fwd(c, copies):
        arrived(ag.at[lf, c, 0], ar_own.at[c, 0, 0])
        copies[0].start()
        arrived(ag.at[rt, c, 1], ar_own.at[c, 1, 1])
        copies[1].start()

    @jax.named_scope('a_mix')
    def a_mix(c, copies):
        with jax.named_scope("af_wait"):
            arrived(ag.at[lf, c, 1], ar_own.at[c, 0, 1])
            arrived(ag.at[rt, c, 0], ar_own.at[c, 1, 0])
            arrived(ag.at[me, c, other], dr_a.at[c])
            if c < NC - 1:
                for f in copies:
                    f.wait_recv()
            else:
                arrived(ag.at[lf, c, 0], ar_own.at[c, 0, 0])
                arrived(ag.at[rt, c, 1], ar_own.at[c, 1, 1])
                for h in range(2):
                    arrived(ag.at[op, c, h], ar_op.at[h])
        lhs = jnp.concatenate([ag[s, c, h] for s in range(n_tp) for h in range(2)], axis=1)
        mm[c * rows : (c + 1) * rows, :] = dot(lhs, wcol[...]).astype(BF)

    t0 = iota((tok, 2 * rows), 0)
    q0 = iota((tok, 2 * rows), 1)

    def back(c):
        there = q0 + c * rows == (t0 & (NC - 1)) * rows + ((t0 >> 2) & (NI - 1)) * nj + (t0 >> 4)
        return jnp.where(there, 1.0, 0.0).astype(BF)

    state, pairs = {}, {}
    edge = z == 0

    def early(c):
        @pl.when(edge & first)
        def _():
            branch16(c)
            branch4(c)

    def pair_first(c):
        pl.when(first)(functools.partial(own_pair, c, pairs[c]))

    for c in range(NC):
        state[c] = x_near(c, x_pass(c))
    for c in range(NC):
        pairs[c] = x_end(c, state[c])
        pair_first(c)
    early(0)
    when(second, c_wc.wait)
    c_w = send(wcol, wcol, ws.at[0], wr.at[0], to_partner, second)
    for c in range(3):
        pl.when(second)(functools.partial(own_pair, c, pairs[c]))

    pl.when(edge & second)(functools.partial(branch4, 0))
    pl.when(second)(functools.partial(own_pair, 3, pairs[3]))
    for b in range(1, cj // 16):
        branch1(b)
    plans = [finish_plan(c) for c in range(NC)]
    fwd = {c: a_plan(c) for c in range(NC - 1)}
    for c in range(3):
        z_pass(0, c)
        pl.when(~edge)(functools.partial(branch4, c))
        pl.when(z == 1)(functools.partial(branch16, c))
    z_pass(0, 3)
    branch1(0)
    pl.when(z >= 2)(functools.partial(branch4, 3))
    for c in range(NC):
        z_pass(1, c)

        @pl.when(z == 2)
        def _():
            branch16(c)
            finish(c)

    @pl.when(z != 2)
    def _():
        for c in range(NC):
            z_wait(2, c)

            @pl.when((z > 2) | (edge & (second | (c > 0))) | (c == 3))
            def _():
                branch16(c)

            if c == 3:
                pl.when(z < 2)(functools.partial(branch4, c))
            elif c > 0:
                pl.when(edge)(functools.partial(branch4, c))
            finish(c)
            if c == 2:
                pl.when(z > 2)(functools.partial(a_fwd, 0, fwd[0]))

    pl.when(z <= 2)(functools.partial(a_fwd, 0, fwd[0]))
    for c in range(1, NC - 1):
        a_fwd(c, fwd[c])
    fwd[NC - 1] = ()
    for c in range(NC):
        plans[c][-1].wait_recv()
    lane = iota((1, hd), 1)
    acc = jnp.zeros((hd, tok), F32)
    for c in range(NC):
        x = jnp.where(lane == 0, lt[0, c].reshape(rows, hd), lt[1, c].reshape(rows, hd))
        hi = x.astype(BF)
        rest = x - hi.astype(F32)
        mid = rest.astype(BF)
        low = (rest - mid.astype(F32)).astype(BF)
        p = perm[c * rows : (c + 1) * rows, :]
        acc = acc + (dot_tn(hi, p) + dot_tn(mid, p) + dot_tn(low, p))
    log_ref[...] = acc[:2, :]
    with jax.named_scope("w_wait"):
        when(first, c_w.wait_recv)
    a_mix(0, fwd[0])
    a_mix(1, fwd[1])
    macc[...] = dot(back(0), mm[: 2 * rows, :])
    a_mix(2, fwd[2])
    a_mix(3, fwd[3])
    out_ref[...] = (macc[...] + dot(back(2), mm[2 * rows :, :])).astype(BF)
    with jax.named_scope("drain"):
        for cond, copy in pending:
            when(cond, copy.wait_send)
    for stage in range(3):
        @pl.when((z >= stage) & has_up)
        def _():
            for c in range(NC):
                for n in range(2):
                    z_copies[stage, c][n].wait_send()


def tables(tok, n_sp, hd):
    inv = ROTARY_BASE ** (-np.arange(0, hd, 2, dtype=np.float64) / hd)
    inv = np.concatenate([inv, inv]).astype(np.float32).astype(np.float64)
    nj = tok // WIDEST
    c, i, j = np.meshgrid(np.arange(NC), np.arange(NI), np.arange(nj), indexing="ij")
    off = (WIDEST * j + c + NC * i).reshape(-1).astype(np.float64)
    base = np.arange(n_sp, dtype=np.float64) * tok
    out = []
    for p in (off, base):
        a = p[:, None] * inv[None, :]
        out += [np.cos(a).astype(np.float32), np.sin(a).astype(np.float32)]
    return out


def local(n_tp, n_sp, hidden, norm_gain, w_query, w_key, w_value, query_gain, key_gain, w_out):
    tok, width = hidden.shape
    heads, hd = query_gain.shape
    rows = tok // NC
    nj = tok // WIDEST
    cj = 2 * nj
    keys = cj + KEYS_BEHIND
    w4 = cj + KEYS_BEHIND // NI
    tabc, tabs, basec, bases = tables(tok, n_sp, hd)
    dma = pltpu.SemaphoreType.DMA
    vm = pltpu.VMEM
    scratch = [
        vm((tok, width), BF),
        vm((n_tp * width // hd, hd), BF),
        vm((n_tp, 1, width), F32),
        vm((heads, hd), F32), vm((heads, hd), F32),
        vm((1, 1, hd), F32), vm((1, 1, hd), F32),
        vm((n_tp, tok, width), BF),
        vm((n_tp * width, 6 * hd), BF),
        vm((tok, hd), F32), vm((tok, hd), F32),
        vm((n_tp * heads * hd, width), BF),
        vm((3, WIDEST, nj, hd), F32),
        vm((3, WIDEST, cj, hd), F32),
        vm((WIDEST, cj, hd), BF),
        vm((2, WIDEST, keys, hd), BF),
        vm((WIDEST * 16, WIDEST * 32), F32), vm((WIDEST * 16, WIDEST * 32), F32),
        vm((NI * cj, NI * w4), F32),
        vm((cj, keys), F32),
        vm((WIDEST, cj, hd), F32), vm((WIDEST, cj, hd), F32), vm((WIDEST, cj, hd), F32),
        vm((WIDEST, cj, hd), F32), vm((WIDEST, cj, hd), F32), vm((WIDEST, cj, hd), F32),
        vm((NC, NI, cj, hd), F32),
        vm((NC, NI, cj, hd), F32),
        vm((NC, rows, hd), BF),
        vm((n_tp, NC, 2, rows, hd), BF),
        vm((2, NC, NI, nj, hd), F32),
        vm((tok, width), BF),
        vm((tok, width), F32),
        dma((15,)),
        dma((NC, 2)), dma((NC, 2)), dma((NC, 2)), dma((NC, 2)),
        dma((NC,)), dma((NC,)),
        dma((3, NC, 2)), dma((3, NC, 2)),
        dma((1,)), dma((1,)),
        dma((NC,)), dma((NC,)), dma((NC,)), dma((NC,)),
        dma((NC, 2, 2)), dma((NC, 2, 2)), dma((NC - 1, 2)), dma((NC - 1, 2)), dma((2,)), dma((2,)),
    ]
    hbm = pl.BlockSpec(memory_space=pltpu.HBM)
    vmem = pl.BlockSpec(memory_space=pltpu.VMEM)
    early_hx, early_wc = pl.pallas_call(
        functools.partial(early_kernel, n_tp),
        out_shape=(
            jax.ShapeDtypeStruct((n_tp, tok, width), BF),
            jax.ShapeDtypeStruct((n_tp * heads * hd, width), BF),
        ),
        in_specs=[hbm] * 2,
        out_specs=(hbm, hbm),
        scratch_shapes=[
            vm((tok, width), BF), vm((n_tp, tok, width), BF), vm((n_tp * heads * hd, width), BF),
            vm((2, heads * hd // 2, width), BF),
            dma((2,)), dma((2, 2)), dma((2, 2)), dma((2, 2)), dma((2, 2)), dma((6,)), dma((6,)), dma((2,)),
        ],
        compiler_params=pltpu.CompilerParams(
            collective_id=1, has_side_effects=True, vmem_limit_bytes=63 * 1024 * 1024
        ),
    )(hidden, w_out)
    mixed, logs = pl.pallas_call(
        functools.partial(kernel, n_tp, n_sp),
        out_shape=(
            pltpu.VMEM((tok, width), BF),
            pltpu.VMEM((heads, tok), F32),
        ),
        in_specs=[hbm] * 13,
        out_specs=(vmem, vmem),
        scratch_shapes=scratch,
        compiler_params=pltpu.CompilerParams(
            collective_id=0, has_side_effects=True, vmem_limit_bytes=63 * 1024 * 1024
        ),
    )(
        early_hx, early_wc, hidden, norm_gain.reshape(n_tp * width // hd, hd), w_query, w_key, w_value,
        query_gain, key_gain,
        jnp.asarray(tabc), jnp.asarray(tabs), jnp.asarray(basec)[:, None], jnp.asarray(bases)[:, None],
    )
    return mixed, logs.T


def solution(mesh):
    placed = (
        P(("grp", "sp"), "tp"),
        P(),
        P(None, "tp"),
        P(None, "tp"),
        P(None, "tp"),
        P("tp", None),
        P("tp", None),
        P("tp", None),
    )
    return jax.shard_map(
        functools.partial(local, mesh.shape["tp"], mesh.shape["sp"]),
        mesh=mesh,
        in_specs=placed,
        out_specs=(P(("grp", "sp"), "tp"), P(("grp", "sp"), "tp")),
        check_vma=False,
    )
```
